256 devices in a mesh: grp: 2 (over y), ep: 32 (over z, core), tp: 4 (over x).
Axes of the slice: x: 4, y: 2, z: 16, core: 2. Of those that a mesh axis runs over, the one named last changes fastest.
The devices are a block of a 4x16x16 slice.
Arguments:
- queries: bfloat16 [32768, 512], P(('grp', 'ep'), 'tp'), parts along dimension 0, may hold values from -6 to 6
- keys: bfloat16 [32768, 512], P(('grp', 'ep'), 'tp'), parts along dimension 0, may hold values from -6 to 6
- values: bfloat16 [32768, 1024], P(('grp', 'ep'), 'tp'), parts along dimension 0, may hold values from -6 to 6
- gate: bfloat16 [32768, 1024], P(('grp', 'ep'), 'tp'), parts along dimension 0, may hold values from -6 to 6
- log_decay: float32 [32768, 8], P(('grp', 'ep'), 'tp'), parts along dimension 0, may hold values from -1 to 0, as said below
- w_out: bfloat16 [1024, 2048], P('tp'), may hold values from -0.1875 to 0.1875
- moe_input: bfloat16 [32768, 2048], P(('grp', 'ep', 'tp')), parts along dimension 0, may hold values from -40 to 40
- moe_gain: float32 [2048], replicated, may hold values from 0.1 to 1.9
- routes: int32 [32768, 2], P(('grp', 'ep', 'tp')), parts along dimension 0, may hold values from 0 to 127, all different within a row; in each aligned block of 128 rows (0 to 127, 128 to 255, ...) at most 3 rows name the same one
- route_weight: float32 [32768, 2], P(('grp', 'ep', 'tp')), parts along dimension 0, may hold values from 0.1 to 1
- expert_gate: bfloat16 [128, 2048, 512], P(('ep', 'tp')), may hold values from -0.125 to 0.125
- expert_up: bfloat16 [128, 2048, 512], P(('ep', 'tp')), may hold values from -0.125 to 0.125
- expert_down: bfloat16 [128, 512, 2048], P(('ep', 'tp')), may hold values from -0.25 to 0.25
- shared_gate: bfloat16 [2048, 512], P(None, 'tp'), may hold values from -0.125 to 0.125
- shared_up: bfloat16 [2048, 512], P(None, 'tp'), may hold values from -0.125 to 0.125
- shared_down: bfloat16 [512, 2048], P('tp'), may hold values from -0.25 to 0.25
Outputs:
- mixer_out: bfloat16 [32768, 2048], P(('grp', 'ep', 'tp')), parts along dimension 0
- moe_out: bfloat16 [32768, 2048], P(('grp', 'ep', 'tp')), parts along dimension 0
The draws below stay inside these ranges and needn't reach their ends.
There are 2 independent parts, one for each index of `grp`. The reference program is written for one: setup_inputs(seed, part) draws one part's arguments, and reference() takes and returns one part's arrays. A program takes and returns all parts, laid end to end along the dimension named above; an argument that names none is the same for every part. Nothing has to cross between parts.
Inputs may be any that keep to these rules, and one draw needn't show every extreme that they name: `routes`: each row names 2 different experts; in each aligned block of 128 rows (the rows of one device) no expert is named by more than 3 rows, a bound that some block reaches. `log_decay`: below zero.
All inputs are finite; a program needn't handle non-finite values.
Results may differ from the reference program's by a relative error of at most 0.015.
Values may be sent and summed in bfloat16 or wider, within the bound.
No kernel may reach another device: no remote copies, remote signals or barrier semaphores. Data moves between devices by JAX's collectives and lax.ppermute only.
A program may use at most 128 MiB of HBM per device.

```python
import math
import jax
import jax.numpy as jnp
import numpy as np
from jax import lax

D = 2048
RETENTION_HEADS = 8
DK = 64
DV = 128
BLOCK = 128
FFE = 512
SH = 512
TOP = 2
TOK_DEV = 128
SPAN = 512
SEQUENCE_LENGTH = 16384
ROWS = 16384
EXPERTS = 128
CAP = 3
N_TP = 4


def draw_log_decay(key, part):
    parallel_flows = jax.random.split(key, 6)
    share = 0.5
    fast_head = jax.random.uniform(parallel_flows[0], (RETENTION_HEADS,)) < share
    reach_len = jnp.exp(jax.random.uniform(parallel_flows[1], (RETENTION_HEADS,), minval=math.log(30.0), maxval=math.log(100.0)))
    slow_rate = jax.random.uniform(parallel_flows[2], (RETENTION_HEADS,), minval=0.05, maxval=0.2) / SEQUENCE_LENGTH
    head_decay_rate = jnp.where(fast_head, math.log(10.0) / reach_len, slow_rate)
    decay_factor = jnp.exp(jax.random.uniform(parallel_flows[3], (SEQUENCE_LENGTH // SPAN, RETENTION_HEADS), minval=math.log(0.5), maxval=math.log(2.0)))
    decay_factor = jnp.repeat(decay_factor, SPAN, axis=0)
    expert_spike = jax.random.uniform(parallel_flows[4], (SEQUENCE_LENGTH, RETENTION_HEADS)) < 2.0 / SEQUENCE_LENGTH
    spike_penalty = jax.random.uniform(parallel_flows[5], (SEQUENCE_LENGTH, RETENTION_HEADS), minval=math.log(0.5), maxval=math.log(0.8))
    return (-head_decay_rate[None, :] * decay_factor + jnp.where(expert_spike, spike_penalty, 0.0)).astype(jnp.float32)


def draw_moe_input(key, part):
    parallel_flows = jax.random.split(key, 2)
    row_scale = jnp.exp(jax.random.uniform(parallel_flows[0], (ROWS, 1), minval=0.0, maxval=math.log(10.0)))
    base = jnp.clip(jax.random.normal(parallel_flows[1], (ROWS, D)), -4.0, 4.0)
    return (base * row_scale).astype(jnp.bfloat16)


def shard_levels(rng, extent, cuts, low, high):
    def one(dim, shards_of):
        steps = jax.random.uniform(jax.random.fold_in(jax.random.fold_in(rng, 6), dim), (shards_of,), jnp.float32, low / len(cuts), high / len(cuts))
        return jnp.repeat(jnp.exp(steps), extent[dim] // shards_of).reshape((-1,) + (1,) * (len(extent) - dim - 1))

    loudness = one(*cuts[0])
    for cut in cuts[1:]:
        loudness = loudness * one(*cut)
    return loudness


def shared_out(own_key, own, number, rows, count, top, reach, slope):
    sequence = jax.random.permutation(own_key, count)
    heavy_load, usual = load_shares(count, rows * top, reach, slope, True), load_shares(count, rows * top, reach, slope, False)
    places = jnp.arange(count)

    def named(sizes, offset_by):
        used = int((sizes > 0).sum())
        fixed = max(1, used // 4)
        shifted = fixed + (places - fixed + offset_by * (used - fixed)) % max(1, count - fixed)
        return jnp.zeros((count,), jnp.int32).at[sequence[jnp.where(places < fixed, places, shifted)]].set(jnp.asarray(sizes, jnp.int32))

    sizes = jnp.where(number % 4 == 0, named(heavy_load, number // 4), named(usual, number - number // 4 - 1))
    mixed = jax.random.permutation(jax.random.fold_in(own, 3), count)
    donor, sink = mixed[0:count // 2 * 2:2], mixed[1:count // 2 * 2:2]
    margin = jnp.minimum(sizes[donor] - 1, reach - sizes[sink]) // 2
    margin = jnp.where((donor == sequence[0]) | (sink == sequence[0]) | (sizes[sink] == 0), 0, jnp.maximum(margin, 0))
    shifted = jax.random.randint(jax.random.fold_in(own, 4), (count // 2,), 0, 1 << 20) % (margin + 1)
    sizes = sizes.at[donor].add(-shifted).at[sink].add(shifted)
    items = jnp.searchsorted(jnp.cumsum(sizes), jnp.arange(rows * top), side="right").astype(jnp.int32)
    listing = items.reshape(top, rows).T
    listing = listing[jax.random.permutation(jax.random.fold_in(own, 1), rows)]
    offset_by = jax.random.randint(jax.random.fold_in(own, 2), (rows, 1), 0, top)
    return jnp.take_along_axis(listing, (jnp.arange(top)[None, :] + offset_by) % top, axis=1)


def load_shares(amount, total, reach, lean, full):
    loads = [(1 << 20) // math.isqrt(grade ** lean) + 1 for grade in range(1, amount + 1)]
    largest = reach if full else min(reach, max(-(-total // amount), total * loads[0] // sum(loads)))
    least = 1 if total - largest >= amount - 1 else 0
    counts, spare = [largest] + [least] * (amount - 1), total - largest - least * (amount - 1)
    while spare > 0:
        movable = [i for i in range(1, amount) if counts[i] < largest] or [i for i in range(1, amount) if counts[i] < reach]
        whole, budget = sum([loads[i] for i in movable]), spare
        for i in movable:
            extra = min(reach - counts[i], max(1, budget * loads[i] // whole), spare)
            counts[i] = counts[i] + extra
            spare = spare - extra
    return np.array(counts)


def normal_values(rng, extent, scale, most, pieces=(), held_as=jnp.bfloat16):
    factor_of = shard_levels(rng, extent, pieces, -0.22, 0.18) if pieces else 1.0
    result = jax.random.normal(rng, extent, jnp.float32) * scale * factor_of
    return jnp.minimum(jnp.maximum(result, -most), most).astype(held_as)


def setup_inputs(seed: int = 0, part: int = 0) -> dict:
    key_list = jax.random.split(jax.random.key(seed), 17)
    part_keys = jax.random.split(jax.random.fold_in(key_list[16], part), 17)
    queries = normal_values(part_keys[0], (SEQUENCE_LENGTH, RETENTION_HEADS * DK), 1.0, 6.0, ((0, 32), (1, 4)))
    keys = normal_values(part_keys[1], (SEQUENCE_LENGTH, RETENTION_HEADS * DK), 1.0, 6.0, ((0, 32), (1, 4)))
    values = normal_values(part_keys[2], (SEQUENCE_LENGTH, RETENTION_HEADS * DV), 1.0, 6.0, ((0, 32), (1, 4)))
    gate = normal_values(part_keys[3], (SEQUENCE_LENGTH, RETENTION_HEADS * DV), 1.0, 6.0, ((0, 32), (1, 4)))
    log_decay = draw_log_decay(jax.random.fold_in(jax.random.fold_in(key_list[16], part), 71), part)
    w_out = normal_values(key_list[5], (RETENTION_HEADS * DV, D), (RETENTION_HEADS * DV) ** -0.5, 0.1875, ((0, 4),))
    moe_input = draw_moe_input(jax.random.fold_in(jax.random.fold_in(key_list[16], part), 71), part)
    moe_gain = jnp.clip(1.0 + 0.18 * jax.random.normal(key_list[7], (D,), jnp.float32), 0.1, 1.9)
    routes_keys = jax.random.split(jax.random.fold_in(part_keys[8], 1), ROWS // TOK_DEV)
    routes_turns = jax.random.permutation(jax.random.fold_in(part_keys[8], 3), ROWS // TOK_DEV)
    routes = jax.vmap(lambda own, number: shared_out(jax.random.fold_in(part_keys[8], 2), own, number, TOK_DEV, EXPERTS, TOP, CAP, 1))(routes_keys, routes_turns).reshape((ROWS, TOP))
    route_weight = jnp.clip(0.1 + 0.9 * jax.random.uniform(part_keys[9], (ROWS, TOP), jnp.float32) ** shard_levels(part_keys[9], (ROWS, TOP), ((0, 128),), -0.2, 0.2), 0.1, 1.0)
    expert_gate = normal_values(key_list[10], (EXPERTS, D, FFE), D ** -0.5, 0.125, ((0, 128),))
    expert_up = normal_values(key_list[11], (EXPERTS, D, FFE), D ** -0.5, 0.125, ((0, 128),))
    expert_down = normal_values(key_list[12], (EXPERTS, FFE, D), FFE ** -0.5, 0.25, ((0, 128),))
    shared_gate = normal_values(key_list[13], (D, SH), D ** -0.5, 0.125, ((1, 4),))
    shared_up = normal_values(key_list[14], (D, SH), D ** -0.5, 0.125, ((1, 4),))
    shared_down = normal_values(key_list[15], (SH, D), SH ** -0.5, 0.25, ((0, 4),))
    return dict(queries=queries, keys=keys, values=values, gate=gate, log_decay=log_decay, w_out=w_out, moe_input=moe_input, moe_gain=moe_gain, routes=routes, route_weight=route_weight, expert_gate=expert_gate, expert_up=expert_up, expert_down=expert_down, shared_gate=shared_gate, shared_up=shared_up, shared_down=shared_down)


ROPE_BASE = 10000.0
GROUP_EPS = 1e-05
NORM_EPS = 1e-06

def rotate(tensor, offset):
    half_dim = tensor.shape[-1] // 2
    frequency = ROPE_BASE ** (-jnp.arange(half_dim, dtype=jnp.float32) / half_dim)
    places = (offset + jnp.arange(tensor.shape[0], dtype=jnp.int32)).astype(jnp.float32)
    angles = places[:, None] * frequency[None, :]
    cosine = jnp.cos(angles)[:, None, :]
    sine_part = jnp.sin(angles)[:, None, :]
    as_float = tensor.astype(jnp.float32)
    first_half = as_float[..., :half_dim]
    second_half = as_float[..., half_dim:]
    return jnp.concatenate([first_half * cosine - second_half * sine_part, first_half * sine_part + second_half * cosine], axis=-1)

def block_step(carry_state, inputs):
    q_block, k_block, v_block, decay_block = inputs
    block_len = decay_block.shape[0]
    running = jnp.cumsum(decay_block, axis=0)
    total_log = running[-1]
    lower_mask = jnp.arange(block_len)[:, None] >= jnp.arange(block_len)[None, :]
    log_gap = jnp.transpose(running)[:, :, None] - jnp.transpose(running)[:, None, :]
    scores = jnp.einsum('ihd,jhd->hij', q_block.astype(jnp.float32), k_block.astype(jnp.float32))
    weights = jnp.where(lower_mask[None], scores * jnp.exp(jnp.where(lower_mask[None], log_gap, 0.0)), 0.0)
    weights = weights.astype(jnp.bfloat16)
    inner_out = jnp.einsum('hij,jhe->ihe', weights.astype(jnp.float32), v_block.astype(jnp.float32))
    lifted = q_block.astype(jnp.float32) * jnp.exp(running)[:, :, None]
    carried = jnp.einsum('ihd,hde->ihe', lifted, carry_state, precision=lax.Precision.HIGHEST)
    key_tail = k_block.astype(jnp.float32) * jnp.exp(total_log[None, :] - running)[:, :, None]
    carry_state = carry_state * jnp.exp(total_log)[:, None, None] + jnp.einsum('jhd,jhe->hde', key_tail, v_block.astype(jnp.float32), precision=lax.Precision.HIGHEST)
    return (carry_state, inner_out + carried)

def round_trip(tensor):
    return lax.optimization_barrier(tensor.astype(jnp.bfloat16)).astype(jnp.float32)

def reference(queries, keys, values, gate, log_decay, w_out, moe_input, moe_gain, routes, route_weight, expert_gate, expert_up, expert_down, shared_gate, shared_up, shared_down):
    q_rot = rotate(queries.reshape(SEQUENCE_LENGTH, RETENTION_HEADS, DK), 0).astype(jnp.bfloat16)
    k_rot = (rotate(keys.reshape(SEQUENCE_LENGTH, RETENTION_HEADS, DK), 0) * DK ** (-0.5)).astype(jnp.bfloat16)
    v_heads = values.reshape(SEQUENCE_LENGTH, RETENTION_HEADS, DV)
    blocks = SEQUENCE_LENGTH // BLOCK

    def to_blocks(tensor):
        return tensor.reshape((blocks, BLOCK) + tensor.shape[1:])
    zero_state = jnp.zeros((RETENTION_HEADS, DK, DV), jnp.float32)
    _, retained = lax.scan(block_step, zero_state, (to_blocks(q_rot), to_blocks(k_rot), to_blocks(v_heads), to_blocks(log_decay)))
    retained = retained.reshape(SEQUENCE_LENGTH, RETENTION_HEADS, DV)
    center = lax.optimization_barrier(jnp.mean(retained, axis=-1, keepdims=True))
    spread = lax.optimization_barrier(jnp.mean(jnp.square(retained - center), axis=-1, keepdims=True))
    normed = (retained - center) * lax.rsqrt(spread + GROUP_EPS)
    gate_act = jax.nn.silu(gate.astype(jnp.float32)).reshape(SEQUENCE_LENGTH, RETENTION_HEADS, DV)
    gated_out = (gate_act * normed).astype(jnp.bfloat16).reshape(SEQUENCE_LENGTH, RETENTION_HEADS * DV)
    group_cols = RETENTION_HEADS * DV // N_TP
    mixer_sum = jnp.zeros((SEQUENCE_LENGTH, D), jnp.float32)
    for member in range(N_TP):
        partial_value = jnp.dot(gated_out[:, member * group_cols:(member + 1) * group_cols], w_out[member * group_cols:(member + 1) * group_cols], preferred_element_type=jnp.float32)
        mixer_sum = mixer_sum + round_trip(partial_value)
    mixer_out = mixer_sum.astype(jnp.bfloat16)
    as_float = moe_input.astype(jnp.float32)
    scale_row = lax.rsqrt(lax.optimization_barrier(jnp.mean(as_float * as_float, axis=-1, keepdims=True)) + NORM_EPS)
    normed_rows = (as_float * scale_row * moe_gain.astype(jnp.float32)[None, :]).astype(jnp.bfloat16)
    shared_hidden = (jax.nn.silu(jnp.dot(normed_rows, shared_gate, preferred_element_type=jnp.float32)) * jnp.dot(normed_rows, shared_up, preferred_element_type=jnp.float32)).astype(jnp.bfloat16)
    unit_cols = SH // N_TP
    shared_sum = jnp.zeros((ROWS, D), jnp.float32)
    for member in range(N_TP):
        partial_value = jnp.dot(shared_hidden[:, member * unit_cols:(member + 1) * unit_cols], shared_down[member * unit_cols:(member + 1) * unit_cols], preferred_element_type=jnp.float32)
        shared_sum = shared_sum + round_trip(partial_value)
    pairs = ROWS * TOP
    sources = ROWS // TOK_DEV
    chosen = routes.reshape(pairs).astype(jnp.int32)
    marked = (chosen[:, None] == jnp.arange(EXPERTS, dtype=jnp.int32)[None, :]).astype(jnp.int32)
    counted = jnp.cumsum(marked.reshape(sources, TOK_DEV * TOP, EXPERTS), axis=1).reshape(pairs, EXPERTS)
    slot_rank = lax.optimization_barrier(jnp.sum(counted * marked, axis=1)) - 1
    owners = jnp.arange(pairs, dtype=jnp.int32) // (TOK_DEV * TOP)
    slots = ((owners * EXPERTS + chosen) * CAP + slot_rank).astype(jnp.int32)
    row_table = jnp.full((sources * EXPERTS * CAP,), ROWS, jnp.int32).at[slots].set(jnp.arange(pairs, dtype=jnp.int32) // TOP)
    weight_table = jnp.zeros((sources * EXPERTS * CAP,), jnp.float32).at[slots].set(route_weight.reshape(pairs).astype(jnp.float32))
    row_table = jnp.transpose(row_table.reshape(sources, EXPERTS, CAP), (1, 0, 2)).reshape(EXPERTS, sources * CAP)
    weight_table = jnp.transpose(weight_table.reshape(sources, EXPERTS, CAP), (1, 0, 2)).reshape(EXPERTS, sources * CAP)
    padded = jnp.concatenate([normed_rows, jnp.zeros((1, D), jnp.bfloat16)], axis=0)

    def expert_step(totals, inputs):
        rows_used, row_weights, gate_w, up_w, down_w = inputs
        picked = padded[rows_used]
        hidden = (jax.nn.silu(jnp.dot(picked, gate_w, preferred_element_type=jnp.float32)) * jnp.dot(picked, up_w, preferred_element_type=jnp.float32)).astype(jnp.bfloat16)
        answer = round_trip(jnp.dot(hidden, down_w, preferred_element_type=jnp.float32))
        return (totals.at[rows_used].add(answer * row_weights[:, None]), None)
    totals, _ = lax.scan(expert_step, jnp.zeros((ROWS + 1, D), jnp.float32), (row_table, weight_table, expert_gate, expert_up, expert_down))
    moe_out = (shared_sum + totals[:ROWS]).astype(jnp.bfloat16)
    return (mixer_out, moe_out)
```

```python
import functools

import jax
import jax.numpy as jnp
from jax import lax
from jax.experimental import pallas as pl
from jax.experimental.pallas import tpu as pltpu
from jax.sharding import Mesh
from jax.sharding import PartitionSpec as P

BLOCK = 128
LANES = 128
TILE = 16
EP = ("ep_0", "ep_1")
EP_TP = ("ep_0", "ep_1", "tp")
GRP_EP = ("grp", "ep_0", "ep_1")
GRP_EP_TP = ("grp", "ep_0", "ep_1", "tp")
STATE_ROWS = 80

ROPE_BASE = 10000.0
GROUP_EPS = 1e-05
NORM_EPS = 1e-06


VMEM = pl.BlockSpec(memory_space=pltpu.VMEM)
SMEM = pl.BlockSpec(memory_space=pltpu.SMEM)
ANY = pl.BlockSpec(memory_space=pl.ANY)
F32 = jnp.float32
BF16 = jnp.bfloat16
MIB = 1 << 20


def call(kernel, name, out_shape, in_specs, out_specs, scratch, flops, moved, limit):
    return pl.pallas_call(
        kernel,
        name=name,
        out_shape=out_shape,
        in_specs=in_specs,
        out_specs=out_specs,
        scratch_shapes=scratch,
        compiler_params=pltpu.CompilerParams(vmem_limit_bytes=limit * MIB),
        cost_estimate=pl.CostEstimate(flops=flops, bytes_accessed=moved, transcendentals=0),
    )


def dot(a, b):
    return jnp.dot(a, b, preferred_element_type=F32)


def swap_matrix():
    side = TILE * TILE
    row = lax.broadcasted_iota(jnp.int32, (side, side), 0)
    col = lax.broadcasted_iota(jnp.int32, (side, side), 1)
    hit = (row // TILE == col % TILE) & (row % TILE == col // TILE)
    return jnp.where(hit, 1.0, 0.0).astype(BF16)


def rows_to_tiles(swap, rows):
    count = rows.shape[0] // TILE
    width = rows.shape[1] // LANES
    found = []
    for at in range(0, count, 2):
        pair = [
            jnp.concatenate(
                [
                    rows[g * TILE : (g + 1) * TILE, k * LANES : (k + 1) * LANES]
                    for k in range(width)
                ],
                axis=0,
            )
            for g in range(at, min(at + 2, count))
        ]
        out = dot(swap, jnp.concatenate(pair, axis=1)).astype(BF16)
        found += [out[:, g * LANES : (g + 1) * LANES] for g in range(len(pair))]
    return found


def prep_kernel(routes, x, gain, normed, outbound, places, tiles, used):
    source = x[...].astype(F32)
    scale = lax.rsqrt(jnp.mean(source * source, axis=-1, keepdims=True) + NORM_EPS)
    rows = (source * scale * gain[...]).astype(BF16)
    normed[...] = rows
    for g, tile in enumerate(rows_to_tiles(swap_matrix(), rows)):
        tiles[g * TILE * TILE : (g + 1) * TILE * TILE, :] = tile
    outbound[...] = jnp.zeros_like(outbound)
    top = routes.shape[0] // x.shape[0]
    experts = used.shape[0]
    capacity = outbound.shape[0] // (experts * TILE)

    @pl.loop(0, experts)
    def _(e):
        used[e] = 0

    @pl.loop(0, x.shape[0])
    def _(n):
        row = tiles[pl.ds(pl.multiple_of(n * TILE, TILE), TILE), :]
        for k in range(top):
            p = n * top + k
            e = routes[p]
            rank = used[e]
            used[e] = rank + 1
            place = e * capacity + rank
            places[p] = place
            outbound[pl.ds(pl.multiple_of(place * TILE, TILE), TILE), :] = row


def expert_kernel(arrived, gate_hbm, up_hbm, down_hbm, out, gate_w, up_w, down_w, rows, sems):
    copies = [
        pltpu.make_async_copy(src, dst, sems.at[i])
        for i, (src, dst) in enumerate(
            ((gate_hbm, gate_w), (up_hbm, up_w), (down_hbm, down_w))
        )
    ]
    for copy in copies:
        copy.start()
    swap = swap_matrix()
    side = TILE * TILE
    groups = arrived.shape[0] // side
    for at in range(0, groups, 2):
        pair = jnp.concatenate(
            [arrived[g * side : (g + 1) * side, :] for g in (at, at + 1)], axis=1
        )
        turned = dot(swap, pair).astype(BF16)
        for j in range(2):
            for k in range(TILE):
                rows[
                    (at + j) * TILE : (at + j + 1) * TILE, k * LANES : (k + 1) * LANES
                ] = turned[k * TILE : (k + 1) * TILE, j * LANES : (j + 1) * LANES]
    copies[0].wait()
    gated = jax.nn.silu(dot(rows[...], gate_w[...]))
    copies[1].wait()
    hidden = (gated * dot(rows[...], up_w[...])).astype(BF16)
    copies[2].wait()
    step = 8 * TILE
    for at in range(0, rows.shape[0], step):
        result = dot(hidden[at : at + step, :], down_w[...]).astype(BF16)
        for g, tile in enumerate(rows_to_tiles(swap, result)):
            out[at * TILE + g * side : at * TILE + (g + 1) * side, :] = tile


def turn_matrix():
    row = lax.broadcasted_iota(jnp.int32, (LANES, LANES), 0)
    col = lax.broadcasted_iota(jnp.int32, (LANES, LANES), 1)
    return row, col


def rotated(x, cosine, sine, half):
    row, col = turn_matrix()
    first = col % (2 * half) < half
    partner = jnp.where(first, col + half, col - half)
    turn = jnp.where(row == partner, jnp.where(first, -1.0, 1.0), 0.0).astype(BF16)
    return x.astype(F32) * cosine + dot(x, turn) * sine


def lower(size, strict=False):
    row = lax.broadcasted_iota(jnp.int32, (size, size), 0)
    col = lax.broadcasted_iota(jnp.int32, (size, size), 1)
    return row > col if strict else row >= col


def summed_f32(a, b, dims):
    return lax.dot_general(
        a, b, (dims, ((), ())), preferred_element_type=F32, precision=lax.Precision.HIGHEST
    )


def spread_heads(per_head, key_size):
    lane = lax.broadcasted_iota(jnp.int32, (per_head.shape[0], LANES), 1)
    out = per_head[:, 0:1]
    for h in range(1, per_head.shape[1]):
        out = jnp.where(lane >= h * key_size, per_head[:, h : h + 1], out)
    return out


def state_kernel(k, v, log_decay, cosine, sine, packed):
    heads = log_decay.shape[1]
    key_size = k.shape[1] // heads
    value_size = v.shape[1] // heads
    span = k.shape[0]
    k_rot = (rotated(k[...], cosine[...], sine[...], key_size // 2) * key_size ** (-0.5)).astype(
        BF16
    )
    above = jnp.where(lower(BLOCK, True), 1.0, 0.0)
    after = jnp.zeros((1, heads), F32)
    tails = [None] * (span // BLOCK)
    for b in reversed(range(span // BLOCK)):
        part = log_decay[b * BLOCK : (b + 1) * BLOCK, :]
        tails[b] = summed_f32(above, part, ((0,), (0,))) + after
        after = after + jnp.sum(part, axis=0, keepdims=True)
    tail = jnp.concatenate(tails, axis=0)
    faded = (k_rot.astype(F32) * jnp.exp(spread_heads(tail, key_size))).astype(BF16)
    state = dot(faded.T, v[...])
    for h in range(heads):
        packed[h * STATE_ROWS : h * STATE_ROWS + key_size, :] = state[
            h * key_size : (h + 1) * key_size, h * value_size : (h + 1) * value_size
        ].astype(BF16)
        whole = after[:, h : h + 1]
        high = whole.astype(BF16)
        low = (whole - high.astype(F32)).astype(BF16)
        pad = STATE_ROWS - key_size
        row = lax.broadcasted_iota(jnp.int32, (pad, LANES), 0)
        packed[h * STATE_ROWS + key_size : (h + 1) * STATE_ROWS, :] = jnp.where(
            row == 0, high.astype(F32), low.astype(F32)
        ).astype(BF16)


def retention_kernel(
    seat, q, k, v, gate, log_decay, cosine, sine, state_in, w_out, *rest
):
    outs, gated = rest[:-1], rest[-1]
    heads = log_decay.shape[1]
    key_size = q.shape[1] // heads
    value_size = v.shape[1] // heads
    span = q.shape[0]
    q_rot = rotated(q[...], cosine[...], sine[...], key_size // 2).astype(BF16)
    k_rot = (rotated(k[...], cosine[...], sine[...], key_size // 2) * key_size ** (-0.5)).astype(
        BF16
    )
    keep = lower(BLOCK)
    ones = jnp.where(keep, 1.0, 0.0)
    lane = lax.broadcasted_iota(jnp.int32, (BLOCK, LANES), 1)
    state = state_in[...]
    for b in range(span // BLOCK):
        at = slice(b * BLOCK, (b + 1) * BLOCK)
        part = log_decay[at, :]
        column = summed_f32(ones, part, ((1,), (0,)))
        across = summed_f32(part, ones, ((0,), (1,)))
        total = column[BLOCK - 1 : BLOCK, :]
        q_part = q_rot[at, :]
        k_part = k_rot[at, :]
        v_part = v[at, :]
        lifted = q_part.astype(F32) * jnp.exp(spread_heads(column, key_size))
        tail = jnp.exp(spread_heads(total - column, key_size))
        faded = (k_part.astype(F32) * tail).astype(BF16)
        held = state.astype(BF16)
        grown = dot(faded.T, v_part)
        fade = []
        for h in range(heads):
            mine = (lane >= h * key_size) & (lane < (h + 1) * key_size)
            q_head = jnp.where(mine, q_part.astype(F32), 0.0).astype(BF16)
            scores = lax.dot_general(
                q_head, k_part, (((1,), (1,)), ((), ())), preferred_element_type=F32
            )
            gap = jnp.where(keep, column[:, h : h + 1] - across[h : h + 1, :], 0.0)
            weights = jnp.where(keep, scores * jnp.exp(gap), 0.0).astype(BF16)
            columns = slice(h * value_size, (h + 1) * value_size)
            kept = dot(weights, v_part[:, columns]) + dot(
                jnp.where(mine, lifted, 0.0).astype(BF16), held
            )
            center = jnp.mean(kept, axis=-1, keepdims=True)
            off = kept - center
            spread = jnp.mean(off * off, axis=-1, keepdims=True)
            act = jax.nn.silu(gate[at, columns].astype(F32))
            gated[at, columns] = (act * (off * lax.rsqrt(spread + GROUP_EPS))).astype(BF16)
            fade.append(
                state[h * key_size : (h + 1) * key_size, :] * jnp.exp(total[:, h : h + 1])
                + grown[h * key_size : (h + 1) * key_size, columns]
            )
        state = jnp.concatenate(fade, axis=0)
    count = len(outs)
    share = span // count
    for d in range(count):
        first = lax.rem(seat[0] + d, count) * share
        outs[d][...] = dot(
            gated[pl.ds(pl.multiple_of(first, share), share), :], w_out[...]
        ).astype(BF16)


def shared_kernel(*refs):
    count = (len(refs) - 3) // 2
    pieces = refs[:count]
    gate_w, up_w, down_w = refs[count : count + 3]
    for rows, out in zip(pieces, refs[count + 3 :]):
        hidden = jax.nn.silu(dot(rows[...], gate_w[...])) * dot(rows[...], up_w[...])
        out[...] = dot(hidden.astype(BF16), down_w[...]).astype(BF16)


def combine_kernel(places, returned, weight, *refs):
    count = (len(refs) - 4) // 2
    mixed, shared = refs[:count], refs[count : 2 * count]
    mixer_out, moe_out, picked, rows = refs[2 * count :]
    total = mixed[0][...].astype(F32)
    for part in mixed[1:]:
        total = total + part[...].astype(F32)
    mixer_out[...] = total.astype(BF16)
    swap = swap_matrix()
    side = TILE * TILE
    number = moe_out.shape[0]
    top = weight.shape[1]
    for k in range(top):

        @pl.loop(0, number)
        def _(n):
            place = places[n * top + k]
            picked[pl.ds(pl.multiple_of(n * TILE, TILE), TILE), :] = returned[
                pl.ds(pl.multiple_of(place * TILE, TILE), TILE), :
            ]

        for at in range(0, number // TILE, 2):
            pair = jnp.concatenate(
                [picked[g * side : (g + 1) * side, :] for g in (at, at + 1)], axis=1
            )
            turned = dot(swap, pair).astype(BF16)
            for j in range(2):
                for c in range(TILE):
                    rows[
                        k,
                        (at + j) * TILE : (at + j + 1) * TILE,
                        c * LANES : (c + 1) * LANES,
                    ] = turned[c * TILE : (c + 1) * TILE, j * LANES : (j + 1) * LANES]
    total = shared[0][...].astype(F32)
    for part in shared[1:]:
        total = total + part[...].astype(F32)
    for k in range(top):
        total = total + rows[k].astype(F32) * weight[:, k : k + 1]
    moe_out[...] = total.astype(BF16)


def moved_by(array, axis, step, around=True):
    count = lax.axis_size(axis)
    pairs = [
        (s, (s + step) % count) for s in range(count) if around or 0 <= s + step < count
    ]
    return lax.ppermute(array, axis, pairs)


def unpacked(packed, key_size):
    wide = packed.astype(F32)
    return wide[key_size, 0] + wide[key_size + 1, 0], wide[:key_size]


def repacked(part, key_size):
    log, state = part
    high = log.astype(BF16).astype(F32)
    low = log - high
    row = lax.broadcasted_iota(jnp.int32, (STATE_ROWS - key_size, state.shape[1]), 0)
    return jnp.concatenate([state, jnp.where(row == 0, high, low)], axis=0).astype(BF16)


def joined(earlier, later):
    return earlier[0] + later[0], earlier[1] * jnp.exp(later[0]) + later[1]


def entering(packed, heads, key_size):
    core = lax.axis_index("ep_1")
    other = moved_by(packed, "ep_1", 1)
    halves = packed.reshape(heads, STATE_ROWS, -1)
    others = other.reshape(heads, STATE_ROWS, -1)
    mine = lax.dynamic_index_in_dim(halves, core, 0, False)
    theirs = lax.dynamic_index_in_dim(others, core, 0, False)
    early = jnp.where(core == 0, mine, theirs)
    late = jnp.where(core == 0, theirs, mine)
    chip = joined(unpacked(early, key_size), unpacked(late, key_size))
    sent = repacked(chip, key_size)
    near = [unpacked(moved_by(sent, "ep_0", d, False), key_size) for d in (3, 2, 1)]
    before = joined(joined(near[0], near[1]), near[2])
    window = repacked(joined(before, chip), key_size)
    return others, before, window


def entering_end(others, before, window, key_size):
    core = lax.axis_index("ep_1")
    far = [unpacked(moved_by(window, "ep_0", d, False), key_size) for d in (12, 8, 4)]
    prefix = joined(joined(joined(far[0], far[1]), far[2]), before)
    sent = repacked(prefix, key_size)
    swapped = moved_by(sent, "ep_1", 1)
    found = []
    for h in range(others.shape[0]):
        chip_before = unpacked(jnp.where(core == h, sent, swapped), key_size)
        with_first = joined(chip_before, unpacked(others[h], key_size))
        found.append(jnp.where(core == 0, chip_before[1], with_first[1]))
    return jnp.concatenate(found, axis=0)


def per_device(
    queries,
    keys,
    values,
    gate,
    log_decay,
    w_out,
    moe_input,
    moe_gain,
    routes,
    route_weight,
    expert_gate,
    expert_up,
    expert_down,
    shared_gate,
    shared_up,
    shared_down,
):
    span = queries.shape[0]
    heads = log_decay.shape[1]
    key_size = queries.shape[1] // heads
    value_size = values.shape[1] // heads
    rows_dev, width = moe_input.shape
    top = routes.shape[1]
    n_tp = lax.axis_size("tp")
    experts = lax.axis_size(EP) * n_tp
    capacity = rows_dev * top * 3 // (2 * experts)
    hidden_size = expert_gate.shape[2]
    shared_size = shared_gate.shape[1]
    slots = experts * capacity
    tile_rows = slots * TILE

    normed, outbound, places = call(
        prep_kernel,
        "prep",
        (
            jax.ShapeDtypeStruct((rows_dev, width), BF16),
            jax.ShapeDtypeStruct((tile_rows, LANES), BF16),
            jax.ShapeDtypeStruct((rows_dev * top,), jnp.int32),
        ),
        [SMEM, VMEM, VMEM],
        (VMEM, VMEM, SMEM),
        [pltpu.VMEM((rows_dev * TILE, LANES), BF16), pltpu.SMEM((experts,), jnp.int32)],
        2 * rows_dev * width * 256,
        4 * rows_dev * width,
        16,
    )(routes.reshape(-1), moe_input, moe_gain.reshape(1, width))

    arrived = lax.all_to_all(
        outbound.reshape(experts, capacity * TILE, LANES),
        EP_TP,
        split_axis=0,
        concat_axis=0,
        tiled=True,
    )

    half = key_size // 2
    frequency = ROPE_BASE ** (-jnp.arange(half, dtype=F32) / half)
    spots = lax.axis_index(EP) * span + jnp.arange(span, dtype=jnp.int32)
    angles = spots.astype(F32)[:, None] * jnp.tile(frequency, LANES // half)[None, :]
    cosine = jnp.cos(angles)
    sine = jnp.sin(angles)

    packed = call(
        state_kernel,
        "state",
        jax.ShapeDtypeStruct((heads * STATE_ROWS, value_size), BF16),
        [VMEM] * 5,
        VMEM,
        [],
        2 * span * LANES * 512,
        4 * span * LANES * 4,
        12,
    )(keys, values, log_decay, cosine, sine)
    others, before, window = entering(packed, heads, key_size)

    pieces = [normed] + [moved_by(normed, "tp", d) for d in range(1, n_tp)]
    shared_parts = call(
        shared_kernel,
        "shared",
        tuple(jax.ShapeDtypeStruct((rows_dev, width), BF16) for _ in range(n_tp)),
        [VMEM] * (n_tp + 3),
        (VMEM,) * n_tp,
        [],
        2 * n_tp * rows_dev * width * shared_size * 3,
        10 * rows_dev * width * 2,
        16,
    )(*pieces, shared_gate, shared_up, shared_down)
    shared_parts = [shared_parts[0]] + [
        moved_by(shared_parts[d], "tp", -d) for d in range(1, n_tp)
    ]

    arrived, window = lax.optimization_barrier((arrived, window))
    answers = call(
        expert_kernel,
        "expert",
        jax.ShapeDtypeStruct((tile_rows, LANES), BF16),
        [VMEM, ANY, ANY, ANY],
        VMEM,
        [
            pltpu.VMEM((width, hidden_size), BF16),
            pltpu.VMEM((width, hidden_size), BF16),
            pltpu.VMEM((hidden_size, width), BF16),
            pltpu.VMEM((slots, width), BF16),
            pltpu.SemaphoreType.DMA((3,)),
        ],
        2 * slots * width * hidden_size * 3,
        3 * 2 * width * hidden_size,
        28,
    )(arrived.reshape(tile_rows, LANES), expert_gate[0], expert_up[0], expert_down[0])
    returned = lax.all_to_all(
        answers.reshape(experts, capacity * TILE, LANES),
        EP_TP,
        split_axis=0,
        concat_axis=0,
        tiled=True,
    )

    state_in = entering_end(others, before, window, key_size)
    mixed_parts = call(
        retention_kernel,
        "retention",
        tuple(jax.ShapeDtypeStruct((rows_dev, width), BF16) for _ in range(n_tp)),
        [SMEM] + [VMEM] * 9,
        (VMEM,) * n_tp,
        [pltpu.VMEM((span, heads * value_size), BF16)],
        2 * span * width * heads * value_size * 4,
        10 * rows_dev * width * 2,
        20,
    )(
        lax.axis_index("tp").reshape(1).astype(jnp.int32),
        queries,
        keys,
        values,
        gate,
        log_decay,
        cosine,
        sine,
        state_in,
        w_out,
    )
    mixed_parts = [mixed_parts[0]] + [moved_by(mixed_parts[d], "tp", d) for d in range(1, n_tp)]

    return call(
        combine_kernel,
        "combine",
        tuple(jax.ShapeDtypeStruct((rows_dev, width), BF16) for _ in range(2)),
        [SMEM] + [VMEM] * (2 + 2 * n_tp),
        (VMEM,) * 2,
        [
            pltpu.VMEM((rows_dev * TILE, LANES), BF16),
            pltpu.VMEM((top, rows_dev, width), BF16),
        ],
        2 * rows_dev * width * 512,
        10 * rows_dev * width * 2,
        20,
    )(places, returned.reshape(tile_rows, LANES), route_weight, *mixed_parts, *shared_parts)


def solution(mesh):
    split = Mesh(
        mesh.devices.reshape(mesh.shape["grp"], mesh.shape["ep"] // 2, 2, mesh.shape["tp"]),
        ("grp", "ep_0", "ep_1", "tp"),
    )
    return jax.shard_map(
        per_device,
        mesh=split,
        in_specs=(
            P(GRP_EP, "tp"),
            P(GRP_EP, "tp"),
            P(GRP_EP, "tp"),
            P(GRP_EP, "tp"),
            P(GRP_EP, "tp"),
            P("tp", None),
            P(GRP_EP_TP, None),
            P(),
            P(GRP_EP_TP, None),
            P(GRP_EP_TP, None),
            P(EP_TP, None, None),
            P(EP_TP, None, None),
            P(EP_TP, None, None),
            P(None, "tp"),
            P(None, "tp"),
            P("tp", None),
        ),
        out_specs=(P(GRP_EP_TP, None), P(GRP_EP_TP, None)),
        check_vma=False,
    )
```

```python
import jax
import jax.numpy as jnp
from jax import lax
from jax.experimental import pallas as pl
from jax.experimental.pallas import tpu as pltpu
from jax.sharding import Mesh
from jax.sharding import PartitionSpec as P


BLOCK = 128
LANES = 128
TILE = 16
EP = ("ep_0", "ep_1")
EP_TP = ("ep_0", "ep_1", "tp")
GRP_EP = ("grp", "ep_0", "ep_1")
GRP_EP_TP = ("grp", "ep_0", "ep_1", "tp")
STATE_ROWS = 80

ROPE_BASE = 10000.0
GROUP_EPS = 1e-05
NORM_EPS = 1e-06


VMEM = pl.BlockSpec(memory_space=pltpu.VMEM)
SMEM = pl.BlockSpec(memory_space=pltpu.SMEM)
HBM = pl.BlockSpec(memory_space=pltpu.HBM)
F32 = jnp.float32
BF16 = jnp.bfloat16
MIB = 1 << 20


def call(kernel, out_shape, in_specs, out_specs, scratch, flops, moved, limit):
    return pl.pallas_call(
        kernel,
        out_shape=out_shape,
        in_specs=in_specs,
        out_specs=out_specs,
        scratch_shapes=scratch,
        compiler_params=pltpu.CompilerParams(vmem_limit_bytes=limit * MIB),
        cost_estimate=pl.CostEstimate(flops=flops, bytes_accessed=moved, transcendentals=0),
    )


def dot(a, b):
    return jnp.dot(a, b, preferred_element_type=F32)


def swap_matrix():
    side = TILE * TILE
    row = lax.broadcasted_iota(jnp.int32, (side, side), 0)
    col = lax.broadcasted_iota(jnp.int32, (side, side), 1)
    hit = (row // TILE == col % TILE) & (row % TILE == col // TILE)
    return jnp.where(hit, 1.0, 0.0).astype(BF16)


def rows_to_tiles(swap, rows):
    count = rows.shape[0] // TILE
    width = rows.shape[1] // LANES
    found = []
    for at in range(0, count, 2):
        pair = [
            jnp.concatenate(
                [
                    rows[g * TILE : (g + 1) * TILE, k * LANES : (k + 1) * LANES]
                    for k in range(width)
                ],
                axis=0,
            )
            for g in range(at, min(at + 2, count))
        ]
        out = dot(swap, jnp.concatenate(pair, axis=1)).astype(BF16)
        found += [out[:, g * LANES : (g + 1) * LANES] for g in range(len(pair))]
    return found


def prep_kernel(
    routes, x_hbm, gain_hbm, normed_hbm, outbound, places, x, gain, normed, tiles, used, sems
):
    copies = [
        pltpu.make_async_copy(x_hbm, x, sems.at[0]),
        pltpu.make_async_copy(gain_hbm, gain, sems.at[1]),
    ]
    for copy in copies:
        copy.start()
    outbound[...] = jnp.zeros_like(outbound)
    top = routes.shape[0] // x.shape[0]
    experts = used.shape[0]
    capacity = outbound.shape[0] // (experts * TILE)
    for e in range(experts):
        used[e] = 0
    for copy in copies:
        copy.wait()
    source = x[...].astype(F32)
    scale = lax.rsqrt(jnp.mean(source * source, axis=-1, keepdims=True) + NORM_EPS)
    rows = (source * scale * gain[...]).astype(BF16)
    normed[...] = rows
    keep = pltpu.make_async_copy(normed, normed_hbm, sems.at[2])
    keep.start()
    for g, tile in enumerate(rows_to_tiles(swap_matrix(), rows)):
        tiles[g * TILE * TILE : (g + 1) * TILE * TILE, :] = tile

    @pl.loop(0, x.shape[0], unroll=4)
    def _(n):
        row = tiles[pl.ds(pl.multiple_of(n * TILE, TILE), TILE), :]
        for k in range(top):
            p = n * top + k
            e = routes[p]
            rank = used[e]
            used[e] = rank + 1
            place = e * capacity + rank
            places[p] = place
            outbound[pl.ds(pl.multiple_of(place * TILE, TILE), TILE), :] = row

    keep.wait()


def expert_kernel(
    arrived_hbm,
    gate_hbm,
    up_hbm,
    down_hbm,
    out_hbm,
    gate_w,
    up_w,
    down_w,
    rows,
    arrived,
    out,
    sems,
    in_sems,
    out_sems,
):
    pieces = sems.shape[1]
    chunks = out_sems.shape[0]
    share = arrived.shape[0] // chunks
    landed = []
    for j in range(chunks):
        at = pl.ds(j * share, share)
        landed.append(pltpu.make_async_copy(arrived_hbm.at[at], arrived.at[at], in_sems.at[j]))
        landed[-1].start()
    copies = [[], [], []]
    for i, (src, dst) in enumerate(((gate_hbm, gate_w), (up_hbm, up_w), (down_hbm, down_w))):
        part = dst.shape[0] // pieces
        for j in range(pieces):
            at = pl.ds(j * part, part)
            copies[i].append(pltpu.make_async_copy(src.at[0, at], dst.at[at], sems.at[i, j]))
            copies[i][-1].start()
    swap = swap_matrix()
    side = TILE * TILE
    groups = arrived.shape[0] // side
    for at in range(0, groups, 2):
        if at * side % share == 0:
            landed[at * side // share].wait()
        pair = jnp.concatenate(
            [arrived[g * side : (g + 1) * side, :] for g in (at, at + 1)], axis=1
        )
        turned = dot(swap, pair).astype(BF16)
        for j in range(2):
            for k in range(TILE):
                rows[
                    (at + j) * TILE : (at + j + 1) * TILE, k * LANES : (k + 1) * LANES
                ] = turned[k * TILE : (k + 1) * TILE, j * LANES : (j + 1) * LANES]
    for copy in copies[0]:
        copy.wait()
    gated = jax.nn.silu(dot(rows[...], gate_w[...]))
    for copy in copies[1]:
        copy.wait()
    hidden = (gated * dot(rows[...], up_w[...])).astype(BF16)
    for copy in copies[2]:
        copy.wait()
    left = []
    step = rows.shape[0] // chunks
    for j in range(chunks):
        result = dot(hidden[j * step : (j + 1) * step, :], down_w[...]).astype(BF16)
        for g, tile in enumerate(rows_to_tiles(swap, result)):
            out[j * share + g * side : j * share + (g + 1) * side, :] = tile
        at = pl.ds(j * share, share)
        left.append(pltpu.make_async_copy(out.at[at], out_hbm.at[at], out_sems.at[j]))
        left[-1].start()
    for copy in left:
        copy.wait()


def turn_matrix():
    row = lax.broadcasted_iota(jnp.int32, (LANES, LANES), 0)
    col = lax.broadcasted_iota(jnp.int32, (LANES, LANES), 1)
    return row, col


def rotated(x, cosine, sine, half):
    row, col = turn_matrix()
    first = col % (2 * half) < half
    partner = jnp.where(first, col + half, col - half)
    turn = jnp.where(row == partner, jnp.where(first, -1.0, 1.0), 0.0).astype(BF16)
    return x.astype(F32) * cosine + dot(x, turn) * sine


def lower(size, strict=False):
    row = lax.broadcasted_iota(jnp.int32, (size, size), 0)
    col = lax.broadcasted_iota(jnp.int32, (size, size), 1)
    return row > col if strict else row >= col


def summed_f32(a, b, dims):
    return lax.dot_general(
        a, b, (dims, ((), ())), preferred_element_type=F32, precision=lax.Precision.HIGHEST
    )


def spread_heads(per_head, key_size):
    lane = lax.broadcasted_iota(jnp.int32, (per_head.shape[0], LANES), 1)
    out = per_head[:, 0:1]
    for h in range(1, per_head.shape[1]):
        out = jnp.where(lane >= h * key_size, per_head[:, h : h + 1], out)
    return out


def state_kernel(k, v, log_decay, cosine, sine, packed):
    heads = log_decay.shape[1]
    key_size = k.shape[1] // heads
    value_size = v.shape[1] // heads
    span = k.shape[0]
    k_rot = (rotated(k[...], cosine[...], sine[...], key_size // 2) * key_size ** (-0.5)).astype(
        BF16
    )
    above = jnp.where(lower(BLOCK, True), 1.0, 0.0)
    after = jnp.zeros((1, heads), F32)
    tails = [None] * (span // BLOCK)
    for b in reversed(range(span // BLOCK)):
        part = log_decay[b * BLOCK : (b + 1) * BLOCK, :]
        tails[b] = summed_f32(above, part, ((0,), (0,))) + after
        after = after + jnp.sum(part, axis=0, keepdims=True)
    tail = jnp.concatenate(tails, axis=0)
    faded = (k_rot.astype(F32) * jnp.exp(spread_heads(tail, key_size))).astype(BF16)
    state = dot(faded.T, v[...])
    for h in range(heads):
        packed[h * STATE_ROWS : h * STATE_ROWS + key_size, :] = state[
            h * key_size : (h + 1) * key_size, h * value_size : (h + 1) * value_size
        ].astype(BF16)
        whole = after[:, h : h + 1]
        high = whole.astype(BF16)
        low = (whole - high.astype(F32)).astype(BF16)
        pad = STATE_ROWS - key_size
        row = lax.broadcasted_iota(jnp.int32, (pad, LANES), 0)
        packed[h * STATE_ROWS + key_size : (h + 1) * STATE_ROWS, :] = jnp.where(
            row == 0, high.astype(F32), low.astype(F32)
        ).astype(BF16)


def retention_kernel(seat, q, k, v, gate, log_decay, cosine, sine, state_in, *rest):
    outs, gated = rest[:-1], rest[-1]
    heads = log_decay.shape[1]
    key_size = q.shape[1] // heads
    value_size = v.shape[1] // heads
    span = q.shape[0]
    q_rot = rotated(q[...], cosine[...], sine[...], key_size // 2).astype(BF16)
    k_rot = (rotated(k[...], cosine[...], sine[...], key_size // 2) * key_size ** (-0.5)).astype(
        BF16
    )
    keep = lower(BLOCK)
    ones = jnp.where(keep, 1.0, 0.0)
    lane = lax.broadcasted_iota(jnp.int32, (BLOCK, LANES), 1)
    state = state_in[...]
    for b in range(span // BLOCK):
        at = slice(b * BLOCK, (b + 1) * BLOCK)
        part = log_decay[at, :]
        column = summed_f32(ones, part, ((1,), (0,)))
        across = summed_f32(part, ones, ((0,), (1,)))
        total = column[BLOCK - 1 : BLOCK, :]
        q_part = q_rot[at, :]
        k_part = k_rot[at, :]
        v_part = v[at, :]
        lifted = q_part.astype(F32) * jnp.exp(spread_heads(column, key_size))
        tail = jnp.exp(spread_heads(total - column, key_size))
        faded = (k_part.astype(F32) * tail).astype(BF16)
        held = state.astype(BF16)
        grown = dot(faded.T, v_part)
        fade = []
        for h in range(heads):
            mine = (lane >= h * key_size) & (lane < (h + 1) * key_size)
            q_head = jnp.where(mine, q_part.astype(F32), 0.0).astype(BF16)
            scores = lax.dot_general(
                q_head, k_part, (((1,), (1,)), ((), ())), preferred_element_type=F32
            )
            gap = jnp.where(keep, column[:, h : h + 1] - across[h : h + 1, :], 0.0)
            weights = jnp.where(keep, scores * jnp.exp(gap), 0.0).astype(BF16)
            columns = slice(h * value_size, (h + 1) * value_size)
            kept = dot(weights, v_part[:, columns]) + dot(
                jnp.where(mine, lifted, 0.0).astype(BF16), held
            )
            center = jnp.mean(kept, axis=-1, keepdims=True)
            off = kept - center
            spread = jnp.mean(off * off, axis=-1, keepdims=True)
            act = jax.nn.silu(gate[at, columns].astype(F32))
            gated[at, columns] = (act * (off * lax.rsqrt(spread + GROUP_EPS))).astype(BF16)
            fade.append(
                state[h * key_size : (h + 1) * key_size, :] * jnp.exp(total[:, h : h + 1])
                + grown[h * key_size : (h + 1) * key_size, columns]
            )
        state = jnp.concatenate(fade, axis=0)
    count = len(outs)
    share = span // count
    for d in range(count):
        first = lax.rem(seat[0] + d, count) * share
        outs[d][...] = gated[pl.ds(pl.multiple_of(first, share), share), :]


def pack_kernel(core, gate_w, up_w, down_w, out):
    half = gate_w.shape[0] // 2
    first = pl.multiple_of(core[0] * half, TILE)
    out[0:half, :] = gate_w[pl.ds(first, half), :]
    out[half : 2 * half, :] = up_w[pl.ds(first, half), :]
    part = down_w.shape[0] // 2
    first = pl.multiple_of(core[0] * part, TILE)
    for k in range(down_w.shape[1] // LANES):
        at = 2 * half + k * part
        out[at : at + part, :] = down_w[pl.ds(first, part), k * LANES : (k + 1) * LANES]


def shared_kernel(core, normed, gate_w, up_w, down_w, *refs):
    count = (len(refs) - 3) // 2
    mine, theirs = refs[:count], refs[count : 2 * count]
    out, packed, down = refs[2 * count :]
    rows = normed[...]
    half = rows.shape[1] // 2
    part = down.shape[0] // 2
    hidden = jax.nn.silu(dot(rows, gate_w[...])) * dot(rows, up_w[...])
    total = dot(hidden.astype(BF16), down_w[...])
    for a, b in zip(mine, theirs):
        packed[0] = jnp.where(core[0] == 0, a[...], b[...])
        packed[1] = jnp.where(core[0] == 0, b[...], a[...])
        gated = dot(rows[:, :half], packed[0, :half]) + dot(rows[:, half:], packed[1, :half])
        up = dot(rows[:, :half], packed[0, half : 2 * half]) + dot(
            rows[:, half:], packed[1, half : 2 * half]
        )
        for c in range(2):
            for k in range(down.shape[1] // LANES):
                at = 2 * half + k * part
                down[c * part : (c + 1) * part, k * LANES : (k + 1) * LANES] = packed[
                    c, at : at + part
                ]
        hidden = (jax.nn.silu(gated) * up).astype(BF16)
        total = total + dot(hidden, down[...])
    out[...] = total


def finish_kernel(places, core, weight, *refs):
    count = (len(refs) - 11) // 3
    gated = refs[:count]
    hbm = refs[count : 3 * count + 1]
    mixer_out, moe_out, picked, rows, returned, shared, own, mine, theirs, sems = refs[
        3 * count + 1 :
    ]
    places_of = [returned, shared, own]
    places_of += [mine.at[d] for d in range(count - 1)] + [theirs.at[d] for d in range(count - 1)]
    copies = [
        pltpu.make_async_copy(a, b, sems.at[i]) for i, (a, b) in enumerate(zip(hbm, places_of))
    ]
    for copy in copies:
        copy.start()
    swap = swap_matrix()
    side = TILE * TILE
    number = moe_out.shape[0]
    top = weight.shape[1]
    copies[0].wait()

    @pl.loop(0, number, unroll=4)
    def _(n):
        for k in range(top):
            place = places[n * top + k]
            picked[k, pl.ds(pl.multiple_of(n * TILE, TILE), TILE), :] = returned[
                pl.ds(pl.multiple_of(place * TILE, TILE), TILE), :
            ]

    for k in range(top):
        for at in range(0, number // TILE, 2):
            pair = jnp.concatenate(
                [picked[k, g * side : (g + 1) * side, :] for g in (at, at + 1)], axis=1
            )
            turned = dot(swap, pair).astype(BF16)
            for j in range(2):
                for c in range(TILE):
                    rows[
                        k,
                        (at + j) * TILE : (at + j + 1) * TILE,
                        c * LANES : (c + 1) * LANES,
                    ] = turned[c * TILE : (c + 1) * TILE, j * LANES : (j + 1) * LANES]
    for copy in copies[1:]:
        copy.wait()
    total = shared[...]
    for k in range(top):
        total = total + rows[k].astype(F32) * weight[:, k : k + 1]
    moe_out[...] = total.astype(BF16)
    mixed = dot(gated[0][...], own[...])
    half = own.shape[0] // 2
    for d in range(count - 1):
        low, high = gated[d + 1][:, :half], gated[d + 1][:, half:]
        mixed = mixed + dot(jnp.where(core[0] == 0, low, high), mine[d])
        mixed = mixed + dot(jnp.where(core[0] == 0, high, low), theirs[d])
    mixer_out[...] = mixed.astype(BF16)


def moved_by(array, axis, step, around=True):
    count = lax.axis_size(axis)
    pairs = [
        (s, (s + step) % count) for s in range(count) if around or 0 <= s + step < count
    ]
    return lax.ppermute(array, axis, pairs)


def opened(packed):
    wide = packed.astype(F32)
    size = STATE_ROWS - TILE
    return wide[size : size + 1, :] + wide[size + 1 : size + 2, :], wide[:size, :]


def closed(part):
    log, state = part
    high = log.astype(BF16).astype(F32)
    row = lax.broadcasted_iota(jnp.int32, (TILE, LANES), 0)
    return jnp.concatenate([state, jnp.where(row == 0, high, log - high)], axis=0).astype(BF16)


def joined(earlier, later):
    return earlier[0] + later[0], earlier[1] * jnp.exp(later[0]) + later[1]


def picked_by(core, a, b):
    return jnp.where(core == 0, a.astype(F32), b.astype(F32)).astype(BF16)


def chip_kernel(core, own, other, out):
    mine = picked_by(core[0], own[:STATE_ROWS, :], own[STATE_ROWS:, :])
    theirs = picked_by(core[0], other[:STATE_ROWS, :], other[STATE_ROWS:, :])
    early, late = picked_by(core[0], mine, theirs), picked_by(core[0], theirs, mine)
    out[...] = closed(joined(opened(early), opened(late)))


def near_kernel(chip, far3, far2, far1, before, window):
    start = joined(joined(opened(far3[...]), opened(far2[...])), opened(far1[...]))
    before[...] = closed(start)
    window[...] = closed(joined(start, opened(chip[...])))


def far_kernel(before, far12, far8, far4, prefix):
    start = joined(joined(opened(far12[...]), opened(far8[...])), opened(far4[...]))
    prefix[...] = closed(joined(start, opened(before[...])))


def enter_kernel(core, mine, theirs, other, state):
    size = STATE_ROWS - TILE
    for h in range(other.shape[0] // STATE_ROWS):
        held = jnp.where(core[0] == h, mine[...].astype(F32), theirs[...].astype(F32))
        chip_before = opened(held)
        first = opened(other[h * STATE_ROWS : (h + 1) * STATE_ROWS, :])
        both = joined(chip_before, first)
        state[h * size : (h + 1) * size, :] = jnp.where(core[0] == 0, chip_before[1], both[1])


def small(kernel, outs, in_specs, out_specs):
    return call(kernel, outs, in_specs, out_specs, [], 100000, 100000, 2)


def per_device(
    queries,
    keys,
    values,
    gate,
    log_decay,
    w_out,
    moe_input,
    moe_gain,
    routes,
    route_weight,
    expert_gate,
    expert_up,
    expert_down,
    shared_gate,
    shared_up,
    shared_down,
):
    span = queries.shape[0]
    heads = log_decay.shape[1]
    key_size = queries.shape[1] // heads
    value_size = values.shape[1] // heads
    rows_dev, width = moe_input.shape
    top = routes.shape[1]
    n_tp = lax.axis_size("tp")
    experts = lax.axis_size(EP) * n_tp
    capacity = rows_dev * top * 3 // (2 * experts)
    hidden_size = expert_gate.shape[2]
    shared_size = shared_gate.shape[1]
    slots = experts * capacity
    tile_rows = slots * TILE

    core = lax.axis_index("ep_1").reshape(1).astype(jnp.int32)
    seat = lax.axis_index("tp").reshape(1).astype(jnp.int32)
    around = range(1, n_tp)
    half_out = w_out.shape[0] // 2
    packed_shape = jax.ShapeDtypeStruct((STATE_ROWS, value_size), BF16)

    out_half = lax.dynamic_slice_in_dim(w_out, core[0] * half_out, half_out, 0)
    out_mine = [moved_by(out_half, "tp", d) for d in around]

    normed, outbound, places = call(
        prep_kernel,
        (
            jax.ShapeDtypeStruct((rows_dev, width), BF16),
            jax.ShapeDtypeStruct((tile_rows, LANES), BF16),
            jax.ShapeDtypeStruct((rows_dev * top,), jnp.int32),
        ),
        [SMEM, HBM, HBM],
        (HBM, VMEM, SMEM),
        [
            pltpu.VMEM((rows_dev, width), BF16),
            pltpu.VMEM((1, width), F32),
            pltpu.VMEM((rows_dev, width), BF16),
            pltpu.VMEM((rows_dev * TILE, LANES), BF16),
            pltpu.SMEM((experts,), jnp.int32),
            pltpu.SemaphoreType.DMA((3,)),
        ],
        2 * rows_dev * width * 256,
        4 * rows_dev * width,
        62,
    )(routes.reshape(-1), moe_input, moe_gain.reshape(1, width))

    arrived = lax.all_to_all(
        outbound.reshape(experts, capacity * TILE, LANES),
        EP_TP,
        split_axis=0,
        concat_axis=0,
        tiled=True,
    )

    half = key_size // 2
    frequency = ROPE_BASE ** (-jnp.arange(half, dtype=F32) / half)
    spots = lax.axis_index(EP) * span + jnp.arange(span, dtype=jnp.int32)
    angles = spots.astype(F32)[:, None] * jnp.tile(frequency, LANES // half)[None, :]
    cosine = jnp.cos(angles)
    sine = jnp.sin(angles)

    own = call(
        state_kernel,
        jax.ShapeDtypeStruct((heads * STATE_ROWS, value_size), BF16),
        [VMEM] * 5,
        VMEM,
        [],
        2 * span * LANES * 512,
        4 * span * LANES * 4,
        12,
    )(keys, values, log_decay, cosine, sine)
    other = moved_by(own, "ep_1", 1)
    chip = small(chip_kernel, packed_shape, [SMEM, VMEM, VMEM], VMEM)(core, own, other)
    near = [moved_by(chip, "ep_0", d, False) for d in (3, 2, 1)]
    before, window = small(
        near_kernel, (packed_shape, packed_shape), [VMEM] * 4, (VMEM, VMEM)
    )(chip, *near)
    far = [moved_by(window, "ep_0", d, False) for d in (12, 8, 4)]
    prefix = small(far_kernel, packed_shape, [VMEM] * 4, VMEM)(before, *far)
    swapped = moved_by(prefix, "ep_1", 1)
    state_in = small(
        enter_kernel,
        jax.ShapeDtypeStruct((heads * key_size, value_size), F32),
        [SMEM] + [VMEM] * 3,
        VMEM,
    )(core, prefix, swapped, other)

    shared_half = call(
        pack_kernel,
        jax.ShapeDtypeStruct((width * 3 * shared_size // 2 // LANES, LANES), BF16),
        [SMEM] + [VMEM] * 3,
        VMEM,
        [],
        100000,
        6 * width * shared_size,
        8,
    )(core, shared_gate, shared_up, shared_down)
    shared_mine = [moved_by(shared_half, "tp", d) for d in around]
    shared_theirs = [moved_by(part, "ep_1", 1) for part in shared_mine]
    out_theirs = [moved_by(part, "ep_1", 1) for part in out_mine]
    shared_sum = call(
        shared_kernel,
        jax.ShapeDtypeStruct((rows_dev, width), F32),
        [SMEM] + [VMEM] * (4 + 2 * (n_tp - 1)),
        VMEM,
        [
            pltpu.VMEM((2,) + shared_half.shape, BF16),
            pltpu.VMEM((shared_size, width), BF16),
        ],
        2 * n_tp * rows_dev * width * shared_size * 3,
        10 * rows_dev * width * 2,
        20,
    )(core, normed, shared_gate, shared_up, shared_down, *shared_mine, *shared_theirs)

    pieces, chunks = 4, 3
    answers = call(
        expert_kernel,
        jax.ShapeDtypeStruct((tile_rows, LANES), BF16),
        [HBM] * 4,
        HBM,
        [
            pltpu.VMEM((width, hidden_size), BF16),
            pltpu.VMEM((width, hidden_size), BF16),
            pltpu.VMEM((hidden_size, width), BF16),
            pltpu.VMEM((slots, width), BF16),
            pltpu.VMEM((tile_rows, LANES), BF16),
            pltpu.VMEM((tile_rows, LANES), BF16),
            pltpu.SemaphoreType.DMA((3, pieces)),
            pltpu.SemaphoreType.DMA((chunks,)),
            pltpu.SemaphoreType.DMA((chunks,)),
        ],
        2 * slots * width * hidden_size * 3,
        3 * 2 * width * hidden_size,
        61,
    )(arrived.reshape(tile_rows, LANES), expert_gate, expert_up, expert_down)
    returned = lax.all_to_all(
        answers.reshape(experts, capacity * TILE, LANES),
        EP_TP,
        split_axis=0,
        concat_axis=0,
        tiled=True,
    )

    gated = call(
        retention_kernel,
        tuple(jax.ShapeDtypeStruct((rows_dev, heads * value_size), BF16) for _ in range(n_tp)),
        [SMEM] + [VMEM] * 8,
        (VMEM,) * n_tp,
        [pltpu.VMEM((span, heads * value_size), BF16)],
        2 * span * heads * value_size * 1000,
        10 * rows_dev * width * 2,
        20,
    )(seat, queries, keys, values, gate, log_decay, cosine, sine, state_in)
    gated = [gated[0]] + [moved_by(gated[d], "tp", d) for d in around]

    return call(
        finish_kernel,
        tuple(jax.ShapeDtypeStruct((rows_dev, width), BF16) for _ in range(2)),
        [SMEM, SMEM, VMEM] + [VMEM] * n_tp + [HBM] * (2 * n_tp + 1),
        (VMEM,) * 2,
        [
            pltpu.VMEM((top, rows_dev * TILE, LANES), BF16),
            pltpu.VMEM((top, rows_dev, width), BF16),
            pltpu.VMEM((tile_rows, LANES), BF16),
            pltpu.VMEM((rows_dev, width), F32),
            pltpu.VMEM((2 * half_out, width), BF16),
            pltpu.VMEM((n_tp - 1, half_out, width), BF16),
            pltpu.VMEM((n_tp - 1, half_out, width), BF16),
            pltpu.SemaphoreType.DMA((2 * n_tp + 1,)),
        ],
        2 * rows_dev * width * 1500,
        10 * rows_dev * width * 2,
        61,
    )(
        places,
        core,
        route_weight,
        *gated,
        returned.reshape(tile_rows, LANES),
        shared_sum,
        w_out,
        *out_mine,
        *out_theirs,
    )


def solution(mesh):
    split = Mesh(
        mesh.devices.reshape(mesh.shape["grp"], mesh.shape["ep"] // 2, 2, mesh.shape["tp"]),
        ("grp", "ep_0", "ep_1", "tp"),
    )
    return jax.shard_map(
        per_device,
        mesh=split,
        in_specs=(
            P(GRP_EP, "tp"),
            P(GRP_EP, "tp"),
            P(GRP_EP, "tp"),
            P(GRP_EP, "tp"),
            P(GRP_EP, "tp"),
            P("tp", None),
            P(GRP_EP_TP, None),
            P(),
            P(GRP_EP_TP, None),
            P(GRP_EP_TP, None),
            P(EP_TP, None, None),
            P(EP_TP, None, None),
            P(EP_TP, None, None),
            P(None, "tp"),
            P(None, "tp"),
            P("tp", None),
        ),
        out_specs=(P(GRP_EP_TP, None), P(GRP_EP_TP, None)),
        check_vma=False,
    )
```

```python
import jax
import jax.numpy as jnp
from jax import lax
from jax.experimental import pallas as pl
from jax.experimental.pallas import tpu as pltpu
from jax.sharding import Mesh
from jax.sharding import PartitionSpec as P


BLOCK = 128
LANES = 128
TILE = 16
EP = ("ep_0", "ep_1")
EP_TP = ("ep_0", "ep_1", "tp")
GRP_EP = ("grp", "ep_0", "ep_1")
GRP_EP_TP = ("grp", "ep_0", "ep_1", "tp")
STATE_ROWS = 80

ROPE_BASE = 10000.0
GROUP_EPS = 1e-05
NORM_EPS = 1e-06


VMEM = pl.BlockSpec(memory_space=pltpu.VMEM)
SMEM = pl.BlockSpec(memory_space=pltpu.SMEM)
HBM = pl.BlockSpec(memory_space=pltpu.HBM)
F32 = jnp.float32
BF16 = jnp.bfloat16
MIB = 1 << 20


def call(kernel, out_shape, in_specs, out_specs, scratch, flops, moved, limit):
    return pl.pallas_call(
        kernel,
        out_shape=out_shape,
        in_specs=in_specs,
        out_specs=out_specs,
        scratch_shapes=scratch,
        compiler_params=pltpu.CompilerParams(vmem_limit_bytes=int(limit * MIB)),
        cost_estimate=pl.CostEstimate(flops=flops, bytes_accessed=moved, transcendentals=0),
    )


def dot(a, b):
    return jnp.dot(a, b, preferred_element_type=F32)


def swap_matrix():
    side = TILE * TILE
    row = lax.broadcasted_iota(jnp.int32, (side, side), 0)
    col = lax.broadcasted_iota(jnp.int32, (side, side), 1)
    hit = (row // TILE == col % TILE) & (row % TILE == col // TILE)
    return jnp.where(hit, 1.0, 0.0).astype(BF16)


def rows_to_tiles(swap, rows):
    count = rows.shape[0] // TILE
    width = rows.shape[1] // LANES
    found = []
    for at in range(0, count, 2):
        pair = [
            jnp.concatenate(
                [
                    rows[g * TILE : (g + 1) * TILE, k * LANES : (k + 1) * LANES]
                    for k in range(width)
                ],
                axis=0,
            )
            for g in range(at, min(at + 2, count))
        ]
        out = dot(swap, jnp.concatenate(pair, axis=1)).astype(BF16)
        found += [out[:, g * LANES : (g + 1) * LANES] for g in range(len(pair))]
    return found


def prep_kernel(
    routes, x_hbm, gain_hbm, normed_hbm, outbound, places, x, gain, normed, tiles, used, sems
):
    copies = [
        pltpu.make_async_copy(x_hbm, x, sems.at[0]),
        pltpu.make_async_copy(gain_hbm, gain, sems.at[1]),
    ]
    for copy in copies:
        copy.start()
    outbound[...] = jnp.zeros_like(outbound)
    top, number = routes.shape
    experts = used.shape[0]
    capacity = outbound.shape[0] // (experts * TILE)
    for e in range(experts):
        used[e] = 0

    @pl.loop(0, number, unroll=8)
    def _(n):
        for k in range(top):
            e = routes[k, n]
            rank = used[e]
            used[e] = rank + 1
            places[k, n] = e * capacity + rank

    for copy in copies:
        copy.wait()
    source = x[...].astype(F32)
    scale = lax.rsqrt(jnp.mean(source * source, axis=-1, keepdims=True) + NORM_EPS)
    rows = (source * scale * gain[...]).astype(BF16)
    normed[...] = rows
    keep = pltpu.make_async_copy(normed, normed_hbm, sems.at[2])
    keep.start()
    for g, tile in enumerate(rows_to_tiles(swap_matrix(), rows)):
        tiles[g * TILE * TILE : (g + 1) * TILE * TILE, :] = tile

    @pl.loop(0, number, unroll=8)
    def _(n):
        row = tiles[pl.ds(pl.multiple_of(n * TILE, TILE), TILE), :]
        for k in range(top):
            at = pl.multiple_of(places[k, n] * TILE, TILE)
            outbound[pl.ds(at, TILE), :] = row

    keep.wait()


def expert_kernel(
    arrived_hbm,
    gate_hbm,
    up_hbm,
    down_hbm,
    out_hbm,
    gate_w,
    up_w,
    down_w,
    rows,
    arrived,
    out,
    sems,
    in_sems,
    out_sems,
):
    pieces = sems.shape[1]
    chunks = out_sems.shape[0]
    share = arrived.shape[0] // chunks
    landed = []
    for j in range(chunks):
        at = pl.ds(j * share, share)
        landed.append(pltpu.make_async_copy(arrived_hbm.at[at], arrived.at[at], in_sems.at[j]))
        landed[-1].start()
    copies = [[], [], []]
    for i, (src, dst) in enumerate(((gate_hbm, gate_w), (up_hbm, up_w), (down_hbm, down_w))):
        part = dst.shape[0] // pieces
        for j in range(pieces):
            at = pl.ds(j * part, part)
            copies[i].append(pltpu.make_async_copy(src.at[0, at], dst.at[at], sems.at[i, j]))
            copies[i][-1].start()
    swap = swap_matrix()
    side = TILE * TILE
    groups = arrived.shape[0] // side
    for at in range(0, groups, 2):
        if at * side % share == 0:
            landed[at * side // share].wait()
        pair = jnp.concatenate(
            [arrived[g * side : (g + 1) * side, :] for g in (at, at + 1)], axis=1
        )
        turned = dot(swap, pair).astype(BF16)
        for j in range(2):
            for k in range(TILE):
                rows[
                    (at + j) * TILE : (at + j + 1) * TILE, k * LANES : (k + 1) * LANES
                ] = turned[k * TILE : (k + 1) * TILE, j * LANES : (j + 1) * LANES]
    for copy in copies[0]:
        copy.wait()
    gated = jax.nn.silu(dot(rows[...], gate_w[...]))
    for copy in copies[1]:
        copy.wait()
    hidden = (gated * dot(rows[...], up_w[...])).astype(BF16)
    for copy in copies[2]:
        copy.wait()
    left = []
    step = rows.shape[0] // chunks
    for j in range(chunks):
        result = dot(hidden[j * step : (j + 1) * step, :], down_w[...]).astype(BF16)
        for g, tile in enumerate(rows_to_tiles(swap, result)):
            out[j * share + g * side : j * share + (g + 1) * side, :] = tile
        at = pl.ds(j * share, share)
        left.append(pltpu.make_async_copy(out.at[at], out_hbm.at[at], out_sems.at[j]))
        left[-1].start()
    for copy in left:
        copy.wait()


def turn_matrix():
    row = lax.broadcasted_iota(jnp.int32, (LANES, LANES), 0)
    col = lax.broadcasted_iota(jnp.int32, (LANES, LANES), 1)
    return row, col


def rotated(x, cosine, sine, half):
    row, col = turn_matrix()
    first = col % (2 * half) < half
    partner = jnp.where(first, col + half, col - half)
    turn = jnp.where(row == partner, jnp.where(first, -1.0, 1.0), 0.0).astype(BF16)
    return x.astype(F32) * cosine + dot(x, turn) * sine


def lower(size, strict=False):
    row = lax.broadcasted_iota(jnp.int32, (size, size), 0)
    col = lax.broadcasted_iota(jnp.int32, (size, size), 1)
    return row > col if strict else row >= col


def summed_f32(a, b, dims):
    return lax.dot_general(
        a, b, (dims, ((), ())), preferred_element_type=F32, precision=lax.Precision.HIGHEST
    )


def spread_heads(per_head, key_size):
    lane = lax.broadcasted_iota(jnp.int32, (per_head.shape[0], LANES), 1)
    out = per_head[:, 0:1]
    for h in range(1, per_head.shape[1]):
        out = jnp.where(lane >= h * key_size, per_head[:, h : h + 1], out)
    return out


def state_kernel(k, v, log_decay, cosine, sine, packed):
    heads = log_decay.shape[0]
    key_size = k.shape[1] // heads
    value_size = v.shape[1] // heads
    span = k.shape[0]
    k_rot = (rotated(k[...], cosine[...], sine[...], key_size // 2) * key_size ** (-0.5)).astype(
        BF16
    )
    above = jnp.where(lower(BLOCK, True), 1.0, 0.0)
    after = jnp.zeros((1, heads), F32)
    tails = [None] * (span // BLOCK)
    for b in reversed(range(span // BLOCK)):
        part = log_decay[:, b * BLOCK : (b + 1) * BLOCK]
        tails[b] = summed_f32(above, part, ((0,), (1,))) + after
        after = after + summed_f32(jnp.ones((1, BLOCK), F32), part, ((1,), (1,)))
    tail = jnp.concatenate(tails, axis=0)
    faded = (k_rot.astype(F32) * jnp.exp(spread_heads(tail, key_size))).astype(BF16)
    state = dot(faded.T, v[...])
    for h in range(heads):
        packed[h * STATE_ROWS : h * STATE_ROWS + key_size, :] = state[
            h * key_size : (h + 1) * key_size, h * value_size : (h + 1) * value_size
        ].astype(BF16)
        whole = after[:, h : h + 1]
        high = whole.astype(BF16)
        low = (whole - high.astype(F32)).astype(BF16)
        pad = STATE_ROWS - key_size
        row = lax.broadcasted_iota(jnp.int32, (pad, LANES), 0)
        packed[h * STATE_ROWS + key_size : (h + 1) * STATE_ROWS, :] = jnp.where(
            row == 0, high.astype(F32), low.astype(F32)
        ).astype(BF16)


def retention_kernel(seat, q, k, v, gate, log_decay, cosine, sine, state_in, w_out, *rest):
    own, *outs, gated = rest
    heads = log_decay.shape[0]
    key_size = q.shape[1] // heads
    value_size = v.shape[1] // heads
    span = q.shape[0]
    q_rot = rotated(q[...], cosine[...], sine[...], key_size // 2).astype(BF16)
    k_rot = (rotated(k[...], cosine[...], sine[...], key_size // 2) * key_size ** (-0.5)).astype(
        BF16
    )
    keep = lower(BLOCK)
    ones = jnp.where(keep, 1.0, 0.0)
    lane = lax.broadcasted_iota(jnp.int32, (BLOCK, LANES), 1)
    state = state_in[...]
    for b in range(span // BLOCK):
        at = slice(b * BLOCK, (b + 1) * BLOCK)
        part = log_decay[:, at]
        column = summed_f32(ones, part, ((1,), (1,)))
        across = summed_f32(part, ones, ((1,), (1,)))
        total = column[BLOCK - 1 : BLOCK, :]
        q_part = q_rot[at, :]
        k_part = k_rot[at, :]
        v_part = v[at, :]
        lifted = q_part.astype(F32) * jnp.exp(spread_heads(column, key_size))
        tail = jnp.exp(spread_heads(total - column, key_size))
        faded = (k_part.astype(F32) * tail).astype(BF16)
        held = state.astype(BF16)
        grown = dot(faded.T, v_part)
        fade = []
        for h in range(heads):
            mine = (lane >= h * key_size) & (lane < (h + 1) * key_size)
            q_head = jnp.where(mine, q_part.astype(F32), 0.0).astype(BF16)
            scores = lax.dot_general(
                q_head, k_part, (((1,), (1,)), ((), ())), preferred_element_type=F32
            )
            gap = jnp.where(keep, column[:, h : h + 1] - across[h : h + 1, :], 0.0)
            weights = jnp.where(keep, scores * jnp.exp(gap), 0.0).astype(BF16)
            columns = slice(h * value_size, (h + 1) * value_size)
            kept = dot(weights, v_part[:, columns]) + dot(
                jnp.where(mine, lifted, 0.0).astype(BF16), held
            )
            center = jnp.mean(kept, axis=-1, keepdims=True)
            off = kept - center
            spread = jnp.mean(off * off, axis=-1, keepdims=True)
            act = jax.nn.silu(gate[at, columns].astype(F32))
            gated[at, columns] = (act * (off * lax.rsqrt(spread + GROUP_EPS))).astype(BF16)
            fade.append(
                state[h * key_size : (h + 1) * key_size, :] * jnp.exp(total[:, h : h + 1])
                + grown[h * key_size : (h + 1) * key_size, columns]
            )
        state = jnp.concatenate(fade, axis=0)
    count = len(outs) + 1
    share = span // count
    for d in range(count):
        first = lax.rem(seat[0] + d, count) * share
        part = gated[pl.ds(pl.multiple_of(first, share), share), :]
        if d == 0:
            own[...] = dot(part, w_out[...]).astype(BF16)
        else:
            outs[d - 1][...] = part


def pack_kernel(core, gate_w, up_w, down_w, w_out, whole, half, out_half):
    def fill(to, first, depth, cut, thin):
        to[0:depth, :] = gate_w[pl.ds(first, depth), :]
        to[depth : 2 * depth, :] = up_w[pl.ds(first, depth), :]
        for k in range(down_w.shape[1] // LANES):
            at = 2 * depth + k * thin
            to[at : at + thin, :] = down_w[pl.ds(cut, thin), k * LANES : (k + 1) * LANES]

    depth, thin = gate_w.shape[0], down_w.shape[0]
    fill(whole, 0, depth, 0, thin)
    at = pl.multiple_of(core[0] * (depth // 2), TILE)
    cut = pl.multiple_of(core[0] * (thin // 2), TILE)
    fill(half, at, depth // 2, cut, thin // 2)
    share = out_half.shape[0]
    out_half[...] = w_out[pl.ds(pl.multiple_of(core[0] * share, TILE), share), :]


def shared_kernel(core, normed, own, near, near_other, mine, theirs, out, packed, down):
    rows = normed[...]
    depth = rows.shape[1]
    total = None
    for part in (own, near, near_other):
        hidden = jax.nn.silu(dot(rows, part[0:depth, :])) * dot(rows, part[depth : 2 * depth, :])
        thin = down.shape[0]
        for k in range(down.shape[1] // LANES):
            at = 2 * depth + k * thin
            down[:, k * LANES : (k + 1) * LANES] = part[at : at + thin, :]
        product = dot(hidden.astype(BF16), down[...])
        total = product if total is None else total + product
    packed[0] = jnp.where(core[0] == 0, mine[...], theirs[...])
    packed[1] = jnp.where(core[0] == 0, theirs[...], mine[...])
    half = depth // 2
    thin = down.shape[0] // 2
    gated = dot(rows[:, :half], packed[0, :half]) + dot(rows[:, half:], packed[1, :half])
    up = dot(rows[:, :half], packed[0, half:depth]) + dot(rows[:, half:], packed[1, half:depth])
    for c in range(2):
        for k in range(down.shape[1] // LANES):
            at = depth + k * thin
            down[c * thin : (c + 1) * thin, k * LANES : (k + 1) * LANES] = packed[c, at : at + thin]
    hidden = (jax.nn.silu(gated) * up).astype(BF16)
    out[...] = total + dot(hidden, down[...])


def finish_kernel(
    places,
    core,
    returned,
    weight,
    own,
    gated_left,
    gated_right,
    gated_far,
    shared_hbm,
    near_hbm,
    other_hbm,
    mine_hbm,
    theirs_hbm,
    mixer_out,
    moe_out,
    picked,
    rows,
    shared,
    near,
    other,
    far,
    sems,
):
    share = far.shape[1]
    pairs = (
        (shared_hbm, shared),
        (near_hbm, near),
        (other_hbm, other),
        (mine_hbm, far.at[0]),
        (theirs_hbm, far.at[1]),
    )
    copies = [pltpu.make_async_copy(a, b, sems.at[i]) for i, (a, b) in enumerate(pairs)]
    for copy in copies:
        copy.start()
    swap = swap_matrix()
    side = TILE * TILE
    number = moe_out.shape[0]
    top = weight.shape[1]

    @pl.loop(0, number, unroll=8)
    def _(n):
        for k in range(top):
            place = places[k, n]
            picked[k, pl.ds(pl.multiple_of(n * TILE, TILE), TILE), :] = returned[
                pl.ds(pl.multiple_of(place * TILE, TILE), TILE), :
            ]

    for k in range(top):
        for at in range(0, number // TILE, 2):
            pair = jnp.concatenate(
                [picked[k, g * side : (g + 1) * side, :] for g in (at, at + 1)], axis=1
            )
            turned = dot(swap, pair).astype(BF16)
            for j in range(2):
                for c in range(TILE):
                    rows[
                        k,
                        (at + j) * TILE : (at + j + 1) * TILE,
                        c * LANES : (c + 1) * LANES,
                    ] = turned[c * TILE : (c + 1) * TILE, j * LANES : (j + 1) * LANES]
    for copy in copies:
        copy.wait()
    total = shared[...]
    for k in range(top):
        total = total + rows[k].astype(F32) * weight[:, k : k + 1]
    moe_out[...] = total.astype(BF16)
    first = core[0] == 0
    left, right, across = gated_left[...], gated_right[...], gated_far[...]
    mixed = own[...].astype(F32)
    mixed = mixed + dot(jnp.where(first, left, right), near[...])
    mixed = mixed + dot(jnp.where(first, right, left), other[...])
    low, high = across[:, :share], across[:, share:]
    mixed = mixed + dot(jnp.where(first, low, high), far[0])
    mixed = mixed + dot(jnp.where(first, high, low), far[1])
    mixer_out[...] = mixed.astype(BF16)


def moved_by(array, axis, step, around=True):
    count = lax.axis_size(axis)
    pairs = [
        (s, (s + step) % count) for s in range(count) if around or 0 <= s + step < count
    ]
    return lax.ppermute(array, axis, pairs)


def outward(array):
    count = lax.axis_size("tp")
    pairs = [(s, (s + 1) % count) for s in range(count)]
    pairs += [(count + s, count + (s - 1) % count) for s in range(count)]
    return lax.ppermute(array, ("ep_1", "tp"), pairs)


def opened(packed):
    wide = packed.astype(F32)
    size = STATE_ROWS - TILE
    return wide[size : size + 1, :] + wide[size + 1 : size + 2, :], wide[:size, :]


def closed(part):
    log, state = part
    high = log.astype(BF16).astype(F32)
    row = lax.broadcasted_iota(jnp.int32, (TILE, LANES), 0)
    return jnp.concatenate([state, jnp.where(row == 0, high, log - high)], axis=0).astype(BF16)


def joined(earlier, later):
    return earlier[0] + later[0], earlier[1] * jnp.exp(later[0]) + later[1]


def picked_by(core, a, b):
    return jnp.where(core == 0, a.astype(F32), b.astype(F32)).astype(BF16)


def chip_kernel(core, own, other, out):
    mine = picked_by(core[0], own[:STATE_ROWS, :], own[STATE_ROWS:, :])
    theirs = picked_by(core[0], other[:STATE_ROWS, :], other[STATE_ROWS:, :])
    early, late = picked_by(core[0], mine, theirs), picked_by(core[0], theirs, mine)
    out[...] = closed(joined(opened(early), opened(late)))


def near_kernel(chip, far3, far2, far1, before, window):
    start = joined(joined(opened(far3[...]), opened(far2[...])), opened(far1[...]))
    before[...] = closed(start)
    window[...] = closed(joined(start, opened(chip[...])))


def far_kernel(before, far12, far8, far4, prefix):
    start = joined(joined(opened(far12[...]), opened(far8[...])), opened(far4[...]))
    prefix[...] = closed(joined(start, opened(before[...])))


def enter_kernel(core, mine, theirs, other, state):
    size = STATE_ROWS - TILE
    for h in range(other.shape[0] // STATE_ROWS):
        held = jnp.where(core[0] == h, mine[...].astype(F32), theirs[...].astype(F32))
        chip_before = opened(held)
        first = opened(other[h * STATE_ROWS : (h + 1) * STATE_ROWS, :])
        both = joined(chip_before, first)
        state[h * size : (h + 1) * size, :] = jnp.where(core[0] == 0, chip_before[1], both[1])


def small(kernel, outs, in_specs, out_specs):
    return call(kernel, outs, in_specs, out_specs, [], 100000, 100000, 2)


def per_device(
    queries,
    keys,
    values,
    gate,
    log_decay,
    w_out,
    moe_input,
    moe_gain,
    routes,
    route_weight,
    expert_gate,
    expert_up,
    expert_down,
    shared_gate,
    shared_up,
    shared_down,
):
    span = queries.shape[0]
    heads = log_decay.shape[1]
    key_size = queries.shape[1] // heads
    value_size = values.shape[1] // heads
    rows_dev, width = moe_input.shape
    top = routes.shape[1]
    n_tp = lax.axis_size("tp")
    experts = lax.axis_size(EP) * n_tp
    capacity = rows_dev * top * 3 // (2 * experts)
    hidden_size = expert_gate.shape[2]
    shared_size = shared_gate.shape[1]
    slots = experts * capacity
    tile_rows = slots * TILE

    core = lax.axis_index("ep_1").reshape(1).astype(jnp.int32)
    seat = lax.axis_index("tp").reshape(1).astype(jnp.int32)
    around = range(1, n_tp)
    half_out = w_out.shape[0] // 2
    packed_shape = jax.ShapeDtypeStruct((STATE_ROWS, value_size), BF16)

    out_near = outward(w_out)

    normed, outbound, places = call(
        prep_kernel,
        (
            jax.ShapeDtypeStruct((rows_dev, width), BF16),
            jax.ShapeDtypeStruct((tile_rows, LANES), BF16),
            jax.ShapeDtypeStruct((top, rows_dev), jnp.int32),
        ),
        [SMEM, HBM, HBM],
        (HBM, VMEM, SMEM),
        [
            pltpu.VMEM((rows_dev, width), BF16),
            pltpu.VMEM((1, width), F32),
            pltpu.VMEM((rows_dev, width), BF16),
            pltpu.VMEM((rows_dev * TILE, LANES), BF16),
            pltpu.SMEM((experts,), jnp.int32),
            pltpu.SemaphoreType.DMA((3,)),
        ],
        2 * rows_dev * width * 256,
        4 * rows_dev * width,
        62,
    )(routes.T, moe_input, moe_gain.reshape(1, width))

    arrived = lax.all_to_all(
        outbound.reshape(experts, capacity * TILE, LANES),
        EP_TP,
        split_axis=0,
        concat_axis=0,
        tiled=True,
    )

    half = key_size // 2
    frequency = ROPE_BASE ** (-jnp.arange(half, dtype=F32) / half)
    spots = lax.axis_index(EP) * span + jnp.arange(span, dtype=jnp.int32)
    angles = spots.astype(F32)[:, None] * jnp.tile(frequency, LANES // half)[None, :]
    cosine = jnp.cos(angles)
    sine = jnp.sin(angles)

    own = call(
        state_kernel,
        jax.ShapeDtypeStruct((heads * STATE_ROWS, value_size), BF16),
        [VMEM] * 5,
        VMEM,
        [],
        2 * span * LANES * 512,
        4 * span * LANES * 4,
        12,
    )(keys, values, log_decay.T, cosine, sine)
    other = moved_by(own, "ep_1", 1)
    chip = small(chip_kernel, packed_shape, [SMEM, VMEM, VMEM], VMEM)(core, own, other)
    near = [moved_by(chip, "ep_0", d, False) for d in (3, 2, 1)]
    before, window = small(
        near_kernel, (packed_shape, packed_shape), [VMEM] * 4, (VMEM, VMEM)
    )(chip, *near)
    far = [moved_by(window, "ep_0", d, False) for d in (12, 8, 4)]
    prefix = small(far_kernel, packed_shape, [VMEM] * 4, VMEM)(before, *far)
    swapped = moved_by(prefix, "ep_1", 1)
    state_in = small(
        enter_kernel,
        jax.ShapeDtypeStruct((heads * key_size, value_size), F32),
        [SMEM] + [VMEM] * 3,
        VMEM,
    )(core, prefix, swapped, other)

    pack_rows = width * 3 * shared_size // LANES
    shared_own, shared_half, out_half = call(
        pack_kernel,
        (
            jax.ShapeDtypeStruct((pack_rows, LANES), BF16),
            jax.ShapeDtypeStruct((pack_rows // 2, LANES), BF16),
            jax.ShapeDtypeStruct((half_out, width), BF16),
        ),
        [SMEM] + [VMEM] * 4,
        (VMEM,) * 3,
        [],
        100000,
        6 * width * shared_size,
        16,
    )(core, shared_gate, shared_up, shared_down, w_out)
    shared_near = outward(shared_own)
    shared_mine = moved_by(shared_half, "tp", 2)
    out_mine = moved_by(out_half, "tp", 2)
    shared_other, shared_theirs, out_other, out_theirs = [
        moved_by(part, "ep_1", 1) for part in (shared_near, shared_mine, out_near, out_mine)
    ]
    shared_sum = call(
        shared_kernel,
        jax.ShapeDtypeStruct((rows_dev, width), F32),
        [SMEM] + [VMEM] * 6,
        VMEM,
        [
            pltpu.VMEM((2,) + shared_half.shape, BF16),
            pltpu.VMEM((shared_size, width), BF16),
        ],
        2 * n_tp * rows_dev * width * shared_size * 3,
        10 * rows_dev * width * 2,
        20,
    )(core, normed, shared_own, shared_near, shared_other, shared_mine, shared_theirs)

    pieces, chunks = 4, 3
    answers = call(
        expert_kernel,
        jax.ShapeDtypeStruct((tile_rows, LANES), BF16),
        [HBM] * 4,
        HBM,
        [
            pltpu.VMEM((width, hidden_size), BF16),
            pltpu.VMEM((width, hidden_size), BF16),
            pltpu.VMEM((hidden_size, width), BF16),
            pltpu.VMEM((slots, width), BF16),
            pltpu.VMEM((tile_rows, LANES), BF16),
            pltpu.VMEM((tile_rows, LANES), BF16),
            pltpu.SemaphoreType.DMA((3, pieces)),
            pltpu.SemaphoreType.DMA((chunks,)),
            pltpu.SemaphoreType.DMA((chunks,)),
        ],
        2 * slots * width * hidden_size * 3,
        3 * 2 * width * hidden_size,
        62,
    )(arrived.reshape(tile_rows, LANES), expert_gate, expert_up, expert_down)
    returned = lax.all_to_all(
        answers.reshape(experts, capacity * TILE, LANES),
        EP_TP,
        split_axis=0,
        concat_axis=0,
        tiled=True,
    )

    gated_shape = jax.ShapeDtypeStruct((rows_dev, heads * value_size), BF16)
    own_mixed, *gated = call(
        retention_kernel,
        (jax.ShapeDtypeStruct((rows_dev, width), BF16),) + (gated_shape,) * (n_tp - 1),
        [SMEM] + [VMEM] * 9,
        (VMEM,) * n_tp,
        [pltpu.VMEM((span, heads * value_size), BF16)],
        2 * span * heads * value_size * 1000,
        10 * rows_dev * width * 2,
        20,
    )(seat, queries, keys, values, gate, log_decay.T, cosine, sine, state_in, w_out)
    gated_left, gated_far, gated_right = [moved_by(gated[d - 1], "tp", d) for d in around]

    return call(
        finish_kernel,
        tuple(jax.ShapeDtypeStruct((rows_dev, width), BF16) for _ in range(2)),
        [SMEM, SMEM] + [VMEM] * 6 + [HBM] * 5,
        (VMEM,) * 2,
        [
            pltpu.VMEM((top, rows_dev * TILE, LANES), BF16),
            pltpu.VMEM((top, rows_dev, width), BF16),
            pltpu.VMEM((rows_dev, width), F32),
            pltpu.VMEM((2 * half_out, width), BF16),
            pltpu.VMEM((2 * half_out, width), BF16),
            pltpu.VMEM((2, half_out, width), BF16),
            pltpu.SemaphoreType.DMA((5,)),
        ],
        2 * rows_dev * width * 1500,
        10 * rows_dev * width * 2,
        28,
    )(
        places,
        core,
        returned.reshape(tile_rows, LANES),
        route_weight,
        own_mixed,
        gated_left,
        gated_right,
        gated_far,
        shared_sum,
        out_near,
        out_other,
        out_mine,
        out_theirs,
    )


def solution(mesh):
    split = Mesh(
        mesh.devices.reshape(mesh.shape["grp"], mesh.shape["ep"] // 2, 2, mesh.shape["tp"]),
        ("grp", "ep_0", "ep_1", "tp"),
    )
    return jax.shard_map(
        per_device,
        mesh=split,
        in_specs=(
            P(GRP_EP, "tp"),
            P(GRP_EP, "tp"),
            P(GRP_EP, "tp"),
            P(GRP_EP, "tp"),
            P(GRP_EP, "tp"),
            P("tp", None),
            P(GRP_EP_TP, None),
            P(),
            P(GRP_EP_TP, None),
            P(GRP_EP_TP, None),
            P(EP_TP, None, None),
            P(EP_TP, None, None),
            P(EP_TP, None, None),
            P(None, "tp"),
            P(None, "tp"),
            P("tp", None),
        ),
        out_specs=(P(GRP_EP_TP, None), P(GRP_EP_TP, None)),
        check_vma=False,
    )
```

```python
import jax
import jax.numpy as jnp
from jax import lax
from jax.experimental import pallas as pl
from jax.experimental.pallas import tpu as pltpu
from jax.sharding import Mesh
from jax.sharding import PartitionSpec as P


BLOCK = 128
LANES = 128
TILE = 16
CHIPS = 4
EP = ("ep_hi", "ep_lo", "ep_1")
EP_TP = EP + ("tp",)
GRP_EP = ("grp",) + EP
GRP_EP_TP = ("grp",) + EP_TP
STATE_ROWS = 80

ROPE_BASE = 10000.0
GROUP_EPS = 1e-05
NORM_EPS = 1e-06


VMEM = pl.BlockSpec(memory_space=pltpu.VMEM)
SMEM = pl.BlockSpec(memory_space=pltpu.SMEM)
HBM = pl.BlockSpec(memory_space=pltpu.HBM)
F32 = jnp.float32
BF16 = jnp.bfloat16
MIB = 1 << 20


def call(kernel, out_shape, in_specs, out_specs, scratch, flops, moved, limit):
    return pl.pallas_call(
        kernel,
        out_shape=out_shape,
        in_specs=in_specs,
        out_specs=out_specs,
        scratch_shapes=scratch,
        compiler_params=pltpu.CompilerParams(vmem_limit_bytes=int(limit * MIB)),
        cost_estimate=pl.CostEstimate(flops=flops, bytes_accessed=moved, transcendentals=0),
    )


def dot(a, b):
    return jnp.dot(a, b, preferred_element_type=F32)


def column(c):
    return slice(c * LANES, (c + 1) * LANES)


def prep_kernel(
    routes, x_hbm, gain_hbm, normed_hbm, outbound, places, x, gain, normed, tiles, used, sems
):
    copies = [
        pltpu.make_async_copy(x_hbm, x, sems.at[0]),
        pltpu.make_async_copy(gain_hbm, gain, sems.at[1]),
    ]
    for copy in copies:
        copy.start()
    outbound[...] = jnp.zeros_like(outbound)
    top, number = routes.shape
    experts = used.shape[0]
    capacity = outbound.shape[0] // (experts * TILE)
    for e in range(experts):
        used[e] = 0

    @pl.loop(0, number, unroll=8)
    def _(n):
        for k in range(top):
            e = routes[k, n]
            rank = used[e]
            used[e] = rank + 1
            places[k, n] = e * capacity + rank

    for copy in copies:
        copy.wait()
    source = x[...].astype(F32)
    scale = lax.rsqrt(jnp.mean(source * source, axis=-1, keepdims=True) + NORM_EPS)
    rows = (source * scale * gain[...]).astype(BF16)
    normed[...] = rows
    keep = pltpu.make_async_copy(normed, normed_hbm, sems.at[2])
    keep.start()
    wide = rows.astype(F32)
    for c in range(TILE):
        tiles[pl.ds(c, number, stride=TILE), :] = wide[:, column(c)]

    @pl.loop(0, number, unroll=8)
    def _(n):
        row = tiles[pl.ds(pl.multiple_of(n * TILE, TILE), TILE), :].astype(BF16)
        for k in range(top):
            at = pl.multiple_of(places[k, n] * TILE, TILE)
            outbound[pl.ds(at, TILE), :] = row

    keep.wait()


def expert_kernel(
    arrived_hbm,
    gate_hbm,
    up_hbm,
    down_hbm,
    out_hbm,
    gate_w,
    up_w,
    down_w,
    rows,
    arrived,
    wide,
    out,
    sems,
    in_sems,
    out_sems,
):
    pieces = sems.shape[1]
    chunks = out_sems.shape[0]
    share = arrived.shape[0] // chunks
    landed = []
    for j in range(chunks):
        at = pl.ds(j * share, share)
        landed.append(pltpu.make_async_copy(arrived_hbm.at[at], arrived.at[at], in_sems.at[j]))
        landed[-1].start()
    copies = [[], [], []]
    for i, (src, dst) in enumerate(((gate_hbm, gate_w), (up_hbm, up_w), (down_hbm, down_w))):
        part = dst.shape[0] // pieces
        for j in range(pieces):
            at = pl.ds(j * part, part)
            copies[i].append(pltpu.make_async_copy(src.at[0, at], dst.at[at], sems.at[i, j]))
            copies[i][-1].start()
    depth = share // TILE
    for j in range(chunks):
        landed[j].wait()
        at = slice(j * share, (j + 1) * share)
        wide[at, :] = arrived[at, :].astype(F32)
        for c in range(TILE):
            rows[j * depth : (j + 1) * depth, column(c)] = wide[
                pl.ds(j * share + c, depth, stride=TILE), :
            ].astype(BF16)
    for copy in copies[0]:
        copy.wait()
    gated = jax.nn.silu(dot(rows[...], gate_w[...]))
    for copy in copies[1]:
        copy.wait()
    hidden = (gated * dot(rows[...], up_w[...])).astype(BF16)
    for copy in copies[2]:
        copy.wait()
    count = rows.shape[0]
    step = 4 * LANES
    for at in range(0, down_w.shape[1], step):
        result = dot(hidden, down_w[:, at : at + step])
        for c in range(step // LANES):
            wide[pl.ds(at // LANES + c, count, stride=TILE), :] = result[:, column(c)]
    left = []
    for j in range(chunks):
        out[j * share : (j + 1) * share, :] = wide[j * share : (j + 1) * share, :].astype(BF16)
        at = pl.ds(j * share, share)
        left.append(pltpu.make_async_copy(out.at[at], out_hbm.at[at], out_sems.at[j]))
        left[-1].start()
    for copy in left:
        copy.wait()


def turn_matrix():
    row = lax.broadcasted_iota(jnp.int32, (LANES, LANES), 0)
    col = lax.broadcasted_iota(jnp.int32, (LANES, LANES), 1)
    return row, col


def rotated(x, cosine, sine, half):
    row, col = turn_matrix()
    first = col % (2 * half) < half
    partner = jnp.where(first, col + half, col - half)
    turn = jnp.where(row == partner, jnp.where(first, -1.0, 1.0), 0.0).astype(BF16)
    return x.astype(F32) * cosine + dot(x, turn) * sine


def lower(size, strict=False):
    row = lax.broadcasted_iota(jnp.int32, (size, size), 0)
    col = lax.broadcasted_iota(jnp.int32, (size, size), 1)
    return row > col if strict else row >= col


def summed_f32(a, b, dims):
    return lax.dot_general(
        a, b, (dims, ((), ())), preferred_element_type=F32, precision=lax.Precision.HIGHEST
    )


def spread_heads(per_head, key_size):
    lane = lax.broadcasted_iota(jnp.int32, (per_head.shape[0], LANES), 1)
    out = per_head[:, 0:1]
    for h in range(1, per_head.shape[1]):
        out = jnp.where(lane >= h * key_size, per_head[:, h : h + 1], out)
    return out


def state_kernel(k, v, log_decay, cosine, sine, packed):
    heads = log_decay.shape[0]
    key_size = k.shape[1] // heads
    value_size = v.shape[1] // heads
    span = k.shape[0]
    k_rot = (rotated(k[...], cosine[...], sine[...], key_size // 2) * key_size ** (-0.5)).astype(
        BF16
    )
    above = jnp.where(lower(BLOCK, True), 1.0, 0.0)
    after = jnp.zeros((1, heads), F32)
    tails = [None] * (span // BLOCK)
    for b in reversed(range(span // BLOCK)):
        part = log_decay[:, b * BLOCK : (b + 1) * BLOCK]
        tails[b] = summed_f32(above, part, ((0,), (1,))) + after
        after = after + summed_f32(jnp.ones((1, BLOCK), F32), part, ((1,), (1,)))
    tail = jnp.concatenate(tails, axis=0)
    faded = (k_rot.astype(F32) * jnp.exp(spread_heads(tail, key_size))).astype(BF16)
    state = dot(faded.T, v[...])
    for h in range(heads):
        packed[h * STATE_ROWS : h * STATE_ROWS + key_size, :] = state[
            h * key_size : (h + 1) * key_size, h * value_size : (h + 1) * value_size
        ].astype(BF16)
        whole = after[:, h : h + 1]
        high = whole.astype(BF16)
        low = (whole - high.astype(F32)).astype(BF16)
        pad = STATE_ROWS - key_size
        row = lax.broadcasted_iota(jnp.int32, (pad, LANES), 0)
        packed[h * STATE_ROWS + key_size : (h + 1) * STATE_ROWS, :] = jnp.where(
            row == 0, high.astype(F32), low.astype(F32)
        ).astype(BF16)


def retention_kernel(seat, q, k, v, gate, log_decay, cosine, sine, state_in, w_out, *rest):
    own, *outs, gated = rest
    heads = log_decay.shape[0]
    key_size = q.shape[1] // heads
    value_size = v.shape[1] // heads
    span = q.shape[0]
    q_rot = rotated(q[...], cosine[...], sine[...], key_size // 2).astype(BF16)
    k_rot = (rotated(k[...], cosine[...], sine[...], key_size // 2) * key_size ** (-0.5)).astype(
        BF16
    )
    keep = lower(BLOCK)
    ones = jnp.where(keep, 1.0, 0.0)
    lane = lax.broadcasted_iota(jnp.int32, (BLOCK, LANES), 1)
    state = state_in[...]
    for b in range(span // BLOCK):
        at = slice(b * BLOCK, (b + 1) * BLOCK)
        part = log_decay[:, at]
        column = summed_f32(ones, part, ((1,), (1,)))
        across = summed_f32(part, ones, ((1,), (1,)))
        total = column[BLOCK - 1 : BLOCK, :]
        q_part = q_rot[at, :]
        k_part = k_rot[at, :]
        v_part = v[at, :]
        lifted = q_part.astype(F32) * jnp.exp(spread_heads(column, key_size))
        tail = jnp.exp(spread_heads(total - column, key_size))
        faded = (k_part.astype(F32) * tail).astype(BF16)
        held = state.astype(BF16)
        grown = dot(faded.T, v_part)
        fade = []
        for h in range(heads):
            mine = (lane >= h * key_size) & (lane < (h + 1) * key_size)
            q_head = jnp.where(mine, q_part.astype(F32), 0.0).astype(BF16)
            scores = lax.dot_general(
                q_head, k_part, (((1,), (1,)), ((), ())), preferred_element_type=F32
            )
            gap = jnp.where(keep, column[:, h : h + 1] - across[h : h + 1, :], 0.0)
            weights = jnp.where(keep, scores * jnp.exp(gap), 0.0).astype(BF16)
            columns = slice(h * value_size, (h + 1) * value_size)
            kept = dot(weights, v_part[:, columns]) + dot(
                jnp.where(mine, lifted, 0.0).astype(BF16), held
            )
            center = jnp.mean(kept, axis=-1, keepdims=True)
            off = kept - center
            spread = jnp.mean(off * off, axis=-1, keepdims=True)
            act = jax.nn.silu(gate[at, columns].astype(F32))
            gated[at, columns] = (act * (off * lax.rsqrt(spread + GROUP_EPS))).astype(BF16)
            fade.append(
                state[h * key_size : (h + 1) * key_size, :] * jnp.exp(total[:, h : h + 1])
                + grown[h * key_size : (h + 1) * key_size, columns]
            )
        state = jnp.concatenate(fade, axis=0)
    count = len(outs) + 1
    share = span // count
    for d in range(count):
        first = lax.rem(seat[0] + d, count) * share
        part = gated[pl.ds(pl.multiple_of(first, share), share), :]
        if d == 0:
            own[...] = dot(part, w_out[...]).astype(BF16)
        else:
            outs[d - 1][...] = part


def pack_kernel(core, gate_w, up_w, down_w, w_out, whole, half, out_half):
    def fill(to, first, depth, cut, thin):
        to[0:depth, :] = gate_w[pl.ds(first, depth), :]
        to[depth : 2 * depth, :] = up_w[pl.ds(first, depth), :]
        for k in range(down_w.shape[1] // LANES):
            at = 2 * depth + k * thin
            to[at : at + thin, :] = down_w[pl.ds(cut, thin), k * LANES : (k + 1) * LANES]

    depth, thin = gate_w.shape[0], down_w.shape[0]
    fill(whole, 0, depth, 0, thin)
    at = pl.multiple_of(core[0] * (depth // 2), TILE)
    cut = pl.multiple_of(core[0] * (thin // 2), TILE)
    fill(half, at, depth // 2, cut, thin // 2)
    share = out_half.shape[0]
    out_half[...] = w_out[pl.ds(pl.multiple_of(core[0] * share, TILE), share), :]


def shared_kernel(core, normed, own, near, near_other, mine, theirs, out, packed, down):
    rows = normed[...]
    depth = rows.shape[1]
    total = None
    for part in (own, near, near_other):
        hidden = jax.nn.silu(dot(rows, part[0:depth, :])) * dot(rows, part[depth : 2 * depth, :])
        thin = down.shape[0]
        for k in range(down.shape[1] // LANES):
            at = 2 * depth + k * thin
            down[:, k * LANES : (k + 1) * LANES] = part[at : at + thin, :]
        product = dot(hidden.astype(BF16), down[...])
        total = product if total is None else total + product
    packed[0] = jnp.where(core[0] == 0, mine[...], theirs[...])
    packed[1] = jnp.where(core[0] == 0, theirs[...], mine[...])
    half = depth // 2
    thin = down.shape[0] // 2
    gated = dot(rows[:, :half], packed[0, :half]) + dot(rows[:, half:], packed[1, :half])
    up = dot(rows[:, :half], packed[0, half:depth]) + dot(rows[:, half:], packed[1, half:depth])
    for c in range(2):
        for k in range(down.shape[1] // LANES):
            at = depth + k * thin
            down[c * thin : (c + 1) * thin, k * LANES : (k + 1) * LANES] = packed[c, at : at + thin]
    hidden = (jax.nn.silu(gated) * up).astype(BF16)
    out[...] = total + dot(hidden, down[...])


def finish_kernel(
    places,
    core,
    returned,
    weight,
    own,
    gated_left,
    gated_right,
    gated_far,
    shared_hbm,
    near_hbm,
    other_hbm,
    mine_hbm,
    theirs_hbm,
    mixer_out,
    moe_out,
    picked,
    shared,
    near,
    other,
    far,
    sems,
):
    share = far.shape[1]
    pairs = (
        (shared_hbm, shared),
        (near_hbm, near),
        (other_hbm, other),
        (mine_hbm, far.at[0]),
        (theirs_hbm, far.at[1]),
    )
    copies = [pltpu.make_async_copy(a, b, sems.at[i]) for i, (a, b) in enumerate(pairs)]
    for copy in copies:
        copy.start()
    number = moe_out.shape[0]
    top = weight.shape[1]

    @pl.loop(0, number, unroll=8)
    def _(n):
        for k in range(top):
            place = places[k, n]
            picked[k, pl.ds(pl.multiple_of(n * TILE, TILE), TILE), :] = returned[
                pl.ds(pl.multiple_of(place * TILE, TILE), TILE), :
            ].astype(F32)

    copies[0].wait()
    for c in range(TILE):
        total = shared[:, column(c)]
        for k in range(top):
            total = total + picked[k, pl.ds(c, number, stride=TILE), :] * weight[:, k : k + 1]
        moe_out[:, column(c)] = total.astype(BF16)
    for copy in copies[1:]:
        copy.wait()
    first = core[0] == 0
    left, right, across = gated_left[...], gated_right[...], gated_far[...]
    mixed = own[...].astype(F32)
    mixed = mixed + dot(jnp.where(first, left, right), near[...])
    mixed = mixed + dot(jnp.where(first, right, left), other[...])
    low, high = across[:, :share], across[:, share:]
    mixed = mixed + dot(jnp.where(first, low, high), far[0])
    mixed = mixed + dot(jnp.where(first, high, low), far[1])
    mixer_out[...] = mixed.astype(BF16)


def moved_by(array, axis, step):
    count = lax.axis_size(axis)
    return lax.ppermute(array, axis, [(s, (s + step) % count) for s in range(count)])


def outward(array):
    count = lax.axis_size("tp")
    pairs = [(s, (s + 1) % count) for s in range(count)]
    pairs += [(count + s, count + (s - 1) % count) for s in range(count)]
    return lax.ppermute(array, ("ep_1", "tp"), pairs)


def opened(packed):
    wide = packed.astype(F32)
    size = STATE_ROWS - TILE
    return wide[size : size + 1, :] + wide[size + 1 : size + 2, :], wide[:size, :]


def closed(part):
    log, state = part
    high = log.astype(BF16).astype(F32)
    row = lax.broadcasted_iota(jnp.int32, (TILE, LANES), 0)
    return jnp.concatenate([state, jnp.where(row == 0, high, log - high)], axis=0).astype(BF16)


def joined(earlier, later):
    return earlier[0] + later[0], earlier[1] * jnp.exp(later[0]) + later[1]


def picked_by(core, a, b):
    return jnp.where(core == 0, a.astype(F32), b.astype(F32)).astype(BF16)


def chip_kernel(core, own, other, out):
    mine = picked_by(core[0], own[:STATE_ROWS, :], own[STATE_ROWS:, :])
    theirs = picked_by(core[0], other[:STATE_ROWS, :], other[STATE_ROWS:, :])
    early, late = picked_by(core[0], mine, theirs), picked_by(core[0], theirs, mine)
    out[...] = closed(joined(opened(early), opened(late)))


def near_kernel(seat, chip, *refs):
    *near, before, window = refs
    count = len(near) + 1
    found = [chip[...].astype(F32)] + [part[...].astype(F32) for part in near]
    start = whole = None
    for p in range(count):
        back = lax.rem(seat[0] + count - p, count)
        part = found[0]
        for d in range(1, count):
            part = jnp.where(back == d, found[d], part)
        item = opened(part)
        early = opened(jnp.where(seat[0] > p, part, 0.0))
        start = early if start is None else joined(start, early)
        whole = item if whole is None else joined(whole, item)
    before[...] = closed(start)
    packed = closed(whole)
    for p in range(window.shape[0] // STATE_ROWS):
        window[p * STATE_ROWS : (p + 1) * STATE_ROWS, :] = packed


def far_kernel(seat, before, window, prefix):
    start = None
    for p in range(window.shape[0] // STATE_ROWS):
        part = window[p * STATE_ROWS : (p + 1) * STATE_ROWS, :].astype(F32)
        early = opened(jnp.where(seat[0] > p, part, 0.0))
        start = early if start is None else joined(start, early)
    prefix[...] = closed(joined(start, opened(before[...])))


def enter_kernel(core, mine, theirs, other, state):
    size = STATE_ROWS - TILE
    for h in range(other.shape[0] // STATE_ROWS):
        held = jnp.where(core[0] == h, mine[...].astype(F32), theirs[...].astype(F32))
        chip_before = opened(held)
        first = opened(other[h * STATE_ROWS : (h + 1) * STATE_ROWS, :])
        both = joined(chip_before, first)
        state[h * size : (h + 1) * size, :] = jnp.where(core[0] == 0, chip_before[1], both[1])


def small(kernel, outs, in_specs, out_specs):
    return call(kernel, outs, in_specs, out_specs, [], 100000, 100000, 2)


def per_device(
    queries,
    keys,
    values,
    gate,
    log_decay,
    w_out,
    moe_input,
    moe_gain,
    routes,
    route_weight,
    expert_gate,
    expert_up,
    expert_down,
    shared_gate,
    shared_up,
    shared_down,
):
    span = queries.shape[0]
    heads = log_decay.shape[1]
    key_size = queries.shape[1] // heads
    value_size = values.shape[1] // heads
    rows_dev, width = moe_input.shape
    top = routes.shape[1]
    n_tp = lax.axis_size("tp")
    experts = lax.axis_size(EP) * n_tp
    capacity = rows_dev * top * 3 // (2 * experts)
    hidden_size = expert_gate.shape[2]
    shared_size = shared_gate.shape[1]
    slots = experts * capacity
    tile_rows = slots * TILE

    core = lax.axis_index("ep_1").reshape(1).astype(jnp.int32)
    seat = lax.axis_index("tp").reshape(1).astype(jnp.int32)
    around = range(1, n_tp)
    half_out = w_out.shape[0] // 2
    packed_shape = jax.ShapeDtypeStruct((STATE_ROWS, value_size), BF16)

    out_near = outward(w_out)

    normed, outbound, places = call(
        prep_kernel,
        (
            jax.ShapeDtypeStruct((rows_dev, width), BF16),
            jax.ShapeDtypeStruct((tile_rows, LANES), BF16),
            jax.ShapeDtypeStruct((top, rows_dev), jnp.int32),
        ),
        [SMEM, HBM, HBM],
        (HBM, VMEM, SMEM),
        [
            pltpu.VMEM((rows_dev, width), BF16),
            pltpu.VMEM((1, width), F32),
            pltpu.VMEM((rows_dev, width), BF16),
            pltpu.VMEM((rows_dev * TILE, LANES), F32),
            pltpu.SMEM((experts,), jnp.int32),
            pltpu.SemaphoreType.DMA((3,)),
        ],
        2 * rows_dev * width * 256,
        4 * rows_dev * width,
        62,
    )(routes.T, moe_input, moe_gain.reshape(1, width))

    arrived = lax.all_to_all(
        outbound.reshape(experts, capacity * TILE, LANES),
        EP_TP,
        split_axis=0,
        concat_axis=0,
        tiled=True,
    )

    half = key_size // 2
    frequency = ROPE_BASE ** (-jnp.arange(half, dtype=F32) / half)
    spots = lax.axis_index(EP) * span + jnp.arange(span, dtype=jnp.int32)
    angles = spots.astype(F32)[:, None] * jnp.tile(frequency, LANES // half)[None, :]
    cosine = jnp.cos(angles)
    sine = jnp.sin(angles)

    own = call(
        state_kernel,
        jax.ShapeDtypeStruct((heads * STATE_ROWS, value_size), BF16),
        [VMEM] * 5,
        VMEM,
        [],
        2 * span * LANES * 512,
        4 * span * LANES * 4,
        12,
    )(keys, values, log_decay.T, cosine, sine)
    other = moved_by(own, "ep_1", 1)
    chip = small(chip_kernel, packed_shape, [SMEM, VMEM, VMEM], VMEM)(core, own, other)
    low_seat = lax.axis_index("ep_lo").reshape(1).astype(jnp.int32)
    high_seat = lax.axis_index("ep_hi").reshape(1).astype(jnp.int32)
    groups = lax.axis_size("ep_hi")
    near = [moved_by(chip, "ep_lo", d) for d in range(1, lax.axis_size("ep_lo"))]
    window_shape = jax.ShapeDtypeStruct((groups * STATE_ROWS, value_size), BF16)
    before, window = small(
        near_kernel, (packed_shape, window_shape), [SMEM] + [VMEM] * (1 + len(near)), (VMEM, VMEM)
    )(low_seat, chip, *near)
    far = lax.all_to_all(
        window.reshape(groups, STATE_ROWS, value_size),
        "ep_hi",
        split_axis=0,
        concat_axis=0,
        tiled=True,
    )
    prefix = small(far_kernel, packed_shape, [SMEM] + [VMEM] * 2, VMEM)(
        high_seat, before, far.reshape(groups * STATE_ROWS, value_size)
    )
    swapped = moved_by(prefix, "ep_1", 1)
    state_in = small(
        enter_kernel,
        jax.ShapeDtypeStruct((heads * key_size, value_size), F32),
        [SMEM] + [VMEM] * 3,
        VMEM,
    )(core, prefix, swapped, other)

    pack_rows = width * 3 * shared_size // LANES
    shared_own, shared_half, out_half = call(
        pack_kernel,
        (
            jax.ShapeDtypeStruct((pack_rows, LANES), BF16),
            jax.ShapeDtypeStruct((pack_rows // 2, LANES), BF16),
            jax.ShapeDtypeStruct((half_out, width), BF16),
        ),
        [SMEM] + [VMEM] * 4,
        (VMEM,) * 3,
        [],
        100000,
        6 * width * shared_size,
        16,
    )(core, shared_gate, shared_up, shared_down, w_out)
    shared_near = outward(shared_own)
    shared_mine = moved_by(shared_half, "tp", 2)
    out_mine = moved_by(out_half, "tp", 2)
    shared_other, shared_theirs, out_other, out_theirs = [
        moved_by(part, "ep_1", 1) for part in (shared_near, shared_mine, out_near, out_mine)
    ]
    shared_sum = call(
        shared_kernel,
        jax.ShapeDtypeStruct((rows_dev, width), F32),
        [SMEM] + [VMEM] * 6,
        VMEM,
        [
            pltpu.VMEM((2,) + shared_half.shape, BF16),
            pltpu.VMEM((shared_size, width), BF16),
        ],
        2 * n_tp * rows_dev * width * shared_size * 3,
        10 * rows_dev * width * 2,
        20,
    )(core, normed, shared_own, shared_near, shared_other, shared_mine, shared_theirs)

    pieces, chunks = 4, 3
    answers = call(
        expert_kernel,
        jax.ShapeDtypeStruct((tile_rows, LANES), BF16),
        [HBM] * 4,
        HBM,
        [
            pltpu.VMEM((width, hidden_size), BF16),
            pltpu.VMEM((width, hidden_size), BF16),
            pltpu.VMEM((hidden_size, width), BF16),
            pltpu.VMEM((slots, width), BF16),
            pltpu.VMEM((tile_rows, LANES), BF16),
            pltpu.VMEM((tile_rows, LANES), F32),
            pltpu.VMEM((tile_rows, LANES), BF16),
            pltpu.SemaphoreType.DMA((3, pieces)),
            pltpu.SemaphoreType.DMA((chunks,)),
            pltpu.SemaphoreType.DMA((chunks,)),
        ],
        2 * slots * width * hidden_size * 3,
        3 * 2 * width * hidden_size,
        62,
    )(arrived.reshape(tile_rows, LANES), expert_gate, expert_up, expert_down)
    returned = lax.all_to_all(
        answers.reshape(experts, capacity * TILE, LANES),
        EP_TP,
        split_axis=0,
        concat_axis=0,
        tiled=True,
    )

    gated_shape = jax.ShapeDtypeStruct((rows_dev, heads * value_size), BF16)
    own_mixed, *gated = call(
        retention_kernel,
        (jax.ShapeDtypeStruct((rows_dev, width), BF16),) + (gated_shape,) * (n_tp - 1),
        [SMEM] + [VMEM] * 9,
        (VMEM,) * n_tp,
        [pltpu.VMEM((span, heads * value_size), BF16)],
        2 * span * heads * value_size * 1000,
        10 * rows_dev * width * 2,
        20,
    )(seat, queries, keys, values, gate, log_decay.T, cosine, sine, state_in, w_out)
    gated_left, gated_far, gated_right = [moved_by(gated[d - 1], "tp", d) for d in around]

    return call(
        finish_kernel,
        tuple(jax.ShapeDtypeStruct((rows_dev, width), BF16) for _ in range(2)),
        [SMEM, SMEM] + [VMEM] * 6 + [HBM] * 5,
        (VMEM,) * 2,
        [
            pltpu.VMEM((top, rows_dev * TILE, LANES), F32),
            pltpu.VMEM((rows_dev, width), F32),
            pltpu.VMEM((2 * half_out, width), BF16),
            pltpu.VMEM((2 * half_out, width), BF16),
            pltpu.VMEM((2, half_out, width), BF16),
            pltpu.SemaphoreType.DMA((5,)),
        ],
        2 * rows_dev * width * 1500,
        10 * rows_dev * width * 2,
        28,
    )(
        places,
        core,
        returned.reshape(tile_rows, LANES),
        route_weight,
        own_mixed,
        gated_left,
        gated_right,
        gated_far,
        shared_sum,
        out_near,
        out_other,
        out_mine,
        out_theirs,
    )


def solution(mesh):
    split = Mesh(
        mesh.devices.reshape(
            mesh.shape["grp"], mesh.shape["ep"] // (2 * CHIPS), CHIPS, 2, mesh.shape["tp"]
        ),
        GRP_EP_TP,
    )
    return jax.shard_map(
        per_device,
        mesh=split,
        in_specs=(
            P(GRP_EP, "tp"),
            P(GRP_EP, "tp"),
            P(GRP_EP, "tp"),
            P(GRP_EP, "tp"),
            P(GRP_EP, "tp"),
            P("tp", None),
            P(GRP_EP_TP, None),
            P(),
            P(GRP_EP_TP, None),
            P(GRP_EP_TP, None),
            P(EP_TP, None, None),
            P(EP_TP, None, None),
            P(EP_TP, None, None),
            P(None, "tp"),
            P(None, "tp"),
            P("tp", None),
        ),
        out_specs=(P(GRP_EP_TP, None), P(GRP_EP_TP, None)),
        check_vma=False,
    )
```

```python
import jax
import jax.numpy as jnp
from jax import lax
from jax.experimental import pallas as pl
from jax.experimental.pallas import tpu as pltpu
from jax.sharding import Mesh
from jax.sharding import PartitionSpec as P


BLOCK = 128
LANES = 128
TILE = 16
CHIPS = 4
EP = ("ep_hi", "ep_lo", "ep_1")
EP_TP = EP + ("tp",)
GRP_EP = ("grp",) + EP
GRP_EP_TP = ("grp",) + EP_TP
STATE_ROWS = 80

ROPE_BASE = 10000.0
GROUP_EPS = 1e-05
NORM_EPS = 1e-06


VMEM = pl.BlockSpec(memory_space=pltpu.VMEM)
SMEM = pl.BlockSpec(memory_space=pltpu.SMEM)
HBM = pl.BlockSpec(memory_space=pltpu.HBM)
F32 = jnp.float32
BF16 = jnp.bfloat16
MIB = 1 << 20


def call(kernel, out_shape, in_specs, out_specs, scratch, flops, moved, limit):
    return pl.pallas_call(
        kernel,
        out_shape=out_shape,
        in_specs=in_specs,
        out_specs=out_specs,
        scratch_shapes=scratch,
        compiler_params=pltpu.CompilerParams(vmem_limit_bytes=int(limit * MIB)),
        cost_estimate=pl.CostEstimate(flops=flops, bytes_accessed=moved, transcendentals=0),
    )


def dot(a, b):
    return jnp.dot(a, b, preferred_element_type=F32)


def swap_matrix():
    side = TILE * TILE
    row = lax.broadcasted_iota(jnp.int32, (side, side), 0)
    col = lax.broadcasted_iota(jnp.int32, (side, side), 1)
    hit = (row // TILE == col % TILE) & (row % TILE == col // TILE)
    return jnp.where(hit, 1.0, 0.0).astype(BF16)


def rows_to_tiles(swap, rows):
    count = rows.shape[0] // TILE
    width = rows.shape[1] // LANES
    found = []
    for at in range(0, count, 2):
        pair = [
            jnp.concatenate(
                [
                    rows[g * TILE : (g + 1) * TILE, k * LANES : (k + 1) * LANES]
                    for k in range(width)
                ],
                axis=0,
            )
            for g in range(at, min(at + 2, count))
        ]
        out = dot(swap, jnp.concatenate(pair, axis=1)).astype(BF16)
        found += [out[:, g * LANES : (g + 1) * LANES] for g in range(len(pair))]
    return found


def column(c):
    return slice(c * LANES, (c + 1) * LANES)


def prep_kernel(
    routes, x_hbm, gain_hbm, normed_hbm, outbound, places, x, gain, normed, tiles, used, sems
):
    copies = [
        pltpu.make_async_copy(x_hbm, x, sems.at[0]),
        pltpu.make_async_copy(gain_hbm, gain, sems.at[1]),
    ]
    for copy in copies:
        copy.start()
    outbound[...] = jnp.zeros_like(outbound)
    top, number = routes.shape
    experts = used.shape[0]
    capacity = outbound.shape[0] // (experts * TILE)
    for e in range(experts):
        used[e] = 0

    @pl.loop(0, number, unroll=8)
    def _(n):
        for k in range(top):
            e = routes[k, n]
            rank = used[e]
            used[e] = rank + 1
            places[k, n] = e * capacity + rank

    for copy in copies:
        copy.wait()
    source = x[...].astype(F32)
    scale = lax.rsqrt(jnp.mean(source * source, axis=-1, keepdims=True) + NORM_EPS)
    rows = (source * scale * gain[...]).astype(BF16)
    normed[...] = rows
    keep = pltpu.make_async_copy(normed, normed_hbm, sems.at[2])
    keep.start()
    wide = rows.astype(F32)
    for c in range(TILE):
        tiles[pl.ds(c, number, stride=TILE), :] = wide[:, column(c)]

    @pl.loop(0, number, unroll=8)
    def _(n):
        row = tiles[pl.ds(pl.multiple_of(n * TILE, TILE), TILE), :].astype(BF16)
        for k in range(top):
            at = pl.multiple_of(places[k, n] * TILE, TILE)
            outbound[pl.ds(at, TILE), :] = row

    keep.wait()


def expert_kernel(
    arrived_hbm,
    gate_hbm,
    up_hbm,
    down_hbm,
    out_hbm,
    gate_w,
    up_w,
    down_w,
    rows,
    arrived,
    out,
    sems,
    in_sems,
    out_sems,
):
    pieces = sems.shape[1]
    chunks = out_sems.shape[0]
    share = arrived.shape[0] // chunks
    landed = []
    for j in range(chunks):
        at = pl.ds(j * share, share)
        landed.append(pltpu.make_async_copy(arrived_hbm.at[at], arrived.at[at], in_sems.at[j]))
        landed[-1].start()
    copies = [[], [], []]
    for i, (src, dst) in enumerate(((gate_hbm, gate_w), (up_hbm, up_w), (down_hbm, down_w))):
        part = dst.shape[0] // pieces
        for j in range(pieces):
            at = pl.ds(j * part, part)
            copies[i].append(pltpu.make_async_copy(src.at[0, at], dst.at[at], sems.at[i, j]))
    swap = swap_matrix()
    side = TILE * TILE
    groups = arrived.shape[0] // side
    for at in range(0, groups, 2):
        if at * side % share == 0:
            landed[at * side // share].wait()
            for copy in copies[at * side // share]:
                copy.start()
        pair = jnp.concatenate(
            [arrived[g * side : (g + 1) * side, :] for g in (at, at + 1)], axis=1
        )
        turned = dot(swap, pair).astype(BF16)
        for j in range(2):
            for k in range(TILE):
                rows[
                    (at + j) * TILE : (at + j + 1) * TILE, k * LANES : (k + 1) * LANES
                ] = turned[k * TILE : (k + 1) * TILE, j * LANES : (j + 1) * LANES]
    for copy in copies[0]:
        copy.wait()
    gated = jax.nn.silu(dot(rows[...], gate_w[...]))
    for copy in copies[1]:
        copy.wait()
    hidden = (gated * dot(rows[...], up_w[...])).astype(BF16)
    for copy in copies[2]:
        copy.wait()
    left = []
    step = rows.shape[0] // chunks
    for at in range(0, down_w.shape[1], 4 * LANES):
        rows[:, at : at + 4 * LANES] = dot(hidden, down_w[:, at : at + 4 * LANES]).astype(BF16)
    for j in range(chunks):
        for g, tile in enumerate(rows_to_tiles(swap, rows[j * step : (j + 1) * step, :])):
            out[j * share + g * side : j * share + (g + 1) * side, :] = tile
        at = pl.ds(j * share, share)
        left.append(pltpu.make_async_copy(out.at[at], out_hbm.at[at], out_sems.at[j]))
        left[-1].start()
    for copy in left:
        copy.wait()


def turn_matrix():
    row = lax.broadcasted_iota(jnp.int32, (LANES, LANES), 0)
    col = lax.broadcasted_iota(jnp.int32, (LANES, LANES), 1)
    return row, col


def rotated(x, cosine, sine, half):
    row, col = turn_matrix()
    first = col % (2 * half) < half
    partner = jnp.where(first, col + half, col - half)
    turn = jnp.where(row == partner, jnp.where(first, -1.0, 1.0), 0.0).astype(BF16)
    return x.astype(F32) * cosine + dot(x, turn) * sine


def lower(size, strict=False):
    row = lax.broadcasted_iota(jnp.int32, (size, size), 0)
    col = lax.broadcasted_iota(jnp.int32, (size, size), 1)
    return row > col if strict else row >= col


def summed_f32(a, b, dims):
    return lax.dot_general(
        a, b, (dims, ((), ())), preferred_element_type=F32, precision=lax.Precision.HIGHEST
    )


def spread_heads(per_head, key_size):
    lane = lax.broadcasted_iota(jnp.int32, (per_head.shape[0], LANES), 1)
    out = per_head[:, 0:1]
    for h in range(1, per_head.shape[1]):
        out = jnp.where(lane >= h * key_size, per_head[:, h : h + 1], out)
    return out


def state_kernel(k, v, log_decay, cosine, sine, packed):
    heads = log_decay.shape[0]
    key_size = k.shape[1] // heads
    value_size = v.shape[1] // heads
    span = k.shape[0]
    k_rot = (rotated(k[...], cosine[...], sine[...], key_size // 2) * key_size ** (-0.5)).astype(
        BF16
    )
    above = jnp.where(lower(BLOCK, True), 1.0, 0.0)
    after = jnp.zeros((1, heads), F32)
    tails = [None] * (span // BLOCK)
    for b in reversed(range(span // BLOCK)):
        part = log_decay[:, b * BLOCK : (b + 1) * BLOCK]
        tails[b] = summed_f32(above, part, ((0,), (1,))) + after
        after = after + summed_f32(jnp.ones((1, BLOCK), F32), part, ((1,), (1,)))
    tail = jnp.concatenate(tails, axis=0)
    faded = (k_rot.astype(F32) * jnp.exp(spread_heads(tail, key_size))).astype(BF16)
    state = dot(faded.T, v[...])
    for h in range(heads):
        packed[h * STATE_ROWS : h * STATE_ROWS + key_size, :] = state[
            h * key_size : (h + 1) * key_size, h * value_size : (h + 1) * value_size
        ].astype(BF16)
        whole = after[:, h : h + 1]
        high = whole.astype(BF16)
        low = (whole - high.astype(F32)).astype(BF16)
        pad = STATE_ROWS - key_size
        row = lax.broadcasted_iota(jnp.int32, (pad, LANES), 0)
        packed[h * STATE_ROWS + key_size : (h + 1) * STATE_ROWS, :] = jnp.where(
            row == 0, high.astype(F32), low.astype(F32)
        ).astype(BF16)


def retention_kernel(seat, q, k, v, gate, log_decay, cosine, sine, state_in, w_out, *rest):
    own, *outs, gated = rest
    heads = log_decay.shape[0]
    key_size = q.shape[1] // heads
    value_size = v.shape[1] // heads
    span = q.shape[0]
    q_rot = rotated(q[...], cosine[...], sine[...], key_size // 2).astype(BF16)
    k_rot = (rotated(k[...], cosine[...], sine[...], key_size // 2) * key_size ** (-0.5)).astype(
        BF16
    )
    keep = lower(BLOCK)
    ones = jnp.where(keep, 1.0, 0.0)
    lane = lax.broadcasted_iota(jnp.int32, (BLOCK, LANES), 1)
    state = state_in[...]
    for b in range(span // BLOCK):
        at = slice(b * BLOCK, (b + 1) * BLOCK)
        part = log_decay[:, at]
        column = summed_f32(ones, part, ((1,), (1,)))
        across = summed_f32(part, ones, ((1,), (1,)))
        total = column[BLOCK - 1 : BLOCK, :]
        q_part = q_rot[at, :]
        k_part = k_rot[at, :]
        v_part = v[at, :]
        lifted = q_part.astype(F32) * jnp.exp(spread_heads(column, key_size))
        tail = jnp.exp(spread_heads(total - column, key_size))
        faded = (k_part.astype(F32) * tail).astype(BF16)
        held = state.astype(BF16)
        grown = dot(faded.T, v_part)
        fade = []
        for h in range(heads):
            mine = (lane >= h * key_size) & (lane < (h + 1) * key_size)
            q_head = jnp.where(mine, q_part.astype(F32), 0.0).astype(BF16)
            scores = lax.dot_general(
                q_head, k_part, (((1,), (1,)), ((), ())), preferred_element_type=F32
            )
            gap = jnp.where(keep, column[:, h : h + 1] - across[h : h + 1, :], 0.0)
            weights = jnp.where(keep, scores * jnp.exp(gap), 0.0).astype(BF16)
            columns = slice(h * value_size, (h + 1) * value_size)
            kept = dot(weights, v_part[:, columns]) + dot(
                jnp.where(mine, lifted, 0.0).astype(BF16), held
            )
            center = jnp.mean(kept, axis=-1, keepdims=True)
            off = kept - center
            spread = jnp.mean(off * off, axis=-1, keepdims=True)
            act = jax.nn.silu(gate[at, columns].astype(F32))
            gated[at, columns] = (act * (off * lax.rsqrt(spread + GROUP_EPS))).astype(BF16)
            fade.append(
                state[h * key_size : (h + 1) * key_size, :] * jnp.exp(total[:, h : h + 1])
                + grown[h * key_size : (h + 1) * key_size, columns]
            )
        state = jnp.concatenate(fade, axis=0)
    count = len(outs) + 1
    share = span // count
    for d in range(count):
        first = lax.rem(seat[0] + d, count) * share
        part = gated[pl.ds(pl.multiple_of(first, share), share), :]
        if d == 0:
            own[...] = dot(part, w_out[...]).astype(BF16)
        else:
            outs[d - 1][...] = part


def pack_kernel(core, gate_w, up_w, down_w, w_out, whole, half, out_half):
    def fill(to, first, depth, cut, thin):
        to[0:depth, :] = gate_w[pl.ds(first, depth), :]
        to[depth : 2 * depth, :] = up_w[pl.ds(first, depth), :]
        for k in range(down_w.shape[1] // LANES):
            at = 2 * depth + k * thin
            to[at : at + thin, :] = down_w[pl.ds(cut, thin), k * LANES : (k + 1) * LANES]

    depth, thin = gate_w.shape[0], down_w.shape[0]
    fill(whole, 0, depth, 0, thin)
    at = pl.multiple_of(core[0] * (depth // 2), TILE)
    cut = pl.multiple_of(core[0] * (thin // 2), TILE)
    fill(half, at, depth // 2, cut, thin // 2)
    share = out_half.shape[0]
    out_half[...] = w_out[pl.ds(pl.multiple_of(core[0] * share, TILE), share), :]


def shared_kernel(core, normed, own, near, near_other, mine, theirs, out, packed, down):
    rows = normed[...]
    depth = rows.shape[1]
    total = None
    for part in (own, near, near_other):
        hidden = jax.nn.silu(dot(rows, part[0:depth, :])) * dot(rows, part[depth : 2 * depth, :])
        thin = down.shape[0]
        for k in range(down.shape[1] // LANES):
            at = 2 * depth + k * thin
            down[:, k * LANES : (k + 1) * LANES] = part[at : at + thin, :]
        product = dot(hidden.astype(BF16), down[...])
        total = product if total is None else total + product
    packed[0] = jnp.where(core[0] == 0, mine[...], theirs[...])
    packed[1] = jnp.where(core[0] == 0, theirs[...], mine[...])
    half = depth // 2
    thin = down.shape[0] // 2
    gated = dot(rows[:, :half], packed[0, :half]) + dot(rows[:, half:], packed[1, :half])
    up = dot(rows[:, :half], packed[0, half:depth]) + dot(rows[:, half:], packed[1, half:depth])
    for c in range(2):
        for k in range(down.shape[1] // LANES):
            at = depth + k * thin
            down[c * thin : (c + 1) * thin, k * LANES : (k + 1) * LANES] = packed[c, at : at + thin]
    hidden = (jax.nn.silu(gated) * up).astype(BF16)
    out[...] = total + dot(hidden, down[...])


def finish_kernel(
    places,
    core,
    returned,
    weight,
    own,
    gated_left,
    gated_right,
    gated_far,
    shared_hbm,
    near_hbm,
    other_hbm,
    mine_hbm,
    theirs_hbm,
    mixer_out,
    moe_out,
    picked,
    shared,
    near,
    other,
    far,
    sems,
):
    share = far.shape[1]
    pairs = (
        (shared_hbm, shared),
        (near_hbm, near),
        (other_hbm, other),
        (mine_hbm, far.at[0]),
        (theirs_hbm, far.at[1]),
    )
    copies = [pltpu.make_async_copy(a, b, sems.at[i]) for i, (a, b) in enumerate(pairs)]
    for copy in copies:
        copy.start()
    number = moe_out.shape[0]
    top = weight.shape[1]

    @pl.loop(0, number, unroll=8)
    def _(n):
        for k in range(top):
            place = places[k, n]
            picked[k, pl.ds(pl.multiple_of(n * TILE, TILE), TILE), :] = returned[
                pl.ds(pl.multiple_of(place * TILE, TILE), TILE), :
            ].astype(F32)

    copies[0].wait()
    for c in range(TILE):
        total = shared[:, column(c)]
        for k in range(top):
            total = total + picked[k, pl.ds(c, number, stride=TILE), :] * weight[:, k : k + 1]
        moe_out[:, column(c)] = total.astype(BF16)
    for copy in copies[1:]:
        copy.wait()
    first = core[0] == 0
    left, right, across = gated_left[...], gated_right[...], gated_far[...]
    mixed = own[...].astype(F32)
    mixed = mixed + dot(jnp.where(first, left, right), near[...])
    mixed = mixed + dot(jnp.where(first, right, left), other[...])
    low, high = across[:, :share], across[:, share:]
    mixed = mixed + dot(jnp.where(first, low, high), far[0])
    mixed = mixed + dot(jnp.where(first, high, low), far[1])
    mixer_out[...] = mixed.astype(BF16)


def moved_by(array, axis, step):
    count = lax.axis_size(axis)
    return lax.ppermute(array, axis, [(s, (s + step) % count) for s in range(count)])


def outward(array):
    count = lax.axis_size("tp")
    pairs = [(s, (s + 1) % count) for s in range(count)]
    pairs += [(count + s, count + (s - 1) % count) for s in range(count)]
    return lax.ppermute(array, ("ep_1", "tp"), pairs)


def opened(packed):
    wide = packed.astype(F32)
    size = STATE_ROWS - TILE
    return wide[size : size + 1, :] + wide[size + 1 : size + 2, :], wide[:size, :]


def closed(part):
    log, state = part
    high = log.astype(BF16).astype(F32)
    row = lax.broadcasted_iota(jnp.int32, (TILE, LANES), 0)
    return jnp.concatenate([state, jnp.where(row == 0, high, log - high)], axis=0).astype(BF16)


def joined(earlier, later):
    return earlier[0] + later[0], earlier[1] * jnp.exp(later[0]) + later[1]


def picked_by(core, a, b):
    return jnp.where(core == 0, a.astype(F32), b.astype(F32)).astype(BF16)


def chip_kernel(core, own, other, out):
    mine = picked_by(core[0], own[:STATE_ROWS, :], own[STATE_ROWS:, :])
    theirs = picked_by(core[0], other[:STATE_ROWS, :], other[STATE_ROWS:, :])
    early, late = picked_by(core[0], mine, theirs), picked_by(core[0], theirs, mine)
    out[...] = closed(joined(opened(early), opened(late)))


def near_kernel(seat, chip, *refs):
    *near, before, window = refs
    count = len(near) + 1
    found = [chip[...].astype(F32)] + [part[...].astype(F32) for part in near]
    start = whole = None
    for p in range(count):
        back = lax.rem(seat[0] + count - p, count)
        part = found[0]
        for d in range(1, count):
            part = jnp.where(back == d, found[d], part)
        item = opened(part)
        early = opened(jnp.where(seat[0] > p, part, 0.0))
        start = early if start is None else joined(start, early)
        whole = item if whole is None else joined(whole, item)
    before[...] = closed(start)
    window[...] = closed(whole)


def far_kernel(seat, before, *refs):
    *far, prefix = refs
    start = None
    for d in range(len(far), 0, -1):
        early = opened(jnp.where(seat[0] >= d, far[d - 1][...].astype(F32), 0.0))
        start = early if start is None else joined(start, early)
    prefix[...] = closed(joined(start, opened(before[...])))


def enter_kernel(core, mine, theirs, other, state):
    size = STATE_ROWS - TILE
    for h in range(other.shape[0] // STATE_ROWS):
        held = jnp.where(core[0] == h, mine[...].astype(F32), theirs[...].astype(F32))
        chip_before = opened(held)
        first = opened(other[h * STATE_ROWS : (h + 1) * STATE_ROWS, :])
        both = joined(chip_before, first)
        state[h * size : (h + 1) * size, :] = jnp.where(core[0] == 0, chip_before[1], both[1])


def small(kernel, outs, in_specs, out_specs):
    return call(kernel, outs, in_specs, out_specs, [], 100000, 100000, 2)


def per_device(
    queries,
    keys,
    values,
    gate,
    log_decay,
    w_out,
    moe_input,
    moe_gain,
    routes,
    route_weight,
    expert_gate,
    expert_up,
    expert_down,
    shared_gate,
    shared_up,
    shared_down,
):
    span = queries.shape[0]
    heads = log_decay.shape[1]
    key_size = queries.shape[1] // heads
    value_size = values.shape[1] // heads
    rows_dev, width = moe_input.shape
    top = routes.shape[1]
    n_tp = lax.axis_size("tp")
    experts = lax.axis_size(EP) * n_tp
    capacity = rows_dev * top * 3 // (2 * experts)
    hidden_size = expert_gate.shape[2]
    shared_size = shared_gate.shape[1]
    slots = experts * capacity
    tile_rows = slots * TILE

    core = lax.axis_index("ep_1").reshape(1).astype(jnp.int32)
    seat = lax.axis_index("tp").reshape(1).astype(jnp.int32)
    around = range(1, n_tp)
    half_out = w_out.shape[0] // 2
    packed_shape = jax.ShapeDtypeStruct((STATE_ROWS, value_size), BF16)

    out_near = outward(w_out)

    normed, outbound, places = call(
        prep_kernel,
        (
            jax.ShapeDtypeStruct((rows_dev, width), BF16),
            jax.ShapeDtypeStruct((tile_rows, LANES), BF16),
            jax.ShapeDtypeStruct((top, rows_dev), jnp.int32),
        ),
        [SMEM, HBM, HBM],
        (HBM, VMEM, SMEM),
        [
            pltpu.VMEM((rows_dev, width), BF16),
            pltpu.VMEM((1, width), F32),
            pltpu.VMEM((rows_dev, width), BF16),
            pltpu.VMEM((rows_dev * TILE, LANES), F32),
            pltpu.SMEM((experts,), jnp.int32),
            pltpu.SemaphoreType.DMA((3,)),
        ],
        2 * rows_dev * width * 256,
        4 * rows_dev * width,
        62,
    )(routes.T, moe_input, moe_gain.reshape(1, width))

    arrived = lax.all_to_all(
        outbound.reshape(experts, capacity * TILE, LANES),
        EP_TP,
        split_axis=0,
        concat_axis=0,
        tiled=True,
    )

    half = key_size // 2
    frequency = ROPE_BASE ** (-jnp.arange(half, dtype=F32) / half)
    spots = lax.axis_index(EP) * span + jnp.arange(span, dtype=jnp.int32)
    angles = spots.astype(F32)[:, None] * jnp.tile(frequency, LANES // half)[None, :]
    cosine = jnp.cos(angles)
    sine = jnp.sin(angles)

    own = call(
        state_kernel,
        jax.ShapeDtypeStruct((heads * STATE_ROWS, value_size), BF16),
        [VMEM] * 5,
        VMEM,
        [],
        2 * span * LANES * 512,
        4 * span * LANES * 4,
        12,
    )(keys, values, log_decay.T, cosine, sine)
    other = moved_by(own, "ep_1", 1)
    chip = small(chip_kernel, packed_shape, [SMEM, VMEM, VMEM], VMEM)(core, own, other)
    low_seat = lax.axis_index("ep_lo").reshape(1).astype(jnp.int32)
    high_seat = lax.axis_index("ep_hi").reshape(1).astype(jnp.int32)
    near = [moved_by(chip, "ep_lo", d) for d in range(1, lax.axis_size("ep_lo"))]
    before, window = small(
        near_kernel, (packed_shape, packed_shape), [SMEM] + [VMEM] * (1 + len(near)), (VMEM, VMEM)
    )(low_seat, chip, *near)
    far = [moved_by(window, "ep_hi", d) for d in range(1, lax.axis_size("ep_hi"))]
    prefix = small(far_kernel, packed_shape, [SMEM] + [VMEM] * (1 + len(far)), VMEM)(
        high_seat, before, *far
    )
    swapped = moved_by(prefix, "ep_1", 1)
    state_in = small(
        enter_kernel,
        jax.ShapeDtypeStruct((heads * key_size, value_size), F32),
        [SMEM] + [VMEM] * 3,
        VMEM,
    )(core, prefix, swapped, other)

    pack_rows = width * 3 * shared_size // LANES
    shared_own, shared_half, out_half = call(
        pack_kernel,
        (
            jax.ShapeDtypeStruct((pack_rows, LANES), BF16),
            jax.ShapeDtypeStruct((pack_rows // 2, LANES), BF16),
            jax.ShapeDtypeStruct((half_out, width), BF16),
        ),
        [SMEM] + [VMEM] * 4,
        (VMEM,) * 3,
        [],
        100000,
        6 * width * shared_size,
        16,
    )(core, shared_gate, shared_up, shared_down, w_out)
    shared_near = outward(shared_own)
    shared_mine = moved_by(shared_half, "tp", 2)
    out_mine = moved_by(out_half, "tp", 2)
    shared_other, shared_theirs, out_other, out_theirs = [
        moved_by(part, "ep_1", 1) for part in (shared_near, shared_mine, out_near, out_mine)
    ]
    shared_sum = call(
        shared_kernel,
        jax.ShapeDtypeStruct((rows_dev, width), F32),
        [SMEM] + [VMEM] * 6,
        VMEM,
        [
            pltpu.VMEM((2,) + shared_half.shape, BF16),
            pltpu.VMEM((shared_size, width), BF16),
        ],
        2 * n_tp * rows_dev * width * shared_size * 3,
        10 * rows_dev * width * 2,
        20,
    )(core, normed, shared_own, shared_near, shared_other, shared_mine, shared_theirs)

    pieces, chunks = 4, 3
    answers = call(
        expert_kernel,
        jax.ShapeDtypeStruct((tile_rows, LANES), BF16),
        [HBM] * 4,
        HBM,
        [
            pltpu.VMEM((width, hidden_size), BF16),
            pltpu.VMEM((width, hidden_size), BF16),
            pltpu.VMEM((hidden_size, width), BF16),
            pltpu.VMEM((slots, width), BF16),
            pltpu.VMEM((tile_rows, LANES), BF16),
            pltpu.VMEM((tile_rows, LANES), BF16),
            pltpu.SemaphoreType.DMA((3, pieces)),
            pltpu.SemaphoreType.DMA((chunks,)),
            pltpu.SemaphoreType.DMA((chunks,)),
        ],
        2 * slots * width * hidden_size * 3,
        3 * 2 * width * hidden_size,
        62,
    )(arrived.reshape(tile_rows, LANES), expert_gate, expert_up, expert_down)
    returned = lax.all_to_all(
        answers.reshape(experts, capacity * TILE, LANES),
        EP_TP,
        split_axis=0,
        concat_axis=0,
        tiled=True,
    )

    gated_shape = jax.ShapeDtypeStruct((rows_dev, heads * value_size), BF16)
    own_mixed, *gated = call(
        retention_kernel,
        (jax.ShapeDtypeStruct((rows_dev, width), BF16),) + (gated_shape,) * (n_tp - 1),
        [SMEM] + [VMEM] * 9,
        (VMEM,) * n_tp,
        [pltpu.VMEM((span, heads * value_size), BF16)],
        2 * span * heads * value_size * 1000,
        10 * rows_dev * width * 2,
        20,
    )(seat, queries, keys, values, gate, log_decay.T, cosine, sine, state_in, w_out)
    gated_left, gated_far, gated_right = [moved_by(gated[d - 1], "tp", d) for d in around]

    return call(
        finish_kernel,
        tuple(jax.ShapeDtypeStruct((rows_dev, width), BF16) for _ in range(2)),
        [SMEM, SMEM] + [VMEM] * 6 + [HBM] * 5,
        (VMEM,) * 2,
        [
            pltpu.VMEM((top, rows_dev * TILE, LANES), F32),
            pltpu.VMEM((rows_dev, width), F32),
            pltpu.VMEM((2 * half_out, width), BF16),
            pltpu.VMEM((2 * half_out, width), BF16),
            pltpu.VMEM((2, half_out, width), BF16),
            pltpu.SemaphoreType.DMA((5,)),
        ],
        2 * rows_dev * width * 1500,
        10 * rows_dev * width * 2,
        28,
    )(
        places,
        core,
        returned.reshape(tile_rows, LANES),
        route_weight,
        own_mixed,
        gated_left,
        gated_right,
        gated_far,
        shared_sum,
        out_near,
        out_other,
        out_mine,
        out_theirs,
    )


def solution(mesh):
    split = Mesh(
        mesh.devices.reshape(
            mesh.shape["grp"], mesh.shape["ep"] // (2 * CHIPS), CHIPS, 2, mesh.shape["tp"]
        ),
        GRP_EP_TP,
    )
    return jax.shard_map(
        per_device,
        mesh=split,
        in_specs=(
            P(GRP_EP, "tp"),
            P(GRP_EP, "tp"),
            P(GRP_EP, "tp"),
            P(GRP_EP, "tp"),
            P(GRP_EP, "tp"),
            P("tp", None),
            P(GRP_EP_TP, None),
            P(),
            P(GRP_EP_TP, None),
            P(GRP_EP_TP, None),
            P(EP_TP, None, None),
            P(EP_TP, None, None),
            P(EP_TP, None, None),
            P(None, "tp"),
            P(None, "tp"),
            P("tp", None),
        ),
        out_specs=(P(GRP_EP_TP, None), P(GRP_EP_TP, None)),
        check_vma=False,
    )
```

```python
import jax
import jax.numpy as jnp
from jax import lax
from jax.experimental import pallas as pl
from jax.experimental.pallas import tpu as pltpu
from jax.sharding import Mesh
from jax.sharding import PartitionSpec as P


BLOCK = 128
LANES = 128
TILE = 16
CHIPS = 2
EP = ("ep_hi", "ep_lo", "ep_1")
EP_TP = EP + ("tp",)
GRP_EP = ("grp",) + EP
GRP_EP_TP = ("grp",) + EP_TP
STATE_ROWS = 80

ROPE_BASE = 10000.0
GROUP_EPS = 1e-05
NORM_EPS = 1e-06


VMEM = pl.BlockSpec(memory_space=pltpu.VMEM)
SMEM = pl.BlockSpec(memory_space=pltpu.SMEM)
HBM = pl.BlockSpec(memory_space=pltpu.HBM)
F32 = jnp.float32
BF16 = jnp.bfloat16
MIB = 1 << 20


def call(kernel, out_shape, in_specs, out_specs, scratch, flops, moved, limit):
    return pl.pallas_call(
        kernel,
        out_shape=out_shape,
        in_specs=in_specs,
        out_specs=out_specs,
        scratch_shapes=scratch,
        compiler_params=pltpu.CompilerParams(vmem_limit_bytes=int(limit * MIB)),
        cost_estimate=pl.CostEstimate(flops=flops, bytes_accessed=moved, transcendentals=0),
    )


def dot(a, b):
    return jnp.dot(a, b, preferred_element_type=F32)


def swap_matrix():
    side = TILE * TILE
    row = lax.broadcasted_iota(jnp.int32, (side, side), 0)
    col = lax.broadcasted_iota(jnp.int32, (side, side), 1)
    hit = (row // TILE == col % TILE) & (row % TILE == col // TILE)
    return jnp.where(hit, 1.0, 0.0).astype(BF16)


def rows_to_tiles(swap, rows):
    count = rows.shape[0] // TILE
    width = rows.shape[1] // LANES
    found = []
    for at in range(0, count, 2):
        pair = [
            jnp.concatenate(
                [
                    rows[g * TILE : (g + 1) * TILE, k * LANES : (k + 1) * LANES]
                    for k in range(width)
                ],
                axis=0,
            )
            for g in range(at, min(at + 2, count))
        ]
        out = dot(swap, jnp.concatenate(pair, axis=1)).astype(BF16)
        found += [out[:, g * LANES : (g + 1) * LANES] for g in range(len(pair))]
    return found


def column(c):
    return slice(c * LANES, (c + 1) * LANES)


def prep_kernel(
    routes, x_hbm, gain_hbm, normed_hbm, outbound, places, x, gain, normed, tiles, used, sems
):
    copies = [
        pltpu.make_async_copy(x_hbm, x, sems.at[0]),
        pltpu.make_async_copy(gain_hbm, gain, sems.at[1]),
    ]
    for copy in copies:
        copy.start()
    outbound[...] = jnp.zeros_like(outbound)
    top, number = routes.shape
    experts = used.shape[0]
    capacity = outbound.shape[0] // (experts * TILE)
    for e in range(experts):
        used[e] = 0

    @pl.loop(0, number, unroll=8)
    def _(n):
        for k in range(top):
            e = routes[k, n]
            rank = used[e]
            used[e] = rank + 1
            places[k, n] = e * capacity + rank

    for copy in copies:
        copy.wait()
    source = x[...].astype(F32)
    scale = lax.rsqrt(jnp.mean(source * source, axis=-1, keepdims=True) + NORM_EPS)
    rows = (source * scale * gain[...]).astype(BF16)
    normed[...] = rows
    keep = pltpu.make_async_copy(normed, normed_hbm, sems.at[2])
    keep.start()
    wide = rows.astype(F32)
    for c in range(TILE):
        tiles[pl.ds(c, number, stride=TILE), :] = wide[:, column(c)]

    @pl.loop(0, number, unroll=8)
    def _(n):
        row = tiles[pl.ds(pl.multiple_of(n * TILE, TILE), TILE), :].astype(BF16)
        for k in range(top):
            at = pl.multiple_of(places[k, n] * TILE, TILE)
            outbound[pl.ds(at, TILE), :] = row

    keep.wait()


def expert_kernel(
    arrived_hbm,
    gate_hbm,
    up_hbm,
    down_hbm,
    out_hbm,
    gate_w,
    up_w,
    down_w,
    rows,
    arrived,
    out,
    sems,
    in_sems,
    out_sems,
):
    pieces = sems.shape[1]
    chunks = out_sems.shape[0]
    share = arrived.shape[0] // chunks
    landed = []
    for j in range(chunks):
        at = pl.ds(j * share, share)
        landed.append(pltpu.make_async_copy(arrived_hbm.at[at], arrived.at[at], in_sems.at[j]))
        landed[-1].start()
    copies = [[], [], []]
    for i, (src, dst) in enumerate(((gate_hbm, gate_w), (up_hbm, up_w), (down_hbm, down_w))):
        part = dst.shape[0] // pieces
        for j in range(pieces):
            at = pl.ds(j * part, part)
            copies[i].append(pltpu.make_async_copy(src.at[0, at], dst.at[at], sems.at[i, j]))
    swap = swap_matrix()
    side = TILE * TILE
    groups = arrived.shape[0] // side
    for at in range(0, groups, 2):
        if at * side % share == 0:
            landed[at * side // share].wait()
            for copy in copies[at * side // share]:
                copy.start()
        pair = jnp.concatenate(
            [arrived[g * side : (g + 1) * side, :] for g in (at, at + 1)], axis=1
        )
        turned = dot(swap, pair).astype(BF16)
        for j in range(2):
            for k in range(TILE):
                rows[
                    (at + j) * TILE : (at + j + 1) * TILE, k * LANES : (k + 1) * LANES
                ] = turned[k * TILE : (k + 1) * TILE, j * LANES : (j + 1) * LANES]
    for copy in copies[0]:
        copy.wait()
    gated = jax.nn.silu(dot(rows[...], gate_w[...]))
    for copy in copies[1]:
        copy.wait()
    hidden = (gated * dot(rows[...], up_w[...])).astype(BF16)
    for copy in copies[2]:
        copy.wait()
    left = []
    step = rows.shape[0] // chunks
    for at in range(0, down_w.shape[1], 4 * LANES):
        rows[:, at : at + 4 * LANES] = dot(hidden, down_w[:, at : at + 4 * LANES]).astype(BF16)
    for j in range(chunks):
        for g, tile in enumerate(rows_to_tiles(swap, rows[j * step : (j + 1) * step, :])):
            out[j * share + g * side : j * share + (g + 1) * side, :] = tile
        at = pl.ds(j * share, share)
        left.append(pltpu.make_async_copy(out.at[at], out_hbm.at[at], out_sems.at[j]))
        left[-1].start()
    for copy in left:
        copy.wait()


def turn_matrix():
    row = lax.broadcasted_iota(jnp.int32, (LANES, LANES), 0)
    col = lax.broadcasted_iota(jnp.int32, (LANES, LANES), 1)
    return row, col


def rotated(x, cosine, sine, half):
    row, col = turn_matrix()
    first = col % (2 * half) < half
    partner = jnp.where(first, col + half, col - half)
    turn = jnp.where(row == partner, jnp.where(first, -1.0, 1.0), 0.0).astype(BF16)
    return x.astype(F32) * cosine + dot(x, turn) * sine


def lower(size, strict=False):
    row = lax.broadcasted_iota(jnp.int32, (size, size), 0)
    col = lax.broadcasted_iota(jnp.int32, (size, size), 1)
    return row > col if strict else row >= col


def summed_f32(a, b, dims):
    return lax.dot_general(
        a, b, (dims, ((), ())), preferred_element_type=F32, precision=lax.Precision.HIGHEST
    )


def spread_heads(per_head, key_size):
    lane = lax.broadcasted_iota(jnp.int32, (per_head.shape[0], LANES), 1)
    out = per_head[:, 0:1]
    for h in range(1, per_head.shape[1]):
        out = jnp.where(lane >= h * key_size, per_head[:, h : h + 1], out)
    return out


def state_kernel(k_hbm, v_hbm, decay_hbm, cosine, sine, packed, k, v, log_decay, sems):
    pairs = ((decay_hbm, log_decay), (k_hbm, k), (v_hbm, v))
    copies = [pltpu.make_async_copy(a, b, sems.at[i]) for i, (a, b) in enumerate(pairs)]
    for copy in copies:
        copy.start()
    for copy in copies:
        copy.wait()
    heads = log_decay.shape[0]
    key_size = k.shape[1] // heads
    value_size = v.shape[1] // heads
    span = k.shape[0]
    k_rot = (rotated(k[...], cosine[...], sine[...], key_size // 2) * key_size ** (-0.5)).astype(
        BF16
    )
    above = jnp.where(lower(BLOCK, True), 1.0, 0.0)
    after = jnp.zeros((1, heads), F32)
    tails = [None] * (span // BLOCK)
    for b in reversed(range(span // BLOCK)):
        part = log_decay[:, b * BLOCK : (b + 1) * BLOCK]
        tails[b] = summed_f32(above, part, ((0,), (1,))) + after
        after = after + summed_f32(jnp.ones((1, BLOCK), F32), part, ((1,), (1,)))
    tail = jnp.concatenate(tails, axis=0)
    faded = (k_rot.astype(F32) * jnp.exp(spread_heads(tail, key_size))).astype(BF16)
    state = dot(faded.T, v[...])
    for h in range(heads):
        packed[h * STATE_ROWS : h * STATE_ROWS + key_size, :] = state[
            h * key_size : (h + 1) * key_size, h * value_size : (h + 1) * value_size
        ].astype(BF16)
        whole = after[:, h : h + 1]
        high = whole.astype(BF16)
        low = (whole - high.astype(F32)).astype(BF16)
        pad = STATE_ROWS - key_size
        row = lax.broadcasted_iota(jnp.int32, (pad, LANES), 0)
        packed[h * STATE_ROWS + key_size : (h + 1) * STATE_ROWS, :] = jnp.where(
            row == 0, high.astype(F32), low.astype(F32)
        ).astype(BF16)


def retention_kernel(seat, q, k, v, gate, log_decay, cosine, sine, state_in, w_out, *rest):
    own, *outs, gated = rest
    heads = log_decay.shape[0]
    key_size = q.shape[1] // heads
    value_size = v.shape[1] // heads
    span = q.shape[0]
    q_rot = rotated(q[...], cosine[...], sine[...], key_size // 2).astype(BF16)
    k_rot = (rotated(k[...], cosine[...], sine[...], key_size // 2) * key_size ** (-0.5)).astype(
        BF16
    )
    keep = lower(BLOCK)
    ones = jnp.where(keep, 1.0, 0.0)
    lane = lax.broadcasted_iota(jnp.int32, (BLOCK, LANES), 1)
    state = state_in[...]
    for b in range(span // BLOCK):
        at = slice(b * BLOCK, (b + 1) * BLOCK)
        part = log_decay[:, at]
        column = summed_f32(ones, part, ((1,), (1,)))
        across = summed_f32(part, ones, ((1,), (1,)))
        total = column[BLOCK - 1 : BLOCK, :]
        q_part = q_rot[at, :]
        k_part = k_rot[at, :]
        v_part = v[at, :]
        lifted = q_part.astype(F32) * jnp.exp(spread_heads(column, key_size))
        tail = jnp.exp(spread_heads(total - column, key_size))
        faded = (k_part.astype(F32) * tail).astype(BF16)
        held = state.astype(BF16)
        grown = dot(faded.T, v_part)
        fade = []
        for h in range(heads):
            mine = (lane >= h * key_size) & (lane < (h + 1) * key_size)
            q_head = jnp.where(mine, q_part.astype(F32), 0.0).astype(BF16)
            scores = lax.dot_general(
                q_head, k_part, (((1,), (1,)), ((), ())), preferred_element_type=F32
            )
            gap = jnp.where(keep, column[:, h : h + 1] - across[h : h + 1, :], 0.0)
            weights = jnp.where(keep, scores * jnp.exp(gap), 0.0).astype(BF16)
            columns = slice(h * value_size, (h + 1) * value_size)
            kept = dot(weights, v_part[:, columns]) + dot(
                jnp.where(mine, lifted, 0.0).astype(BF16), held
            )
            center = jnp.mean(kept, axis=-1, keepdims=True)
            off = kept - center
            spread = jnp.mean(off * off, axis=-1, keepdims=True)
            act = jax.nn.silu(gate[at, columns].astype(F32))
            gated[at, columns] = (act * (off * lax.rsqrt(spread + GROUP_EPS))).astype(BF16)
            fade.append(
                state[h * key_size : (h + 1) * key_size, :] * jnp.exp(total[:, h : h + 1])
                + grown[h * key_size : (h + 1) * key_size, columns]
            )
        state = jnp.concatenate(fade, axis=0)
    count = len(outs) + 1
    share = span // count
    for d in range(count):
        first = lax.rem(seat[0] + d, count) * share
        part = gated[pl.ds(pl.multiple_of(first, share), share), :]
        if d == 0:
            own[...] = dot(part, w_out[...]).astype(BF16)
        else:
            outs[d - 1][...] = part


def pack_kernel(core, gate_w, up_w, down_w, w_out, whole, half, out_half):
    def fill(to, first, depth, cut, thin):
        to[0:depth, :] = gate_w[pl.ds(first, depth), :]
        to[depth : 2 * depth, :] = up_w[pl.ds(first, depth), :]
        for k in range(down_w.shape[1] // LANES):
            at = 2 * depth + k * thin
            to[at : at + thin, :] = down_w[pl.ds(cut, thin), k * LANES : (k + 1) * LANES]

    depth, thin = gate_w.shape[0], down_w.shape[0]
    fill(whole, 0, depth, 0, thin)
    at = pl.multiple_of(core[0] * (depth // 2), TILE)
    cut = pl.multiple_of(core[0] * (thin // 2), TILE)
    fill(half, at, depth // 2, cut, thin // 2)
    share = out_half.shape[0]
    out_half[...] = w_out[pl.ds(pl.multiple_of(core[0] * share, TILE), share), :]


def shared_kernel(core, normed, own, near, near_other, mine, theirs, out, packed, down):
    rows = normed[...]
    depth = rows.shape[1]
    total = None
    for part in (own, near, near_other):
        hidden = jax.nn.silu(dot(rows, part[0:depth, :])) * dot(rows, part[depth : 2 * depth, :])
        thin = down.shape[0]
        for k in range(down.shape[1] // LANES):
            at = 2 * depth + k * thin
            down[:, k * LANES : (k + 1) * LANES] = part[at : at + thin, :]
        product = dot(hidden.astype(BF16), down[...])
        total = product if total is None else total + product
    packed[0] = jnp.where(core[0] == 0, mine[...], theirs[...])
    packed[1] = jnp.where(core[0] == 0, theirs[...], mine[...])
    half = depth // 2
    thin = down.shape[0] // 2
    gated = dot(rows[:, :half], packed[0, :half]) + dot(rows[:, half:], packed[1, :half])
    up = dot(rows[:, :half], packed[0, half:depth]) + dot(rows[:, half:], packed[1, half:depth])
    for c in range(2):
        for k in range(down.shape[1] // LANES):
            at = depth + k * thin
            down[c * thin : (c + 1) * thin, k * LANES : (k + 1) * LANES] = packed[c, at : at + thin]
    hidden = (jax.nn.silu(gated) * up).astype(BF16)
    out[...] = total + dot(hidden, down[...])


def finish_kernel(
    places,
    core,
    returned,
    weight,
    own,
    gated_left,
    gated_right,
    gated_far,
    shared_hbm,
    near_hbm,
    other_hbm,
    mine_hbm,
    theirs_hbm,
    mixer_out,
    moe_out,
    picked,
    shared,
    near,
    other,
    far,
    sems,
):
    share = far.shape[1]
    pairs = (
        (shared_hbm, shared),
        (near_hbm, near),
        (other_hbm, other),
        (mine_hbm, far.at[0]),
        (theirs_hbm, far.at[1]),
    )
    copies = [pltpu.make_async_copy(a, b, sems.at[i]) for i, (a, b) in enumerate(pairs)]
    for copy in copies:
        copy.start()
    number = moe_out.shape[0]
    top = weight.shape[1]

    @pl.loop(0, number, unroll=8)
    def _(n):
        for k in range(top):
            place = places[k, n]
            picked[k, pl.ds(pl.multiple_of(n * TILE, TILE), TILE), :] = returned[
                pl.ds(pl.multiple_of(place * TILE, TILE), TILE), :
            ].astype(F32)

    copies[0].wait()
    for c in range(TILE):
        total = shared[:, column(c)]
        for k in range(top):
            total = total + picked[k, pl.ds(c, number, stride=TILE), :] * weight[:, k : k + 1]
        moe_out[:, column(c)] = total.astype(BF16)
    for copy in copies[1:]:
        copy.wait()
    first = core[0] == 0
    left, right, across = gated_left[...], gated_right[...], gated_far[...]
    mixed = own[...].astype(F32)
    mixed = mixed + dot(jnp.where(first, left, right), near[...])
    mixed = mixed + dot(jnp.where(first, right, left), other[...])
    low, high = across[:, :share], across[:, share:]
    mixed = mixed + dot(jnp.where(first, low, high), far[0])
    mixed = mixed + dot(jnp.where(first, high, low), far[1])
    mixer_out[...] = mixed.astype(BF16)


def moved_by(array, axis, step):
    count = lax.axis_size(axis)
    return lax.ppermute(array, axis, [(s, (s + step) % count) for s in range(count)])


def outward(array):
    count = lax.axis_size("tp")
    pairs = [(s, (s + 1) % count) for s in range(count)]
    pairs += [(count + s, count + (s - 1) % count) for s in range(count)]
    return lax.ppermute(array, ("ep_1", "tp"), pairs)


def opened(packed):
    wide = packed.astype(F32)
    size = STATE_ROWS - TILE
    return wide[size : size + 1, :] + wide[size + 1 : size + 2, :], wide[:size, :]


def closed(part):
    log, state = part
    high = log.astype(BF16).astype(F32)
    row = lax.broadcasted_iota(jnp.int32, (TILE, LANES), 0)
    return jnp.concatenate([state, jnp.where(row == 0, high, log - high)], axis=0).astype(BF16)


def joined(earlier, later):
    return earlier[0] + later[0], earlier[1] * jnp.exp(later[0]) + later[1]


def picked_by(core, a, b):
    return jnp.where(core == 0, a.astype(F32), b.astype(F32)).astype(BF16)


def chip_kernel(core, own, other, out):
    mine = picked_by(core[0], own[:STATE_ROWS, :], own[STATE_ROWS:, :])
    theirs = picked_by(core[0], other[:STATE_ROWS, :], other[STATE_ROWS:, :])
    early, late = picked_by(core[0], mine, theirs), picked_by(core[0], theirs, mine)
    out[...] = closed(joined(opened(early), opened(late)))


def near_kernel(seat, chip, *refs):
    *near, before, window = refs
    count = len(near) + 1
    found = [chip[...].astype(F32)] + [part[...].astype(F32) for part in near]
    start = whole = None
    for p in range(count):
        back = lax.rem(seat[0] + count - p, count)
        part = found[0]
        for d in range(1, count):
            part = jnp.where(back == d, found[d], part)
        item = opened(part)
        early = opened(jnp.where(seat[0] > p, part, 0.0))
        start = early if start is None else joined(start, early)
        whole = item if whole is None else joined(whole, item)
    before[...] = closed(start)
    window[...] = closed(whole)


def far_kernel(seat, before, *refs):
    *far, prefix = refs
    start = None
    for d in range(len(far), 0, -1):
        early = opened(jnp.where(seat[0] >= d, far[d - 1][...].astype(F32), 0.0))
        start = early if start is None else joined(start, early)
    prefix[...] = closed(joined(start, opened(before[...])))


def enter_kernel(core, mine, theirs, other, state):
    size = STATE_ROWS - TILE
    for h in range(other.shape[0] // STATE_ROWS):
        held = jnp.where(core[0] == h, mine[...].astype(F32), theirs[...].astype(F32))
        chip_before = opened(held)
        first = opened(other[h * STATE_ROWS : (h + 1) * STATE_ROWS, :])
        both = joined(chip_before, first)
        state[h * size : (h + 1) * size, :] = jnp.where(core[0] == 0, chip_before[1], both[1])


def small(kernel, outs, in_specs, out_specs):
    return call(kernel, outs, in_specs, out_specs, [], 100000, 100000, 2)


def per_device(
    queries,
    keys,
    values,
    gate,
    log_decay,
    w_out,
    moe_input,
    moe_gain,
    routes,
    route_weight,
    expert_gate,
    expert_up,
    expert_down,
    shared_gate,
    shared_up,
    shared_down,
):
    span = queries.shape[0]
    heads = log_decay.shape[1]
    key_size = queries.shape[1] // heads
    value_size = values.shape[1] // heads
    rows_dev, width = moe_input.shape
    top = routes.shape[1]
    n_tp = lax.axis_size("tp")
    experts = lax.axis_size(EP) * n_tp
    capacity = rows_dev * top * 3 // (2 * experts)
    hidden_size = expert_gate.shape[2]
    shared_size = shared_gate.shape[1]
    slots = experts * capacity
    tile_rows = slots * TILE

    core = lax.axis_index("ep_1").reshape(1).astype(jnp.int32)
    seat = lax.axis_index("tp").reshape(1).astype(jnp.int32)
    around = range(1, n_tp)
    half_out = w_out.shape[0] // 2
    packed_shape = jax.ShapeDtypeStruct((STATE_ROWS, value_size), BF16)

    out_near = outward(w_out)

    normed, outbound, places = call(
        prep_kernel,
        (
            jax.ShapeDtypeStruct((rows_dev, width), BF16),
            jax.ShapeDtypeStruct((tile_rows, LANES), BF16),
            jax.ShapeDtypeStruct((top, rows_dev), jnp.int32),
        ),
        [SMEM, HBM, HBM],
        (HBM, VMEM, SMEM),
        [
            pltpu.VMEM((rows_dev, width), BF16),
            pltpu.VMEM((1, width), F32),
            pltpu.VMEM((rows_dev, width), BF16),
            pltpu.VMEM((rows_dev * TILE, LANES), F32),
            pltpu.SMEM((experts,), jnp.int32),
            pltpu.SemaphoreType.DMA((3,)),
        ],
        2 * rows_dev * width * 256,
        4 * rows_dev * width,
        62,
    )(routes.T, moe_input, moe_gain.reshape(1, width))

    arrived = lax.all_to_all(
        outbound.reshape(experts, capacity * TILE, LANES),
        EP_TP,
        split_axis=0,
        concat_axis=0,
        tiled=True,
    )

    half = key_size // 2
    frequency = ROPE_BASE ** (-jnp.arange(half, dtype=F32) / half)
    spots = lax.axis_index(EP) * span + jnp.arange(span, dtype=jnp.int32)
    angles = spots.astype(F32)[:, None] * jnp.tile(frequency, LANES // half)[None, :]
    cosine = jnp.cos(angles)
    sine = jnp.sin(angles)

    own = call(
        state_kernel,
        jax.ShapeDtypeStruct((heads * STATE_ROWS, value_size), BF16),
        [HBM] * 3 + [VMEM] * 2,
        VMEM,
        [
            pltpu.VMEM(keys.shape, BF16),
            pltpu.VMEM(values.shape, BF16),
            pltpu.VMEM((heads, span), F32),
            pltpu.SemaphoreType.DMA((3,)),
        ],
        2 * span * LANES * 512,
        4 * span * LANES * 4,
        61,
    )(keys, values, log_decay.T, cosine, sine)
    other = moved_by(own, "ep_1", 1)
    chip = small(chip_kernel, packed_shape, [SMEM, VMEM, VMEM], VMEM)(core, own, other)
    low_seat = lax.axis_index("ep_lo").reshape(1).astype(jnp.int32)
    high_seat = lax.axis_index("ep_hi").reshape(1).astype(jnp.int32)
    near = [moved_by(chip, "ep_lo", d) for d in range(1, lax.axis_size("ep_lo"))]
    before, window = small(
        near_kernel, (packed_shape, packed_shape), [SMEM] + [VMEM] * (1 + len(near)), (VMEM, VMEM)
    )(low_seat, chip, *near)
    far = [moved_by(window, "ep_hi", d) for d in range(1, lax.axis_size("ep_hi"))]
    prefix = small(far_kernel, packed_shape, [SMEM] + [VMEM] * (1 + len(far)), VMEM)(
        high_seat, before, *far
    )
    swapped = moved_by(prefix, "ep_1", 1)
    state_in = small(
        enter_kernel,
        jax.ShapeDtypeStruct((heads * key_size, value_size), F32),
        [SMEM] + [VMEM] * 3,
        VMEM,
    )(core, prefix, swapped, other)

    pack_rows = width * 3 * shared_size // LANES
    shared_own, shared_half, out_half = call(
        pack_kernel,
        (
            jax.ShapeDtypeStruct((pack_rows, LANES), BF16),
            jax.ShapeDtypeStruct((pack_rows // 2, LANES), BF16),
            jax.ShapeDtypeStruct((half_out, width), BF16),
        ),
        [SMEM] + [VMEM] * 4,
        (VMEM,) * 3,
        [],
        100000,
        6 * width * shared_size,
        16,
    )(core, shared_gate, shared_up, shared_down, w_out)
    shared_near = outward(shared_own)
    shared_mine = moved_by(shared_half, "tp", 2)
    out_mine = moved_by(out_half, "tp", 2)
    shared_other, shared_theirs, out_other, out_theirs = [
        moved_by(part, "ep_1", 1) for part in (shared_near, shared_mine, out_near, out_mine)
    ]
    shared_sum = call(
        shared_kernel,
        jax.ShapeDtypeStruct((rows_dev, width), F32),
        [SMEM] + [VMEM] * 6,
        VMEM,
        [
            pltpu.VMEM((2,) + shared_half.shape, BF16),
            pltpu.VMEM((shared_size, width), BF16),
        ],
        2 * n_tp * rows_dev * width * shared_size * 3,
        10 * rows_dev * width * 2,
        20,
    )(core, normed, shared_own, shared_near, shared_other, shared_mine, shared_theirs)

    pieces, chunks = 4, 3
    answers = call(
        expert_kernel,
        jax.ShapeDtypeStruct((tile_rows, LANES), BF16),
        [HBM] * 4,
        HBM,
        [
            pltpu.VMEM((width, hidden_size), BF16),
            pltpu.VMEM((width, hidden_size), BF16),
            pltpu.VMEM((hidden_size, width), BF16),
            pltpu.VMEM((slots, width), BF16),
            pltpu.VMEM((tile_rows, LANES), BF16),
            pltpu.VMEM((tile_rows, LANES), BF16),
            pltpu.SemaphoreType.DMA((3, pieces)),
            pltpu.SemaphoreType.DMA((chunks,)),
            pltpu.SemaphoreType.DMA((chunks,)),
        ],
        2 * slots * width * hidden_size * 3,
        3 * 2 * width * hidden_size,
        62,
    )(arrived.reshape(tile_rows, LANES), expert_gate, expert_up, expert_down)
    returned = lax.all_to_all(
        answers.reshape(experts, capacity * TILE, LANES),
        EP_TP,
        split_axis=0,
        concat_axis=0,
        tiled=True,
    )

    gated_shape = jax.ShapeDtypeStruct((rows_dev, heads * value_size), BF16)
    own_mixed, *gated = call(
        retention_kernel,
        (jax.ShapeDtypeStruct((rows_dev, width), BF16),) + (gated_shape,) * (n_tp - 1),
        [SMEM] + [VMEM] * 9,
        (VMEM,) * n_tp,
        [pltpu.VMEM((span, heads * value_size), BF16)],
        2 * span * heads * value_size * 1000,
        10 * rows_dev * width * 2,
        20,
    )(seat, queries, keys, values, gate, log_decay.T, cosine, sine, state_in, w_out)
    gated_left, gated_far, gated_right = [moved_by(gated[d - 1], "tp", d) for d in around]

    return call(
        finish_kernel,
        tuple(jax.ShapeDtypeStruct((rows_dev, width), BF16) for _ in range(2)),
        [SMEM, SMEM] + [VMEM] * 6 + [HBM] * 5,
        (VMEM,) * 2,
        [
            pltpu.VMEM((top, rows_dev * TILE, LANES), F32),
            pltpu.VMEM((rows_dev, width), F32),
            pltpu.VMEM((2 * half_out, width), BF16),
            pltpu.VMEM((2 * half_out, width), BF16),
            pltpu.VMEM((2, half_out, width), BF16),
            pltpu.SemaphoreType.DMA((5,)),
        ],
        2 * rows_dev * width * 1500,
        10 * rows_dev * width * 2,
        28,
    )(
        places,
        core,
        returned.reshape(tile_rows, LANES),
        route_weight,
        own_mixed,
        gated_left,
        gated_right,
        gated_far,
        shared_sum,
        out_near,
        out_other,
        out_mine,
        out_theirs,
    )


def solution(mesh):
    split = Mesh(
        mesh.devices.reshape(
            mesh.shape["grp"], mesh.shape["ep"] // (2 * CHIPS), CHIPS, 2, mesh.shape["tp"]
        ),
        GRP_EP_TP,
    )
    return jax.shard_map(
        per_device,
        mesh=split,
        in_specs=(
            P(GRP_EP, "tp"),
            P(GRP_EP, "tp"),
            P(GRP_EP, "tp"),
            P(GRP_EP, "tp"),
            P(GRP_EP, "tp"),
            P("tp", None),
            P(GRP_EP_TP, None),
            P(),
            P(GRP_EP_TP, None),
            P(GRP_EP_TP, None),
            P(EP_TP, None, None),
            P(EP_TP, None, None),
            P(EP_TP, None, None),
            P(None, "tp"),
            P(None, "tp"),
            P("tp", None),
        ),
        out_specs=(P(GRP_EP_TP, None), P(GRP_EP_TP, None)),
        check_vma=False,
    )
```

```python
import jax
import jax.numpy as jnp
from jax import lax
from jax.experimental import pallas as pl
from jax.experimental.pallas import tpu as pltpu
from jax.sharding import Mesh
from jax.sharding import PartitionSpec as P


BLOCK = 128
LANES = 128
TILE = 16
CHIPS = 2
EP = ("ep_hi", "ep_lo", "ep_1")
EP_TP = EP + ("tp",)
GRP_EP = ("grp",) + EP
GRP_EP_TP = ("grp",) + EP_TP
STATE_ROWS = 80

ROPE_BASE = 10000.0
GROUP_EPS = 1e-05
NORM_EPS = 1e-06


VMEM = pl.BlockSpec(memory_space=pltpu.VMEM)
SMEM = pl.BlockSpec(memory_space=pltpu.SMEM)
HBM = pl.BlockSpec(memory_space=pltpu.HBM)
F32 = jnp.float32
BF16 = jnp.bfloat16
MIB = 1 << 20


def call(kernel, out_shape, in_specs, out_specs, scratch, flops, moved, limit):
    return pl.pallas_call(
        kernel,
        out_shape=out_shape,
        in_specs=in_specs,
        out_specs=out_specs,
        scratch_shapes=scratch,
        compiler_params=pltpu.CompilerParams(vmem_limit_bytes=int(limit * MIB)),
        cost_estimate=pl.CostEstimate(flops=flops, bytes_accessed=moved, transcendentals=0),
    )


def dot(a, b):
    return jnp.dot(a, b, preferred_element_type=F32)


def swap_matrix():
    side = TILE * TILE
    row = lax.broadcasted_iota(jnp.int32, (side, side), 0)
    col = lax.broadcasted_iota(jnp.int32, (side, side), 1)
    hit = (row // TILE == col % TILE) & (row % TILE == col // TILE)
    return jnp.where(hit, 1.0, 0.0).astype(BF16)


def rows_to_tiles(swap, rows):
    count = rows.shape[0] // TILE
    width = rows.shape[1] // LANES
    found = []
    for at in range(0, count, 2):
        pair = [
            jnp.concatenate(
                [
                    rows[g * TILE : (g + 1) * TILE, k * LANES : (k + 1) * LANES]
                    for k in range(width)
                ],
                axis=0,
            )
            for g in range(at, min(at + 2, count))
        ]
        out = dot(swap, jnp.concatenate(pair, axis=1)).astype(BF16)
        found += [out[:, g * LANES : (g + 1) * LANES] for g in range(len(pair))]
    return found


def column(c):
    return slice(c * LANES, (c + 1) * LANES)


def prep_kernel(
    routes, x_hbm, gain_hbm, normed_hbm, outbound, places, x, gain, normed, tiles, used, sems
):
    copies = [
        pltpu.make_async_copy(x_hbm, x, sems.at[0]),
        pltpu.make_async_copy(gain_hbm, gain, sems.at[1]),
    ]
    for copy in copies:
        copy.start()
    outbound[...] = jnp.zeros_like(outbound)
    top, number = routes.shape
    experts = used.shape[0]
    capacity = outbound.shape[0] // (experts * TILE)
    for e in range(experts):
        used[e] = 0

    @pl.loop(0, number, unroll=8)
    def _(n):
        for k in range(top):
            e = routes[k, n]
            rank = used[e]
            used[e] = rank + 1
            places[k, n] = e * capacity + rank

    for copy in copies:
        copy.wait()
    source = x[...].astype(F32)
    scale = lax.rsqrt(jnp.mean(source * source, axis=-1, keepdims=True) + NORM_EPS)
    rows = (source * scale * gain[...]).astype(BF16)
    normed[...] = rows
    keep = pltpu.make_async_copy(normed, normed_hbm, sems.at[2])
    keep.start()
    wide = rows.astype(F32)
    for c in range(TILE):
        tiles[pl.ds(c, number, stride=TILE), :] = wide[:, column(c)]

    @pl.loop(0, number, unroll=8)
    def _(n):
        row = tiles[pl.ds(pl.multiple_of(n * TILE, TILE), TILE), :].astype(BF16)
        for k in range(top):
            at = pl.multiple_of(places[k, n] * TILE, TILE)
            outbound[pl.ds(at, TILE), :] = row

    keep.wait()


def expert_kernel(
    arrived_hbm,
    gate_hbm,
    up_hbm,
    down_hbm,
    out_hbm,
    gate_w,
    up_w,
    down_w,
    rows,
    arrived,
    out,
    sems,
    in_sems,
    out_sems,
):
    pieces = sems.shape[1]
    chunks = out_sems.shape[0]
    share = arrived.shape[0] // chunks
    landed = []
    for j in range(chunks):
        at = pl.ds(j * share, share)
        landed.append(pltpu.make_async_copy(arrived_hbm.at[at], arrived.at[at], in_sems.at[j]))
        landed[-1].start()
    copies = [[], [], []]
    for i, (src, dst) in enumerate(((gate_hbm, gate_w), (up_hbm, up_w), (down_hbm, down_w))):
        part = dst.shape[0] // pieces
        for j in range(pieces):
            at = pl.ds(j * part, part)
            copies[i].append(pltpu.make_async_copy(src.at[0, at], dst.at[at], sems.at[i, j]))
    swap = swap_matrix()
    side = TILE * TILE
    groups = arrived.shape[0] // side
    for at in range(0, groups, 2):
        if at * side % share == 0:
            landed[at * side // share].wait()
            for copy in copies[at * side // share]:
                copy.start()
        pair = jnp.concatenate(
            [arrived[g * side : (g + 1) * side, :] for g in (at, at + 1)], axis=1
        )
        turned = dot(swap, pair).astype(BF16)
        for j in range(2):
            for k in range(TILE):
                rows[
                    (at + j) * TILE : (at + j + 1) * TILE, k * LANES : (k + 1) * LANES
                ] = turned[k * TILE : (k + 1) * TILE, j * LANES : (j + 1) * LANES]
    for copy in copies[0]:
        copy.wait()
    gated = jax.nn.silu(dot(rows[...], gate_w[...]))
    for copy in copies[1]:
        copy.wait()
    hidden = (gated * dot(rows[...], up_w[...])).astype(BF16)
    for copy in copies[2]:
        copy.wait()
    left = []
    step = rows.shape[0] // chunks
    for at in range(0, down_w.shape[1], 4 * LANES):
        rows[:, at : at + 4 * LANES] = dot(hidden, down_w[:, at : at + 4 * LANES]).astype(BF16)
    for j in range(chunks):
        for g, tile in enumerate(rows_to_tiles(swap, rows[j * step : (j + 1) * step, :])):
            out[j * share + g * side : j * share + (g + 1) * side, :] = tile
        at = pl.ds(j * share, share)
        left.append(pltpu.make_async_copy(out.at[at], out_hbm.at[at], out_sems.at[j]))
        left[-1].start()
    for copy in left:
        copy.wait()


def turn_matrix():
    row = lax.broadcasted_iota(jnp.int32, (LANES, LANES), 0)
    col = lax.broadcasted_iota(jnp.int32, (LANES, LANES), 1)
    return row, col


def rotated(x, cosine, sine, half):
    row, col = turn_matrix()
    first = col % (2 * half) < half
    partner = jnp.where(first, col + half, col - half)
    turn = jnp.where(row == partner, jnp.where(first, -1.0, 1.0), 0.0).astype(BF16)
    return x.astype(F32) * cosine + dot(x, turn) * sine


def lower(size, strict=False):
    row = lax.broadcasted_iota(jnp.int32, (size, size), 0)
    col = lax.broadcasted_iota(jnp.int32, (size, size), 1)
    return row > col if strict else row >= col


def summed_f32(a, b, dims):
    return lax.dot_general(
        a, b, (dims, ((), ())), preferred_element_type=F32, precision=lax.Precision.HIGHEST
    )


def spread_heads(per_head, key_size):
    lane = lax.broadcasted_iota(jnp.int32, (per_head.shape[0], LANES), 1)
    out = per_head[:, 0:1]
    for h in range(1, per_head.shape[1]):
        out = jnp.where(lane >= h * key_size, per_head[:, h : h + 1], out)
    return out


def state_kernel(first, k_hbm, v_hbm, decay_hbm, frequency, packed, k, v, log_decay, sems):
    pairs = ((decay_hbm, log_decay), (k_hbm, k), (v_hbm, v))
    copies = [pltpu.make_async_copy(a, b, sems.at[i]) for i, (a, b) in enumerate(pairs)]
    for copy in copies:
        copy.start()
    half = k.shape[1] // log_decay.shape[0] // 2
    groups = LANES // half
    depth = k.shape[0] // groups
    lane = lax.broadcasted_iota(jnp.int32, (depth, LANES), 1)
    spots = first[0] + lax.broadcasted_iota(jnp.int32, (depth, LANES), 0) + lane // half * depth
    angles = spots.astype(F32) * frequency[...]

    def spread(packed):
        found = []
        for b in range(groups):
            part = jnp.where(lane // half == b, packed, 0.0)
            shift = half
            while shift < LANES:
                part = part + pltpu.roll(part, shift, 1)
                shift *= 2
            found.append(part)
        return jnp.concatenate(found, axis=0)

    cosine, sine = spread(jnp.cos(angles)), spread(jnp.sin(angles))
    for copy in copies:
        copy.wait()
    heads = log_decay.shape[0]
    key_size = k.shape[1] // heads
    value_size = v.shape[1] // heads
    span = k.shape[0]
    k_rot = (rotated(k[...], cosine, sine, key_size // 2) * key_size ** (-0.5)).astype(BF16)
    above = jnp.where(lower(BLOCK, True), 1.0, 0.0)
    after = jnp.zeros((1, heads), F32)
    tails = [None] * (span // BLOCK)
    for b in reversed(range(span // BLOCK)):
        part = log_decay[:, b * BLOCK : (b + 1) * BLOCK]
        tails[b] = summed_f32(above, part, ((0,), (1,))) + after
        after = after + summed_f32(jnp.ones((1, BLOCK), F32), part, ((1,), (1,)))
    tail = jnp.concatenate(tails, axis=0)
    faded = (k_rot.astype(F32) * jnp.exp(spread_heads(tail, key_size))).astype(BF16)
    state = dot(faded.T, v[...])
    for h in range(heads):
        packed[h * STATE_ROWS : h * STATE_ROWS + key_size, :] = state[
            h * key_size : (h + 1) * key_size, h * value_size : (h + 1) * value_size
        ].astype(BF16)
        whole = after[:, h : h + 1]
        high = whole.astype(BF16)
        low = (whole - high.astype(F32)).astype(BF16)
        pad = STATE_ROWS - key_size
        row = lax.broadcasted_iota(jnp.int32, (pad, LANES), 0)
        packed[h * STATE_ROWS + key_size : (h + 1) * STATE_ROWS, :] = jnp.where(
            row == 0, high.astype(F32), low.astype(F32)
        ).astype(BF16)


def retention_kernel(seat, q, k, v, gate, log_decay, cosine, sine, state_in, w_out, *rest):
    own, *outs, gated = rest
    heads = log_decay.shape[0]
    key_size = q.shape[1] // heads
    value_size = v.shape[1] // heads
    span = q.shape[0]
    q_rot = rotated(q[...], cosine[...], sine[...], key_size // 2).astype(BF16)
    k_rot = (rotated(k[...], cosine[...], sine[...], key_size // 2) * key_size ** (-0.5)).astype(
        BF16
    )
    keep = lower(BLOCK)
    ones = jnp.where(keep, 1.0, 0.0)
    lane = lax.broadcasted_iota(jnp.int32, (BLOCK, LANES), 1)
    state = state_in[...]
    for b in range(span // BLOCK):
        at = slice(b * BLOCK, (b + 1) * BLOCK)
        part = log_decay[:, at]
        column = summed_f32(ones, part, ((1,), (1,)))
        across = summed_f32(part, ones, ((1,), (1,)))
        total = column[BLOCK - 1 : BLOCK, :]
        q_part = q_rot[at, :]
        k_part = k_rot[at, :]
        v_part = v[at, :]
        lifted = q_part.astype(F32) * jnp.exp(spread_heads(column, key_size))
        tail = jnp.exp(spread_heads(total - column, key_size))
        faded = (k_part.astype(F32) * tail).astype(BF16)
        held = state.astype(BF16)
        grown = dot(faded.T, v_part)
        fade = []
        for h in range(heads):
            mine = (lane >= h * key_size) & (lane < (h + 1) * key_size)
            q_head = jnp.where(mine, q_part.astype(F32), 0.0).astype(BF16)
            scores = lax.dot_general(
                q_head, k_part, (((1,), (1,)), ((), ())), preferred_element_type=F32
            )
            gap = jnp.where(keep, column[:, h : h + 1] - across[h : h + 1, :], 0.0)
            weights = jnp.where(keep, scores * jnp.exp(gap), 0.0).astype(BF16)
            columns = slice(h * value_size, (h + 1) * value_size)
            kept = dot(weights, v_part[:, columns]) + dot(
                jnp.where(mine, lifted, 0.0).astype(BF16), held
            )
            center = jnp.mean(kept, axis=-1, keepdims=True)
            off = kept - center
            spread = jnp.mean(off * off, axis=-1, keepdims=True)
            act = jax.nn.silu(gate[at, columns].astype(F32))
            gated[at, columns] = (act * (off * lax.rsqrt(spread + GROUP_EPS))).astype(BF16)
            fade.append(
                state[h * key_size : (h + 1) * key_size, :] * jnp.exp(total[:, h : h + 1])
                + grown[h * key_size : (h + 1) * key_size, columns]
            )
        state = jnp.concatenate(fade, axis=0)
    count = len(outs) + 1
    share = span // count
    for d in range(count):
        first = lax.rem(seat[0] + d, count) * share
        part = gated[pl.ds(pl.multiple_of(first, share), share), :]
        if d == 0:
            own[...] = dot(part, w_out[...]).astype(BF16)
        else:
            outs[d - 1][...] = part


def pack_kernel(core, gate_w, up_w, down_w, w_out, whole, half, out_half):
    def fill(to, first, depth, cut, thin):
        to[0:depth, :] = gate_w[pl.ds(first, depth), :]
        to[depth : 2 * depth, :] = up_w[pl.ds(first, depth), :]
        for k in range(down_w.shape[1] // LANES):
            at = 2 * depth + k * thin
            to[at : at + thin, :] = down_w[pl.ds(cut, thin), k * LANES : (k + 1) * LANES]

    depth, thin = gate_w.shape[0], down_w.shape[0]
    fill(whole, 0, depth, 0, thin)
    at = pl.multiple_of(core[0] * (depth // 2), TILE)
    cut = pl.multiple_of(core[0] * (thin // 2), TILE)
    fill(half, at, depth // 2, cut, thin // 2)
    share = out_half.shape[0]
    out_half[...] = w_out[pl.ds(pl.multiple_of(core[0] * share, TILE), share), :]


def shared_kernel(core, normed, own, near, near_other, mine, theirs, out, packed, down):
    rows = normed[...]
    depth = rows.shape[1]
    total = None
    for part in (own, near, near_other):
        hidden = jax.nn.silu(dot(rows, part[0:depth, :])) * dot(rows, part[depth : 2 * depth, :])
        thin = down.shape[0]
        for k in range(down.shape[1] // LANES):
            at = 2 * depth + k * thin
            down[:, k * LANES : (k + 1) * LANES] = part[at : at + thin, :]
        product = dot(hidden.astype(BF16), down[...])
        total = product if total is None else total + product
    packed[0] = jnp.where(core[0] == 0, mine[...], theirs[...])
    packed[1] = jnp.where(core[0] == 0, theirs[...], mine[...])
    half = depth // 2
    thin = down.shape[0] // 2
    gated = dot(rows[:, :half], packed[0, :half]) + dot(rows[:, half:], packed[1, :half])
    up = dot(rows[:, :half], packed[0, half:depth]) + dot(rows[:, half:], packed[1, half:depth])
    for c in range(2):
        for k in range(down.shape[1] // LANES):
            at = depth + k * thin
            down[c * thin : (c + 1) * thin, k * LANES : (k + 1) * LANES] = packed[c, at : at + thin]
    hidden = (jax.nn.silu(gated) * up).astype(BF16)
    out[...] = total + dot(hidden, down[...])


def finish_kernel(
    places,
    core,
    returned,
    weight,
    own,
    gated_left,
    gated_right,
    gated_far,
    shared_hbm,
    near_hbm,
    other_hbm,
    mine_hbm,
    theirs_hbm,
    mixer_out,
    moe_out,
    picked,
    shared,
    near,
    other,
    far,
    sems,
):
    share = far.shape[1]
    pairs = (
        (shared_hbm, shared),
        (near_hbm, near),
        (other_hbm, other),
        (mine_hbm, far.at[0]),
        (theirs_hbm, far.at[1]),
    )
    copies = [pltpu.make_async_copy(a, b, sems.at[i]) for i, (a, b) in enumerate(pairs)]
    for copy in copies:
        copy.start()
    number = moe_out.shape[0]
    top = weight.shape[1]

    @pl.loop(0, number, unroll=8)
    def _(n):
        for k in range(top):
            place = places[k, n]
            picked[k, pl.ds(pl.multiple_of(n * TILE, TILE), TILE), :] = returned[
                pl.ds(pl.multiple_of(place * TILE, TILE), TILE), :
            ].astype(F32)

    copies[0].wait()
    for c in range(TILE):
        total = shared[:, column(c)]
        for k in range(top):
            total = total + picked[k, pl.ds(c, number, stride=TILE), :] * weight[:, k : k + 1]
        moe_out[:, column(c)] = total.astype(BF16)
    for copy in copies[1:]:
        copy.wait()
    first = core[0] == 0
    left, right, across = gated_left[...], gated_right[...], gated_far[...]
    mixed = own[...].astype(F32)
    mixed = mixed + dot(jnp.where(first, left, right), near[...])
    mixed = mixed + dot(jnp.where(first, right, left), other[...])
    low, high = across[:, :share], across[:, share:]
    mixed = mixed + dot(jnp.where(first, low, high), far[0])
    mixed = mixed + dot(jnp.where(first, high, low), far[1])
    mixer_out[...] = mixed.astype(BF16)


def moved_by(array, axis, step):
    count = lax.axis_size(axis)
    return lax.ppermute(array, axis, [(s, (s + step) % count) for s in range(count)])


def outward(array):
    count = lax.axis_size("tp")
    pairs = [(s, (s + 1) % count) for s in range(count)]
    pairs += [(count + s, count + (s - 1) % count) for s in range(count)]
    return lax.ppermute(array, ("ep_1", "tp"), pairs)


def opened(packed):
    wide = packed.astype(F32)
    size = STATE_ROWS - TILE
    return wide[size : size + 1, :] + wide[size + 1 : size + 2, :], wide[:size, :]


def closed(part):
    log, state = part
    high = log.astype(BF16).astype(F32)
    row = lax.broadcasted_iota(jnp.int32, (TILE, LANES), 0)
    return jnp.concatenate([state, jnp.where(row == 0, high, log - high)], axis=0).astype(BF16)


def joined(earlier, later):
    return earlier[0] + later[0], earlier[1] * jnp.exp(later[0]) + later[1]


def picked_by(core, a, b):
    return jnp.where(core == 0, a.astype(F32), b.astype(F32)).astype(BF16)


def chip_kernel(core, own, other, out):
    mine = picked_by(core[0], own[:STATE_ROWS, :], own[STATE_ROWS:, :])
    theirs = picked_by(core[0], other[:STATE_ROWS, :], other[STATE_ROWS:, :])
    early, late = picked_by(core[0], mine, theirs), picked_by(core[0], theirs, mine)
    out[...] = closed(joined(opened(early), opened(late)))


def near_kernel(seat, chip, *refs):
    *near, before, window = refs
    count = len(near) + 1
    found = [chip[...].astype(F32)] + [part[...].astype(F32) for part in near]
    start = whole = None
    for p in range(count):
        back = lax.rem(seat[0] + count - p, count)
        part = found[0]
        for d in range(1, count):
            part = jnp.where(back == d, found[d], part)
        item = opened(part)
        early = opened(jnp.where(seat[0] > p, part, 0.0))
        start = early if start is None else joined(start, early)
        whole = item if whole is None else joined(whole, item)
    before[...] = closed(start)
    window[...] = closed(whole)


def far_kernel(seat, before, *refs):
    *far, prefix = refs
    start = None
    for d in range(len(far), 0, -1):
        early = opened(jnp.where(seat[0] >= d, far[d - 1][...].astype(F32), 0.0))
        start = early if start is None else joined(start, early)
    prefix[...] = closed(joined(start, opened(before[...])))


def enter_kernel(core, mine, theirs, other, state):
    size = STATE_ROWS - TILE
    for h in range(other.shape[0] // STATE_ROWS):
        held = jnp.where(core[0] == h, mine[...].astype(F32), theirs[...].astype(F32))
        chip_before = opened(held)
        first = opened(other[h * STATE_ROWS : (h + 1) * STATE_ROWS, :])
        both = joined(chip_before, first)
        state[h * size : (h + 1) * size, :] = jnp.where(core[0] == 0, chip_before[1], both[1])


def small(kernel, outs, in_specs, out_specs):
    return call(kernel, outs, in_specs, out_specs, [], 100000, 100000, 2)


def per_device(
    queries,
    keys,
    values,
    gate,
    log_decay,
    w_out,
    moe_input,
    moe_gain,
    routes,
    route_weight,
    expert_gate,
    expert_up,
    expert_down,
    shared_gate,
    shared_up,
    shared_down,
):
    span = queries.shape[0]
    heads = log_decay.shape[1]
    key_size = queries.shape[1] // heads
    value_size = values.shape[1] // heads
    rows_dev, width = moe_input.shape
    top = routes.shape[1]
    n_tp = lax.axis_size("tp")
    experts = lax.axis_size(EP) * n_tp
    capacity = rows_dev * top * 3 // (2 * experts)
    hidden_size = expert_gate.shape[2]
    shared_size = shared_gate.shape[1]
    slots = experts * capacity
    tile_rows = slots * TILE

    core = lax.axis_index("ep_1").reshape(1).astype(jnp.int32)
    seat = lax.axis_index("tp").reshape(1).astype(jnp.int32)
    around = range(1, n_tp)
    half_out = w_out.shape[0] // 2
    packed_shape = jax.ShapeDtypeStruct((STATE_ROWS, value_size), BF16)

    out_near = outward(w_out)

    normed, outbound, places = call(
        prep_kernel,
        (
            jax.ShapeDtypeStruct((rows_dev, width), BF16),
            jax.ShapeDtypeStruct((tile_rows, LANES), BF16),
            jax.ShapeDtypeStruct((top, rows_dev), jnp.int32),
        ),
        [SMEM, HBM, HBM],
        (HBM, VMEM, SMEM),
        [
            pltpu.VMEM((rows_dev, width), BF16),
            pltpu.VMEM((1, width), F32),
            pltpu.VMEM((rows_dev, width), BF16),
            pltpu.VMEM((rows_dev * TILE, LANES), F32),
            pltpu.SMEM((experts,), jnp.int32),
            pltpu.SemaphoreType.DMA((3,)),
        ],
        2 * rows_dev * width * 256,
        4 * rows_dev * width,
        62,
    )(routes.T, moe_input, moe_gain.reshape(1, width))

    arrived = lax.all_to_all(
        outbound.reshape(experts, capacity * TILE, LANES),
        EP_TP,
        split_axis=0,
        concat_axis=0,
        tiled=True,
    )

    half = key_size // 2
    frequency = ROPE_BASE ** (-jnp.arange(half, dtype=F32) / half)
    frequency = jnp.tile(frequency, LANES // half)[None, :]
    first = lax.axis_index(EP) * span
    spots = first + jnp.arange(span, dtype=jnp.int32)
    angles = spots.astype(F32)[:, None] * frequency
    cosine = jnp.cos(angles)
    sine = jnp.sin(angles)

    own = call(
        state_kernel,
        jax.ShapeDtypeStruct((heads * STATE_ROWS, value_size), BF16),
        [SMEM] + [HBM] * 3 + [VMEM],
        VMEM,
        [
            pltpu.VMEM(keys.shape, BF16),
            pltpu.VMEM(values.shape, BF16),
            pltpu.VMEM((heads, span), F32),
            pltpu.SemaphoreType.DMA((3,)),
        ],
        2 * span * LANES * 512,
        4 * span * LANES * 4,
        61,
    )(first.reshape(1).astype(jnp.int32), keys, values, log_decay.T, frequency)
    other = moved_by(own, "ep_1", 1)
    chip = small(chip_kernel, packed_shape, [SMEM, VMEM, VMEM], VMEM)(core, own, other)
    low_seat = lax.axis_index("ep_lo").reshape(1).astype(jnp.int32)
    high_seat = lax.axis_index("ep_hi").reshape(1).astype(jnp.int32)
    near = [moved_by(chip, "ep_lo", d) for d in range(1, lax.axis_size("ep_lo"))]
    before, window = small(
        near_kernel, (packed_shape, packed_shape), [SMEM] + [VMEM] * (1 + len(near)), (VMEM, VMEM)
    )(low_seat, chip, *near)
    far = [moved_by(window, "ep_hi", d) for d in range(1, lax.axis_size("ep_hi"))]
    prefix = small(far_kernel, packed_shape, [SMEM] + [VMEM] * (1 + len(far)), VMEM)(
        high_seat, before, *far
    )
    swapped = moved_by(prefix, "ep_1", 1)
    state_in = small(
        enter_kernel,
        jax.ShapeDtypeStruct((heads * key_size, value_size), F32),
        [SMEM] + [VMEM] * 3,
        VMEM,
    )(core, prefix, swapped, other)

    pack_rows = width * 3 * shared_size // LANES
    shared_own, shared_half, out_half = call(
        pack_kernel,
        (
            jax.ShapeDtypeStruct((pack_rows, LANES), BF16),
            jax.ShapeDtypeStruct((pack_rows // 2, LANES), BF16),
            jax.ShapeDtypeStruct((half_out, width), BF16),
        ),
        [SMEM] + [VMEM] * 4,
        (VMEM,) * 3,
        [],
        100000,
        6 * width * shared_size,
        16,
    )(core, shared_gate, shared_up, shared_down, w_out)
    shared_near = outward(shared_own)
    shared_mine = moved_by(shared_half, "tp", 2)
    out_mine = moved_by(out_half, "tp", 2)
    shared_other, shared_theirs, out_other, out_theirs = [
        moved_by(part, "ep_1", 1) for part in (shared_near, shared_mine, out_near, out_mine)
    ]
    shared_sum = call(
        shared_kernel,
        jax.ShapeDtypeStruct((rows_dev, width), F32),
        [SMEM] + [VMEM] * 6,
        VMEM,
        [
            pltpu.VMEM((2,) + shared_half.shape, BF16),
            pltpu.VMEM((shared_size, width), BF16),
        ],
        2 * n_tp * rows_dev * width * shared_size * 3,
        10 * rows_dev * width * 2,
        20,
    )(core, normed, shared_own, shared_near, shared_other, shared_mine, shared_theirs)

    pieces, chunks = 4, 3
    answers = call(
        expert_kernel,
        jax.ShapeDtypeStruct((tile_rows, LANES), BF16),
        [HBM] * 4,
        HBM,
        [
            pltpu.VMEM((width, hidden_size), BF16),
            pltpu.VMEM((width, hidden_size), BF16),
            pltpu.VMEM((hidden_size, width), BF16),
            pltpu.VMEM((slots, width), BF16),
            pltpu.VMEM((tile_rows, LANES), BF16),
            pltpu.VMEM((tile_rows, LANES), BF16),
            pltpu.SemaphoreType.DMA((3, pieces)),
            pltpu.SemaphoreType.DMA((chunks,)),
            pltpu.SemaphoreType.DMA((chunks,)),
        ],
        2 * slots * width * hidden_size * 3,
        3 * 2 * width * hidden_size,
        62,
    )(arrived.reshape(tile_rows, LANES), expert_gate, expert_up, expert_down)
    returned = lax.all_to_all(
        answers.reshape(experts, capacity * TILE, LANES),
        EP_TP,
        split_axis=0,
        concat_axis=0,
        tiled=True,
    )

    gated_shape = jax.ShapeDtypeStruct((rows_dev, heads * value_size), BF16)
    own_mixed, *gated = call(
        retention_kernel,
        (jax.ShapeDtypeStruct((rows_dev, width), BF16),) + (gated_shape,) * (n_tp - 1),
        [SMEM] + [VMEM] * 9,
        (VMEM,) * n_tp,
        [pltpu.VMEM((span, heads * value_size), BF16)],
        2 * span * heads * value_size * 1000,
        10 * rows_dev * width * 2,
        20,
    )(seat, queries, keys, values, gate, log_decay.T, cosine, sine, state_in, w_out)
    gated_left, gated_far, gated_right = [moved_by(gated[d - 1], "tp", d) for d in around]

    return call(
        finish_kernel,
        tuple(jax.ShapeDtypeStruct((rows_dev, width), BF16) for _ in range(2)),
        [SMEM, SMEM] + [VMEM] * 6 + [HBM] * 5,
        (VMEM,) * 2,
        [
            pltpu.VMEM((top, rows_dev * TILE, LANES), F32),
            pltpu.VMEM((rows_dev, width), F32),
            pltpu.VMEM((2 * half_out, width), BF16),
            pltpu.VMEM((2 * half_out, width), BF16),
            pltpu.VMEM((2, half_out, width), BF16),
            pltpu.SemaphoreType.DMA((5,)),
        ],
        2 * rows_dev * width * 1500,
        10 * rows_dev * width * 2,
        28,
    )(
        places,
        core,
        returned.reshape(tile_rows, LANES),
        route_weight,
        own_mixed,
        gated_left,
        gated_right,
        gated_far,
        shared_sum,
        out_near,
        out_other,
        out_mine,
        out_theirs,
    )


def solution(mesh):
    split = Mesh(
        mesh.devices.reshape(
            mesh.shape["grp"], mesh.shape["ep"] // (2 * CHIPS), CHIPS, 2, mesh.shape["tp"]
        ),
        GRP_EP_TP,
    )
    return jax.shard_map(
        per_device,
        mesh=split,
        in_specs=(
            P(GRP_EP, "tp"),
            P(GRP_EP, "tp"),
            P(GRP_EP, "tp"),
            P(GRP_EP, "tp"),
            P(GRP_EP, "tp"),
            P("tp", None),
            P(GRP_EP_TP, None),
            P(),
            P(GRP_EP_TP, None),
            P(GRP_EP_TP, None),
            P(EP_TP, None, None),
            P(EP_TP, None, None),
            P(EP_TP, None, None),
            P(None, "tp"),
            P(None, "tp"),
            P("tp", None),
        ),
        out_specs=(P(GRP_EP_TP, None), P(GRP_EP_TP, None)),
        check_vma=False,
    )
```
